256 devices in a mesh: kv: 32 (over z, x), tp: 8 (over y, core).
Axes of the slice: x: 4, y: 4, z: 8, core: 2. Of those that a mesh axis runs over, the one named last changes fastest.
Arguments:
- tokens: bfloat16 [256, 2048], P(None, 'kv'), may hold values from -16 to 16
- norm_gain: float32 [2048], P('kv'), may hold values from 0.1 to 1.9
- query_weight: bfloat16 [2048, 2048], P('kv', 'tp'), may hold values from -0.125 to 0.125
- key_weight: bfloat16 [2048, 2048], P('kv', 'tp'), may hold values from -0.125 to 0.125
- value_weight: bfloat16 [2048, 2048], P('kv', 'tp'), may hold values from -0.125 to 0.125
- gate_weight: bfloat16 [2048, 2048], P('kv', 'tp'), may hold values from -0.125 to 0.125
- beta_weight: bfloat16 [2048, 16], replicated, may hold values from -0.125 to 0.125
- decay_weight: bfloat16 [2048, 16], replicated, may hold values from -0.5 to 0.5
- decay_rate: float32 [16], P('tp'), may hold values from 0.0005 to 0.1
- head_gain: float32 [128], replicated, may hold values from 0.1 to 1.9
- carried_state: float32 [256, 16, 128, 128], P('kv', 'tp'), may hold values from -4 to 4
- block_keys: bfloat16 [256, 16, 64, 128], P('kv', 'tp'), may hold values from -1 to 1, as said below
- block_values: bfloat16 [256, 16, 64, 128], P('kv', 'tp'), may hold values from -6 to 6
- block_beta: float32 [256, 16, 64], P('kv', 'tp'), may hold values from 0.1 to 0.9
- block_decay: float32 [256, 16, 64], P('kv', 'tp'), may hold values from -1.2 to 0
- live_count: int32 [256], P('kv'), may hold values from 1 to 64, 6553 in all
- out_weight: bfloat16 [2048, 2048], P('tp', 'kv'), may hold values from -0.125 to 0.125
- mlp_gain: float32 [2048], replicated, may hold values from 0.1 to 1.9
- up_weight: bfloat16 [2048, 8192], P('kv', 'tp'), may hold values from -0.125 to 0.125
- down_weight: bfloat16 [8192, 2048], P('tp', 'kv'), may hold values from -0.0625 to 0.0625
Outputs:
- mixed: bfloat16 [256, 2048], P(None, 'kv')
- new_state: float32 [256, 16, 128, 128], P('kv', 'tp')
The draws below stay inside these ranges and needn't reach their ends.
Inputs may be any that keep to these rules, and one draw needn't show every extreme that they name: `block_keys`: every key vector along the last dimension has unit length up to rounding.
All inputs are finite; a program needn't handle non-finite values. No bound on the sum of `live_count` on one device may be relied on, other than what follows from the above.
Results may differ from the reference program's by a relative error of at most 0.023.
Values may be sent and summed in bfloat16 or wider, within the bound.
A program may use at most 64 MiB of HBM per device.

```python
import math
import jax
import jax.numpy as jnp
import numpy as np
from jax import lax

MODEL = 2048
HEADS = 16
HEAD_DIM = 128
MLP_UNITS = 8192
BLOCK_POSITIONS = 64
SEQ_DEV = 8
BATCH_TOTAL = 256
N_KV = 32
N_TP = 8


def head_rates(key):
    key_pick, key_fast, key_slow = jax.random.split(jax.random.fold_in(key, 11), 3)
    fast_heads = jax.random.randint(key_pick, (HEADS,), 0, 2) == 1
    fast_rate = jnp.exp(jax.random.uniform(key_fast, (HEADS,), jnp.float32, jnp.log(0.03), jnp.log(0.1)))
    slow_rate = jnp.exp(jax.random.uniform(key_slow, (HEADS,), jnp.float32, jnp.log(0.001), jnp.log(0.01)))
    return jnp.where(fast_heads, fast_rate, slow_rate)


def draw_decay_rate(key, part):
    return head_rates(key).astype(jnp.float32)


def draw_block_decay(key, part):
    decay_rates = head_rates(key)
    sequence_multiplier = jnp.exp(jax.random.uniform(jax.random.fold_in(key, 12), (BATCH_TOTAL, 1, 1), jnp.float32, jnp.log(0.5), jnp.log(2.0)))
    coarse_multiplier = jnp.exp(jax.random.uniform(jax.random.fold_in(key, 13), (BATCH_TOTAL, HEADS, BLOCK_POSITIONS), jnp.float32, jnp.log(0.3), jnp.log(2.0)))
    spike_selector = jax.random.randint(jax.random.fold_in(key, 14), (BATCH_TOTAL, 1, BLOCK_POSITIONS), 0, BLOCK_POSITIONS // 2) == 0
    spike_penalty = jnp.log(jax.random.uniform(jax.random.fold_in(key, 15), (BATCH_TOTAL, 1, BLOCK_POSITIONS), jnp.float32, 0.5, 0.8))
    decay_logarithm = -(decay_rates[None, :, None] * sequence_multiplier * coarse_multiplier) + jnp.where(spike_selector, spike_penalty, 0.0)
    return decay_logarithm.astype(jnp.float32)


def draw_block_keys(key, part):
    key_shared, key_noise = jax.random.split(jax.random.fold_in(key, 21))
    shared_shape = (BATCH_TOTAL, HEADS, 1, HEAD_DIM)
    noise_shape = (BATCH_TOTAL, HEADS, BLOCK_POSITIONS, HEAD_DIM)
    shared = jax.random.normal(key_shared, shared_shape, jnp.float32)
    noise = jax.random.normal(key_noise, noise_shape, jnp.float32)
    raw_keys = 0.6 * shared + 0.8 * noise
    lengths_sq = jnp.sum(raw_keys * raw_keys, axis=3, keepdims=True) + 1e-06
    return (raw_keys / jnp.sqrt(lengths_sq)).astype(jnp.bfloat16)


def draw_tokens(key, part):
    key_rough, key_vals = jax.random.split(key, 2)
    column_ramp = jnp.exp(jnp.log(4.0) * jnp.arange(MODEL, dtype=jnp.float32) / MODEL)
    rough_scale = jnp.exp(jax.random.uniform(key_rough, (MODEL,), jnp.float32, -0.5, 0.5))
    entries = jax.random.normal(key_vals, (BATCH_TOTAL, MODEL), jnp.float32)
    return jnp.clip(entries * column_ramp * rough_scale * 0.6, -16.0, 16.0).astype(jnp.bfloat16)


def block_scale(key, shape, shards, low, top_value):
    level, own = 1.0, jax.random.fold_in(key, 6)
    for dim, shards_of in shards:
        steps = jnp.exp(jax.random.uniform(jax.random.fold_in(own, dim), (shards_of,), jnp.float32, low / len(shards), top_value / len(shards)))
        level = level * jnp.repeat(steps, shape[dim] // shards_of).reshape([-1 if axis == dim else 1 for axis in range(len(shape))])
    return level


def split_up(count, total, reach, lean):
    portions = [(1 << 20) // math.isqrt(grade ** lean) + 1 for grade in range(2, count + 1)]
    rest, counts = total - reach - (count - 1), [1] * (count - 1)
    while rest > 0:
        free = [i for i in range(count - 1) if counts[i] < reach]
        whole, budget = sum([portions[i] for i in free]), rest
        for i in free:
            extra = min(reach - counts[i], max(1, budget * portions[i] // whole), rest)
            counts[i] = counts[i] + extra
            rest = rest - extra
    return np.array([reach] + counts)


def ragged(key, amount, total, most, lean):
    if amount == 2:
        one = jax.random.randint(key, (), max(1, total - most), min(most, total - 1) + 1)
        return jnp.stack([one, total - one])
    sizes = jnp.asarray(split_up(amount, total, most, lean), jnp.int32)
    couples = (amount - 1) // 2
    giver, receiver = sizes[1:1 + 2 * couples:2], sizes[2:2 + 2 * couples:2]
    margin = jnp.minimum(giver - 1, most - receiver)
    moved = jax.random.randint(jax.random.fold_in(key, 1), (couples,), 0, 1 << 20) % (margin + 1)
    sizes = sizes.at[1:1 + 2 * couples:2].set(giver - moved).at[2:2 + 2 * couples:2].set(receiver + moved)
    return sizes[jax.random.permutation(jax.random.fold_in(key, 2), amount)]


def scatter_about(own_key, shape, deviation, bound, pieces=(), held_as=jnp.bfloat16):
    drawn = deviation * jax.random.normal(own_key, shape, jnp.float32)
    if pieces:
        drawn = drawn * block_scale(own_key, shape, pieces, -0.22, 0.18)
    return jnp.clip(drawn, -bound, bound).astype(held_as)


def setup_inputs(seed: int = 0) -> dict:
    key_of = jax.random.split(jax.random.key(seed), 21)
    return {
        "tokens": draw_tokens(jax.random.fold_in(key_of[20], 71), 0),
        "norm_gain": jnp.clip(1.0 + 0.18 * jax.random.normal(key_of[1], (MODEL,), jnp.float32), 0.1, 1.9),
        "query_weight": scatter_about(key_of[2], (MODEL, HEADS * HEAD_DIM), MODEL ** -0.5, 0.125, ((0, 32), (1, 8))),
        "key_weight": scatter_about(key_of[3], (MODEL, HEADS * HEAD_DIM), MODEL ** -0.5, 0.125, ((0, 32), (1, 8))),
        "value_weight": scatter_about(key_of[4], (MODEL, HEADS * HEAD_DIM), MODEL ** -0.5, 0.125, ((0, 32), (1, 8))),
        "gate_weight": scatter_about(key_of[5], (MODEL, HEADS * HEAD_DIM), MODEL ** -0.5, 0.125, ((0, 32), (1, 8))),
        "beta_weight": scatter_about(key_of[6], (MODEL, HEADS), MODEL ** -0.5, 0.125),
        "decay_weight": scatter_about(key_of[7], (MODEL, HEADS), (MODEL // 16) ** -0.5, 0.5),
        "decay_rate": draw_decay_rate(jax.random.fold_in(key_of[20], 71), 0),
        "head_gain": jnp.clip(1.0 + 0.18 * jax.random.normal(key_of[9], (HEAD_DIM,), jnp.float32), 0.1, 1.9),
        "carried_state": scatter_about(key_of[10], (BATCH_TOTAL, HEADS, HEAD_DIM, HEAD_DIM), 0.3, 4.0, ((0, 32), (1, 8)), jnp.float32),
        "block_keys": draw_block_keys(jax.random.fold_in(key_of[20], 71), 0),
        "block_values": scatter_about(key_of[12], (BATCH_TOTAL, HEADS, BLOCK_POSITIONS, HEAD_DIM), 1.0, 6.0, ((0, 32), (1, 8))),
        "block_beta": jnp.clip(0.1 + 0.79999997 * jax.random.uniform(key_of[13], (BATCH_TOTAL, HEADS, BLOCK_POSITIONS), jnp.float32) ** block_scale(key_of[13], (BATCH_TOTAL, HEADS, BLOCK_POSITIONS), ((0, 32), (1, 8)), -0.2, 0.2), 0.1, 0.9),
        "block_decay": draw_block_decay(jax.random.fold_in(key_of[20], 71), 0),
        "live_count": ragged(key_of[15], BATCH_TOTAL, BATCH_TOTAL * BLOCK_POSITIONS * 2 // 5, BLOCK_POSITIONS, 2).astype(jnp.int32),
        "out_weight": scatter_about(key_of[16], (HEADS * HEAD_DIM, MODEL), (HEADS * HEAD_DIM) ** -0.5, 0.125, ((0, 8), (1, 32))),
        "mlp_gain": jnp.clip(1.0 + 0.18 * jax.random.normal(key_of[17], (MODEL,), jnp.float32), 0.1, 1.9),
        "up_weight": scatter_about(key_of[18], (MODEL, MLP_UNITS), MODEL ** -0.5, 0.125, ((0, 32), (1, 8))),
        "down_weight": scatter_about(key_of[19], (MLP_UNITS, MODEL), MLP_UNITS ** -0.5, 0.0625, ((0, 8), (1, 32))),
    }


EPS = 1e-06
PRECISE = lax.Precision.HIGHEST

def unit_inverse(strict_lower):
    slots_count = strict_lower.shape[-1]
    identity = jnp.eye(slots_count, dtype=strict_lower.dtype)
    powered = -strict_lower
    product_sum = identity + powered
    for repeat in range(slots_count.bit_length() - 2):
        powered = jnp.matmul(powered, powered, precision=PRECISE)
        product_sum = product_sum + jnp.matmul(product_sum, powered, precision=PRECISE)
    return product_sum

def delta_block(queries, key_new, value_new, beta_new, decay_new, keys, values, betas, decays, live_count, carried_state):
    slots_count = keys.shape[2]
    slot_ids = jnp.arange(slots_count, dtype=jnp.int32)
    newest = (live_count.astype(jnp.int32) - 1)[:, None, None]
    pending = slot_ids[None, None, :] < newest
    current = slot_ids[None, None, :] == newest
    keys_all = jnp.where(pending[..., None], keys, jnp.where(current[..., None], key_new[:, :, None, :], jnp.zeros_like(keys)))
    values_all = jnp.where(pending[..., None], values, jnp.where(current[..., None], value_new[:, :, None, :], jnp.zeros_like(values)))
    betas_all = jnp.where(pending, betas, jnp.where(current, beta_new[:, :, None], 0.0))
    decays_all = jnp.where(pending, decays, jnp.where(current, decay_new[:, :, None], 0.0))
    totals = jnp.cumsum(decays_all, axis=2)
    strict = slot_ids[:, None] > slot_ids[None, :]
    spread = jnp.where(strict, totals[..., :, None] - totals[..., None, :], 0.0)
    key_vals = keys_all.astype(jnp.float32)
    intersection = jnp.einsum('shid,shjd->shij', key_vals, key_vals, precision=PRECISE)
    strict_lower = jnp.where(strict, betas_all[..., :, None] * intersection * jnp.exp(spread), 0.0)
    inverse = unit_inverse(strict_lower)
    right_values = betas_all[..., None] * values_all.astype(jnp.float32)
    right_keys = (betas_all * jnp.exp(totals))[..., None] * key_vals
    solved_values = jnp.einsum('shij,shjv->shiv', inverse, right_values, precision=PRECISE)
    solved_keys = jnp.einsum('shij,shjk->shik', inverse, right_keys, precision=PRECISE)
    update = solved_values - jnp.einsum('shik,shkv->shiv', solved_keys, carried_state, precision=PRECISE)
    ending = totals[..., -1]
    faded_keys = key_vals * jnp.exp(ending[..., None] - totals)[..., None]
    new_state = jnp.exp(ending)[..., None, None] * carried_state + jnp.einsum('shik,shiv->shkv', faded_keys, update, precision=PRECISE)
    readout = jnp.einsum('shk,shkv->shv', queries, new_state, precision=PRECISE)
    return (readout, new_state)

def reference(tokens, norm_gain, query_weight, key_weight, value_weight, gate_weight, beta_weight, decay_weight, decay_rate, head_gain, carried_state, block_keys, block_values, block_beta, block_decay, live_count, out_weight, mlp_gain, up_weight, down_weight):
    token_vals = tokens.astype(jnp.float32)
    inverse_rms = lax.rsqrt(lax.optimization_barrier(jnp.mean(token_vals * token_vals, axis=1)) + EPS)[:, None]
    normed = (token_vals * norm_gain).astype(jnp.bfloat16)

    def project(weight):
        return jnp.dot(normed, weight, preferred_element_type=jnp.float32) * inverse_rms
    queries = project(query_weight).reshape(BATCH_TOTAL, HEADS, HEAD_DIM)
    key_raw = project(key_weight).reshape(BATCH_TOTAL, HEADS, HEAD_DIM)
    value_raw = project(value_weight).reshape(BATCH_TOTAL, HEADS, HEAD_DIM)
    gate_raw = project(gate_weight).reshape(BATCH_TOTAL, HEADS, HEAD_DIM)
    beta_new = jax.nn.sigmoid(project(beta_weight))
    decay_new = -decay_rate * jax.nn.softplus(project(decay_weight))
    key_new = (key_raw * lax.rsqrt(lax.optimization_barrier(jnp.sum(key_raw * key_raw, axis=2, keepdims=True)) + EPS)).astype(jnp.bfloat16)
    value_new = value_raw.astype(jnp.bfloat16)

    def grouped(array):
        return array.reshape((N_KV, SEQ_DEV) + array.shape[1:])
    grouped_args = tuple((grouped(item) for item in (queries, key_new, value_new, beta_new, decay_new, block_keys, block_values, block_beta, block_decay, live_count, carried_state)))
    readout, new_state = lax.map(lambda member: delta_block(*member), grouped_args)
    readout = readout.reshape(BATCH_TOTAL, HEADS, HEAD_DIM)
    new_state = new_state.reshape(BATCH_TOTAL, HEADS, HEAD_DIM, HEAD_DIM)
    scaled = readout * lax.rsqrt(lax.optimization_barrier(jnp.mean(readout * readout, axis=2, keepdims=True)) + EPS) * head_gain
    mixed_heads = (scaled * jax.nn.silu(gate_raw)).reshape(BATCH_TOTAL, HEADS * HEAD_DIM).astype(jnp.bfloat16)
    heads_dev = HEADS // N_TP
    blocks_in = mixed_heads.reshape(BATCH_TOTAL, N_TP, heads_dev * HEAD_DIM).astype(jnp.float32)
    blocks_weight = out_weight.reshape(N_TP, heads_dev * HEAD_DIM, MODEL).astype(jnp.float32)
    partial_value = jnp.einsum('btj,tjd->tbd', blocks_in, blocks_weight, precision=PRECISE)
    partial_value = lax.optimization_barrier(partial_value.astype(jnp.bfloat16)).astype(jnp.float32)
    attended = lax.optimization_barrier(jnp.sum(partial_value, axis=0))
    residual = lax.optimization_barrier((token_vals + attended).astype(jnp.bfloat16))
    resid_vals = residual.astype(jnp.float32)
    mlp_rms = lax.rsqrt(lax.optimization_barrier(jnp.mean(resid_vals * resid_vals, axis=1)) + EPS)[:, None]
    mlp_in = (resid_vals * mlp_gain).astype(jnp.bfloat16)
    pre_act = jnp.dot(mlp_in, up_weight, preferred_element_type=jnp.float32) * mlp_rms
    hidden = jnp.square(jax.nn.relu(pre_act)).astype(jnp.bfloat16)
    mixed = (resid_vals + jnp.dot(hidden, down_weight, preferred_element_type=jnp.float32)).astype(jnp.bfloat16)
    return (mixed, new_state)
```

```python
import functools

import jax
import jax.numpy as jnp
from jax import lax
from jax.experimental import pallas as pl
from jax.experimental.pallas import tpu as pltpu
from jax.sharding import PartitionSpec as P

MODEL = 2048
HEADS = 16
EPS = 1e-06
NX = 4
F32 = jnp.float32
BF16 = jnp.bfloat16


def dot(a, b):
    return jnp.dot(a, b, preferred_element_type=F32)


def split(a):
    high = a.astype(BF16)
    return high, (a - high.astype(F32)).astype(BF16)


def dot3(a, b):
    ah, al = split(a)
    bh, bl = split(b)
    return dot(ah, bh) + (dot(ah, bl) + dot(al, bh))


def dot2(a, b):
    bh, bl = split(b)
    return dot(a, bh) + dot(a, bl)


def iota(shape, dim):
    return lax.broadcasted_iota(jnp.int32, shape, dim)


def unit_inverse(lower, r, c):
    def same(bits):
        return (r >> bits) == (c >> bits)

    ident = jnp.where(r == c, 1.0, 0.0)
    power = jnp.where(same(3), -lower, 0.0)
    total = ident + power
    for _ in range(2):
        power = dot3(power, power)
        total = total + dot3(total, power)
    for bits in (3, 4, 5):
        off = jnp.where(same(bits + 1) & jnp.logical_not(same(bits)), lower, 0.0)
        total = total - dot3(total, dot3(off, total))
    return total


def state_before(g, keys, vals, state, bbeta, bdecay, live):
    r = iota((256, 256), 0)
    c = iota((256, 256), 1)
    same = (r >> 6) == (c >> 6)
    n0, n1 = live[2 * g] - 1, live[2 * g + 1] - 1
    lane = iota((1, 256), 1)
    live_row = (lane & 63) < jnp.where(lane < 128, n0, n1)
    d_row = jnp.where(live_row, bdecay[g], 0.0)
    b_row = jnp.where(live_row, bbeta[g], 0.0)
    r1 = iota((256, 128), 0)
    live_col = (r1 & 63) < jnp.where(r1 < 128, n0, n1)
    k_all = jnp.where(live_col, keys[pl.ds(2 * g, 2)].astype(F32).reshape(256, 128), 0.0)
    v_all = jnp.where(live_col, vals[pl.ds(2 * g, 2)].astype(F32).reshape(256, 128), 0.0)
    d_col = jnp.sum(jnp.where(r == c, d_row, 0.0), axis=1, keepdims=True)
    b_col = jnp.sum(jnp.where(r == c, b_row, 0.0), axis=1, keepdims=True)
    tot_col = jnp.sum(jnp.where(same & (c <= r), d_row, 0.0), axis=1, keepdims=True)
    tot_row = jnp.sum(jnp.where(same & (r <= c), d_col, 0.0), axis=0, keepdims=True)
    end_col = jnp.sum(jnp.where(same, d_row, 0.0), axis=1, keepdims=True)
    kb = k_all.astype(BF16)
    kt = k_all.T.astype(BF16)
    strict = same & (c < r)
    fade = jnp.exp(jnp.where(strict, tot_col - tot_row, 0.0))
    lower = jnp.where(strict, b_col * dot(kb, kt) * fade, 0.0)
    inverse = unit_inverse(lower, r, c)
    old = jnp.concatenate([state[2 * g + p // 2, p % 2] for p in range(4)], axis=1)
    seen = dot2(kb, old)
    seen = jnp.concatenate(
        [seen[64 * p : 64 * p + 64, 128 * p : 128 * p + 128] for p in range(4)], axis=0
    )
    right = b_col * (v_all - jnp.exp(tot_col) * seen)
    update = dot3(inverse, right) * jnp.exp(end_col - tot_col)
    r4 = iota((256, 512), 0)
    c4 = iota((256, 512), 1)
    wide = jnp.concatenate([update] * 4, axis=1)
    wide = jnp.where((r4 >> 6) == (c4 >> 7), wide, 0.0)
    added = dot2(kt, wide)
    for p in range(4):
        end = jnp.exp(end_col[64 * p : 64 * p + 1, :])
        at = slice(128 * p, 128 * p + 128)
        state[2 * g + p // 2, p % 2] = end * old[:, at] + added[:, at]


def halves(a):
    n = a.shape[0] // 2
    return jnp.concatenate([a[:n], a[n:]], axis=1)


def folded(a, blocks):
    n = a.shape[0] // 2
    return [
        a[:n, 128 * b : 128 * b + 64] + a[n:, 128 * b + 64 : 128 * b + 128] for b in range(blocks)
    ]


def kernel(
    tok_ref,
    ngain_ref,
    qw_hbm,
    kw_hbm,
    vw_hbm,
    gw_hbm,
    bw_hbm,
    dw_hbm,
    rate_ref,
    hgain_ref,
    state_hbm,
    keys_hbm,
    vals_hbm,
    bbeta_ref,
    bdecay_ref,
    live_ref,
    out_hbm,
    mgain_ref,
    up_hbm,
    down_hbm,
    mixed_ref,
    nstate_hbm,
    wst,
    wcat,
    bwv,
    dwv,
    tokp,
    gp,
    tokt,
    proj_s,
    proj_r,
    ex_s,
    ex_r,
    keys,
    vals,
    state,
    up_all,
    down_all,
    out_all,
    down_tmp,
    out_tmp,
    bbeta,
    bdecay,
    mh,
    ar,
    ax,
    rs_s,
    rs_r,
    resid,
    fin_s,
    mx,
    loc,
    xs,
    xr,
    ts,
    tr,
    ps,
    pr,
    ms,
    mr,
    asem,
    arr,
    us,
    ur,
    ds_,
    dr,
    fs,
    fr,
    ring_s,
    ring_r,
    *,
    n_kv,
    n_tp,
):
    kv = lax.axis_index("kv")
    tp = lax.axis_index("tp")
    nz = n_kv // NX
    z = kv // NX
    x = kv % NX

    def local(src, dst, i):
        copy = pltpu.make_async_copy(src, dst, loc.at[i])
        copy.start()
        return copy

    def remote(src, dst, s, r, kv_to, tp_to):
        return pltpu.make_async_remote_copy(
            src_ref=src,
            dst_ref=dst,
            send_sem=s,
            recv_sem=r,
            device_id={"kv": kv_to, "tp": tp_to},
            device_id_type=pl.DeviceIdType.MESH,
        )

    in_w = [local(w, wst.at[i], i) for i, w in enumerate((qw_hbm, kw_hbm, vw_hbm, gw_hbm))]
    rows = pl.ds(pl.multiple_of(z * 256, 256), 256)
    in_b = [local(bw_hbm.at[rows], bwv, 4), local(dw_hbm.at[rows], dwv, 5)]
    in_out = local(out_hbm, out_tmp, 6)
    in_up = local(up_hbm, up_all.at[z], 7)
    in_down = local(down_hbm, down_tmp, 8)
    in_keys = local(keys_hbm, keys, 9)
    in_vals = local(vals_hbm, vals, 10)
    in_state = local(state_hbm, state, 11)

    barrier = pltpu.get_barrier_semaphore()

    def greet_kv(d, carry):
        pl.semaphore_signal(
            barrier,
            inc=1,
            device_id={"kv": (kv + d) % n_kv, "tp": tp},
            device_id_type=pl.DeviceIdType.MESH,
        )
        return carry

    def greet_tp(d, carry):
        pl.semaphore_signal(
            barrier,
            inc=1,
            device_id={"kv": kv, "tp": (tp + d) % n_tp},
            device_id_type=pl.DeviceIdType.MESH,
        )
        return carry

    lax.fori_loop(1, n_kv, greet_kv, 0)
    lax.fori_loop(1, n_tp, greet_tp, 0)

    tokp[x] = halves(tok_ref[...].astype(F32)).astype(BF16)
    gp[x] = jnp.concatenate([ngain_ref[...], ngain_ref[...]], axis=1)
    for i in range(4):
        bbeta[i] = jnp.concatenate([bbeta_ref[2 * i + j // 2, j % 2 : j % 2 + 1] for j in range(4)], axis=1)
        bdecay[i] = jnp.concatenate([bdecay_ref[2 * i + j // 2, j % 2 : j % 2 + 1] for j in range(4)], axis=1)
    for copy in in_b:
        copy.wait()
    wcat[:, 256:384] = jnp.concatenate(
        [bwv[...].astype(F32), dwv[...].astype(F32), jnp.zeros((256, 96), F32)], axis=1
    ).astype(BF16)
    for copy in in_w:
        copy.wait()
    wcat[pl.ds(pl.multiple_of(x * 64, 64), 64), 0:256] = wst[x]
    in_out.wait()
    lane_z = pl.ds(pl.multiple_of(z * 128, 128), 128)
    out_all[:, lane_z] = halves(out_tmp[...].astype(F32)).astype(BF16)
    in_up.wait()
    in_down.wait()
    down_all[:, lane_z] = halves(down_tmp[...].astype(F32)).astype(BF16)
    tokt[z] = tok_ref[pl.ds(pl.multiple_of(z * 32, 32), 32), :]

    pl.semaphore_wait(barrier, n_kv - 1 + n_tp - 1)

    mine = pl.ds(pl.multiple_of(x * 64, 64), 64)
    sent_x = []
    for d in range(1, NX):
        to = (x + d) % NX
        peer = z * NX + to
        sent_x.append(remote(tokp.at[x], tokp.at[x], xs.at[0, d], xr.at[0, d], peer, tp))
        sent_x.append(remote(gp.at[x], gp.at[x], xs.at[1, d], xr.at[1, d], peer, tp))
        sent_x.append(
            remote(wst.at[to], wcat.at[mine, pl.ds(0, 256)], xs.at[2, d], xr.at[2, d], peer, tp)
        )
    for copy in sent_x:
        copy.start()

    sent_t = []
    for d in range(1, nz):
        to = (z + d) % nz
        sent_t.append(
            remote(
                tok_ref.at[pl.ds(pl.multiple_of(to * 32, 32), 32), :],
                tokt.at[z],
                ts.at[d],
                tr.at[d],
                to * NX + x,
                tp,
            )
        )
    for copy in sent_t:
        copy.start()

    def ring(way, step, what):
        to = (z + 1) % nz if way == 0 else (z + nz - 1) % nz
        block = (z + nz - (step - 1)) % nz if way == 0 else (z + step - 1) % nz
        lanes = pl.ds(pl.multiple_of(block * 128, 128), 128)
        ref = (out_all.at[:, lanes], up_all.at[block], down_all.at[:, lanes])[what]
        return remote(
            ref, ref, ring_s.at[way, step - 1, what], ring_r.at[way, step - 1, what], to * NX + x, tp
        )

    half = nz // 2
    plan = {}
    for step in range(1, half + 1):
        plan[step] = [
            (way, what)
            for what in range(3)
            for way in range(2)
            if step < half or way == (1 if what == 2 else 0)
        ]

    def ring_start(step):
        for way, what in plan[step]:
            ring(way, step, what).start()

    def ring_pass(step):
        for way, what in plan[step]:
            ring(way, step, what).wait_recv()
            if step < half and (way, what) in plan[step + 1]:
                ring(way, step + 1, what).start()

    ring_start(1)

    in_keys.wait()
    in_vals.wait()
    in_state.wait()

    def before(g, carry):
        state_before(g, keys, vals, state, bbeta, bdecay, live_ref)
        return carry

    lax.fori_loop(0, 2, before, 0)

    for copy in sent_x:
        copy.wait_recv()
    parts, squares = [], jnp.zeros((128, 128), F32)
    for i in range(NX):
        t = tokp[i].astype(F32)
        squares = squares + t * t
        parts.append(t * gp[i])
    tops = jnp.concatenate([p[:, :64] for p in parts], axis=1)
    bottoms = jnp.concatenate([p[:, 64:] for p in parts], axis=1)
    normed = jnp.concatenate([tops, bottoms], axis=0).astype(BF16)
    squares = jnp.concatenate(
        [
            jnp.sum(squares[:, :64], axis=1, keepdims=True),
            jnp.sum(squares[:, 64:], axis=1, keepdims=True),
        ],
        axis=0,
    )
    projected = dot(normed, wcat[...])
    proj_s[...] = projected[:, :256].reshape(n_kv, 8, 256).astype(BF16)
    lane = iota((256, 128), 1)
    high = squares.astype(BF16).astype(F32)
    extra = projected[:, 256:384]
    extra = jnp.where(lane == 32, high, jnp.where(lane == 33, squares - high, extra))
    ex_s[...] = extra.reshape(n_kv, 8, 128).astype(BF16)
    proj_r[kv] = proj_s[kv]
    ex_r[z] = ex_s[kv]

    def send_proj(d, carry):
        to = (kv + d) % n_kv
        remote(proj_s.at[to], proj_r.at[kv], ps.at[0], pr.at[0], to, tp).start()
        return carry

    def send_extra(d, carry):
        to = ((z + d) % nz) * NX + x
        remote(ex_s.at[to], ex_r.at[z], ps.at[1], pr.at[1], to, tp).start()
        return carry

    lax.fori_loop(1, nz, send_extra, 0)
    lax.fori_loop(1, n_kv, send_proj, 0)

    ring_pass(1)
    lax.fori_loop(2, 4, before, 0)

    some = pl.ds(0, n_kv - 1)
    few = pl.ds(0, nz - 1)
    all_proj = remote(proj_s.at[some], proj_r.at[some], ps.at[0], pr.at[0], kv, tp)
    all_extra = remote(ex_s.at[few], ex_r.at[few], ps.at[1], pr.at[1], kv, tp)
    all_extra.wait_recv()
    all_proj.wait_recv()

    total = jnp.sum(proj_r[...].astype(F32).reshape(nz, NX, 8, 256), axis=0)
    extra = jnp.sum(ex_r[...].astype(F32), axis=0)
    inverse_rms = lax.rsqrt((extra[:, 32:33] + extra[:, 33:34]) / MODEL + EPS)
    extra = extra * inverse_rms
    queries, key_raw, value_raw, gate_raw = [total[i] * inverse_rms for i in range(4)]
    lane = iota((8, 128), 1)
    cols, heads = [], []
    for h in range(2):
        at = slice(128 * h, 128 * h + 128)
        k = key_raw[:, at]
        k = k * lax.rsqrt(jnp.sum(k * k, axis=1, keepdims=True) + EPS)
        k = k.astype(BF16).astype(F32)
        v = value_raw[:, at].astype(BF16).astype(F32)
        q = queries[:, at]
        b = jnp.sum(jnp.where(lane == 2 * tp + h, extra, 0.0), axis=1, keepdims=True)
        b = 1.0 / (1.0 + jnp.exp(-b))
        a = jnp.sum(jnp.where(lane == HEADS + 2 * tp + h, extra, 0.0), axis=1, keepdims=True)
        a = jnp.maximum(a, 0.0) + jnp.log1p(jnp.exp(-jnp.abs(a)))
        e = jnp.exp(-rate_ref[h] * a)
        qk = jnp.sum(q * k, axis=1, keepdims=True)
        cols += [k, q]
        heads.append((k, v, q, b, e, qk))
    columns = jnp.concatenate(cols + [jnp.zeros((96, 128), F32)], axis=0).T
    updates, readouts = {}, []
    for h in range(2):
        k, v, q, b, e, qk = heads[h]
        lines = []
        for s in range(8):
            old = state[s, h]
            one = slice(s, s + 1)
            kcol = columns[:, 16 * h + s : 16 * h + s + 1]
            qcol = columns[:, 16 * h + 8 + s : 16 * h + 9 + s]
            ks = jnp.sum(old * kcol, axis=0, keepdims=True)
            qs = jnp.sum(old * qcol, axis=0, keepdims=True)
            u = b[one] * (v[one] - e[one] * ks)
            updates[s, h] = u
            lines.append(e[one] * qs + qk[one] * u)
        readouts.append(jnp.concatenate(lines, axis=0))
    gated = []
    for h in range(2):
        rd = readouts[h]
        gate = gate_raw[:, 128 * h : 128 * h + 128]
        scaled = rd * lax.rsqrt(jnp.sum(rd * rd, axis=1, keepdims=True) / 128 + EPS) * hgain_ref[...]
        gated.append(scaled * (gate / (1.0 + jnp.exp(-gate))))
    mh[x] = jnp.concatenate(gated, axis=1).astype(BF16).astype(F32)
    sent_m = []
    for d in range(1, NX):
        peer = z * NX + (x + d) % NX
        sent_m.append(remote(mh.at[x], mh.at[x], ms.at[d], mr.at[d], peer, tp))
    for copy in sent_m:
        copy.start()
    ring_pass(2)

    for h in range(2):
        e = heads[h][4]
        for s in range(8):
            kcol = columns[:, 16 * h + s : 16 * h + s + 1]
            state[s, h] = e[s : s + 1] * state[s, h] + kcol * updates[s, h]
    put_state = local(state, nstate_hbm, 0)
    ring_pass(3)

    for copy in sent_m:
        copy.wait_recv()
    ring_pass(4)
    m = mh[...].reshape(32, 256)
    m = jnp.concatenate([m[:, :128], m[:, 128:]], axis=0).astype(BF16)
    blocks = folded(dot(m, out_all[...]), nz)
    ar[tp] = jnp.concatenate(blocks, axis=1).astype(BF16)

    def send_ar(d, carry):
        to = (tp + d) % n_tp
        remote(ar.at[tp], ar.at[tp], asem, arr, kv, to).start()
        return carry

    lax.fori_loop(1, n_tp, send_ar, 0)
    tps = pl.ds(0, n_tp - 1)
    all_ar = remote(ar.at[tps], ar.at[tps], asem, arr, kv, tp)
    for copy in sent_t:
        copy.wait_recv()
    tokens = jnp.concatenate([tokt[i].astype(F32) for i in range(nz)], axis=1)
    gains = []
    for p in range(nz):
        gain = mgain_ref[pl.ds(2 * p + x // 2, 1), :]
        gains.append(jnp.where(x % 2 == 0, gain[:, :64], gain[:, 64:]))
    gains = jnp.concatenate(gains, axis=1)
    all_ar.wait_recv()

    attended = jnp.sum(ar[...].astype(F32), axis=0)
    residual = (tokens + attended).astype(BF16).astype(F32)
    for i in range(nz):
        resid[i] = residual[:, 64 * i : 64 * i + 64]
    squares = jnp.sum(residual * residual, axis=1, keepdims=True)
    mlp_in = (residual * gains).astype(BF16)
    pre = dot(mlp_in, up_all[...].reshape(nz * 64, 1024))
    high = squares.astype(BF16).astype(F32)
    lane = iota((32, 128), 1)
    tail = jnp.where(lane == 0, high, jnp.where(lane == 1, squares - high, 0.0))
    ax[x] = jnp.concatenate([pre, tail], axis=1).astype(BF16)
    sent_u = []
    for d in range(1, NX):
        peer = z * NX + (x + d) % NX
        sent_u.append(remote(ax.at[x], ax.at[x], us.at[d], ur.at[d], peer, tp))
    for copy in sent_u:
        copy.start()
    for copy in sent_u:
        copy.wait_recv()
    total = jnp.sum(ax[...].astype(F32), axis=0)
    rms = lax.rsqrt((total[:, 1024:1025] + total[:, 1025:1026]) / MODEL + EPS)
    hidden = jnp.maximum(total[:, :1024] * rms, 0.0)
    hidden = (hidden * hidden).astype(BF16)
    hidden = jnp.concatenate([hidden[:, :512], hidden[:, 512:]], axis=0)
    blocks = folded(dot(hidden, down_all[...]), nz)
    for i in range(nz):
        rs_s[i] = blocks[i].astype(BF16)
    rs_r[tp] = rs_s[tp]

    def send_rs(d, carry):
        to = (tp + d) % n_tp
        remote(rs_s.at[to], rs_r.at[tp], ds_, dr, kv, to).start()
        return carry

    lax.fori_loop(1, n_tp, send_rs, 0)
    all_rs = remote(rs_s.at[tps], rs_r.at[tps], ds_, dr, kv, tp)
    all_rs.wait_recv()
    fin_s[...] = (resid[tp] + jnp.sum(rs_r[...].astype(F32), axis=0)).astype(BF16)

    at_home = z == tp
    far = tp * NX + x

    def send_fin(t, carry):
        @pl.when(jnp.logical_or(jnp.logical_not(at_home), t != tp))
        def _():
            remote(fin_s, mx.at[z], fs, fr, far, t).start()

        return carry

    @pl.when(at_home)
    def _():
        mx[z] = fin_s[...]

    lax.fori_loop(0, n_tp, send_fin, 0)

    put_state.wait()
    for copy in sent_x + sent_t + sent_m + sent_u:
        copy.wait_send()
    for step in plan:
        for way, what in plan[step]:
            ring(way, step, what).wait_send()
    all_proj.wait_send()
    all_extra.wait_send()
    all_ar.wait_send()
    all_rs.wait_send()

    eight = remote(mx, mx, fs, fr, kv, tp)
    seven = remote(mx.at[few], mx.at[few], fs, fr, kv, tp)

    @pl.when(at_home)
    def _():
        seven.wait_recv()
        seven.wait_send()

    @pl.when(jnp.logical_not(at_home))
    def _():
        eight.wait_recv()
        eight.wait_send()

    for i in range(nz):
        mixed_ref[32 * i : 32 * i + 32, :] = mx[i]


def body(
    tokens,
    norm_gain,
    query_weight,
    key_weight,
    value_weight,
    gate_weight,
    beta_weight,
    decay_weight,
    decay_rate,
    head_gain,
    carried_state,
    block_keys,
    block_values,
    block_beta,
    block_decay,
    live_count,
    out_weight,
    mlp_gain,
    up_weight,
    down_weight,
):
    n_kv = lax.axis_size("kv")
    n_tp = lax.axis_size("tp")
    nz = n_kv // NX
    vmem = pl.BlockSpec(memory_space=pltpu.VMEM)
    smem = pl.BlockSpec(memory_space=pltpu.SMEM)
    hbm = pl.BlockSpec(memory_space=pl.ANY)
    dma = pltpu.SemaphoreType.DMA
    return pl.pallas_call(
        functools.partial(kernel, n_kv=n_kv, n_tp=n_tp),
        out_shape=(
            jax.ShapeDtypeStruct(tokens.shape, BF16),
            jax.ShapeDtypeStruct(carried_state.shape, F32),
        ),
        in_specs=[vmem, vmem, hbm, hbm, hbm, hbm, hbm, hbm, smem, vmem, hbm, hbm, hbm, vmem, vmem, smem, hbm, vmem, hbm, hbm],
        out_specs=(vmem, hbm),
        scratch_shapes=[
            pltpu.VMEM((4, 64, 256), BF16),
            pltpu.VMEM((256, 384), BF16),
            pltpu.VMEM((256, 16), BF16),
            pltpu.VMEM((256, 16), BF16),
            pltpu.VMEM((NX, 128, 128), BF16),
            pltpu.VMEM((NX, 1, 128), F32),
            pltpu.VMEM((nz, 32, 64), BF16),
            pltpu.VMEM((n_kv, 8, 256), BF16),
            pltpu.VMEM((n_kv, 8, 256), BF16),
            pltpu.VMEM((n_kv, 8, 128), BF16),
            pltpu.VMEM((nz, 8, 128), BF16),
            pltpu.VMEM((8, 2, 64, 128), BF16),
            pltpu.VMEM((8, 2, 64, 128), BF16),
            pltpu.VMEM((8, 2, 128, 128), F32),
            pltpu.VMEM((nz, 64, 1024), BF16),
            pltpu.VMEM((512, 128 * nz), BF16),
            pltpu.VMEM((128, 128 * nz), BF16),
            pltpu.VMEM((1024, 64), BF16),
            pltpu.VMEM((256, 64), BF16),
            pltpu.VMEM((4, 1, 256), F32),
            pltpu.VMEM((4, 1, 256), F32),
            pltpu.VMEM((NX, 8, 256), F32),
            pltpu.VMEM((n_tp, 32, 512), BF16),
            pltpu.VMEM((NX, 32, 1152), BF16),
            pltpu.VMEM((n_tp, 32, 64), BF16),
            pltpu.VMEM((n_tp, 32, 64), BF16),
            pltpu.VMEM((nz, 32, 64), F32),
            pltpu.VMEM((32, 64), BF16),
            pltpu.VMEM((nz, 32, 64), BF16),
            dma((12,)),
            dma((3, NX)),
            dma((3, NX)),
            dma((nz,)),
            dma((nz,)),
            dma((2,)),
            dma((2,)),
            dma((NX,)),
            dma((NX,)),
            dma,
            dma,
            dma((NX,)),
            dma((NX,)),
            dma,
            dma,
            dma,
            dma,
            dma((2, 4, 3)),
            dma((2, 4, 3)),
        ],
        compiler_params=pltpu.CompilerParams(
            collective_id=0, has_side_effects=True, vmem_limit_bytes=48 * 1024 * 1024
        ),
        name="layer",
    )(
        tokens,
        norm_gain.reshape(1, -1),
        query_weight,
        key_weight,
        value_weight,
        gate_weight,
        beta_weight,
        decay_weight,
        decay_rate,
        head_gain.reshape(1, -1),
        carried_state,
        block_keys,
        block_values,
        block_beta,
        block_decay,
        live_count,
        out_weight,
        mlp_gain.reshape(-1, 128),
        up_weight,
        down_weight,
    )


def solution(mesh):
    placed = (
        P(None, "kv"),
        P("kv"),
        P("kv", "tp"),
        P("kv", "tp"),
        P("kv", "tp"),
        P("kv", "tp"),
        P(),
        P(),
        P("tp"),
        P(),
        P("kv", "tp", None, None),
        P("kv", "tp", None, None),
        P("kv", "tp", None, None),
        P("kv", "tp", None),
        P("kv", "tp", None),
        P("kv"),
        P("tp", "kv"),
        P(),
        P("kv", "tp"),
        P("tp", "kv"),
    )
    return jax.shard_map(
        body,
        mesh=mesh,
        in_specs=placed,
        out_specs=(P(None, "kv"), P("kv", "tp", None, None)),
        check_vma=False,
    )
```

```python
import functools

import jax
import jax.numpy as jnp
from jax import lax
from jax.experimental import pallas as pl
from jax.experimental.pallas import tpu as pltpu
from jax.sharding import PartitionSpec as P

MODEL = 2048
HEADS = 16
EPS = 1e-06
NX = 4
F32 = jnp.float32
BF16 = jnp.bfloat16


def dot(a, b):
    return jnp.dot(a, b, preferred_element_type=F32)


def split(a):
    high = a.astype(BF16)
    return high, (a - high.astype(F32)).astype(BF16)


def dot_nt(a, b):
    return lax.dot_general(a, b, (((1,), (1,)), ((), ())), preferred_element_type=F32)


def dot3(a, b):
    ah, al = split(a)
    bh, bl = split(b)
    return dot(ah, bh) + (dot(ah, bl) + dot(al, bh))


def dot2(a, b):
    bh, bl = split(b)
    return dot(a, bh) + dot(a, bl)


def iota(shape, dim):
    return lax.broadcasted_iota(jnp.int32, shape, dim)


def unit_inverse(lower, r, c):
    def same(bits):
        return (r >> bits) == (c >> bits)

    ident = jnp.where(r == c, 1.0, 0.0)
    power = jnp.where(same(3), -lower, 0.0)
    total = ident + power
    for _ in range(2):
        power = dot3(power, power)
        total = total + dot3(total, power)
    for bits in (3, 4, 5):
        off = jnp.where(same(bits + 1) & jnp.logical_not(same(bits)), lower, 0.0)
        total = total - dot3(total, dot3(off, total))
    return total


def state_before(g, keys, vals, state, bbeta, bdecay, live):
    r = iota((256, 256), 0)
    c = iota((256, 256), 1)
    same = (r >> 6) == (c >> 6)
    n0, n1 = live[2 * g] - 1, live[2 * g + 1] - 1
    lane = iota((1, 256), 1)
    live_row = (lane & 63) < jnp.where(lane < 128, n0, n1)
    d_row = jnp.where(live_row, bdecay[g], 0.0)
    b_row = jnp.where(live_row, bbeta[g], 0.0)
    r1 = iota((256, 128), 0)
    live_col = (r1 & 63) < jnp.where(r1 < 128, n0, n1)
    k_all = jnp.where(live_col, keys[pl.ds(2 * g, 2)].astype(F32).reshape(256, 128), 0.0)
    v_all = jnp.where(live_col, vals[pl.ds(2 * g, 2)].astype(F32).reshape(256, 128), 0.0)
    d_col = jnp.sum(jnp.where(r == c, d_row, 0.0), axis=1, keepdims=True)
    b_col = jnp.sum(jnp.where(r == c, b_row, 0.0), axis=1, keepdims=True)
    tot_col = jnp.sum(jnp.where(same & (c <= r), d_row, 0.0), axis=1, keepdims=True)
    tot_row = jnp.sum(jnp.where(same & (r <= c), d_col, 0.0), axis=0, keepdims=True)
    end_col = jnp.sum(jnp.where(same, d_row, 0.0), axis=1, keepdims=True)
    kb = k_all.astype(BF16)
    kt = k_all.T.astype(BF16)
    strict = same & (c < r)
    fade = jnp.exp(jnp.where(strict, tot_col - tot_row, 0.0))
    lower = jnp.where(strict, b_col * dot(kb, kt) * fade, 0.0)
    inverse = unit_inverse(lower, r, c)
    old = jnp.concatenate([state[2 * g + p // 2, p % 2] for p in range(4)], axis=1)
    seen = dot2(kb, old)
    seen = jnp.concatenate(
        [seen[64 * p : 64 * p + 64, 128 * p : 128 * p + 128] for p in range(4)], axis=0
    )
    right = b_col * (v_all - jnp.exp(tot_col) * seen)
    update = dot3(inverse, right) * jnp.exp(end_col - tot_col)
    r4 = iota((256, 512), 0)
    c4 = iota((256, 512), 1)
    wide = jnp.concatenate([update] * 4, axis=1)
    wide = jnp.where((r4 >> 6) == (c4 >> 7), wide, 0.0)
    added = dot2(kt, wide)
    for p in range(4):
        end = jnp.exp(end_col[64 * p : 64 * p + 1, :])
        at = slice(128 * p, 128 * p + 128)
        state[2 * g + p // 2, p % 2] = end * old[:, at] + added[:, at]


def kernel(
    tok_hbm,
    ngain_hbm,
    qw_hbm,
    kw_hbm,
    vw_hbm,
    gw_hbm,
    bw_hbm,
    dw_hbm,
    rate_hbm,
    hgain_hbm,
    state_hbm,
    keys_hbm,
    vals_hbm,
    bbeta_hbm,
    bdecay_hbm,
    live_hbm,
    out_hbm,
    mgain_hbm,
    up_hbm,
    down_hbm,
    mixed_ref,
    nstate_hbm,
    wst,
    wcat,
    bdw,
    tokx,
    gp,
    tokl,
    tokt,
    rate_ref,
    hgain_ref,
    bbeta_ref,
    bdecay_ref,
    live_ref,
    mgain_ref,
    proj_s,
    proj_r,
    ex_s,
    ex_r,
    keys,
    vals,
    state,
    up_all,
    down_all,
    out_all,
    bbeta,
    bdecay,
    mh,
    ar,
    ax,
    rs_s,
    rs_r,
    resid,
    fin_s,
    mx,
    loc,
    xs,
    xr,
    ts,
    tr,
    ps,
    pr,
    ms,
    mr,
    asem,
    arr,
    us,
    ur,
    ds_,
    dr,
    fs,
    fr,
    ring_s,
    ring_r,
    *,
    n_kv,
    n_tp,
):
    kv = lax.axis_index("kv")
    tp = lax.axis_index("tp")
    nz = n_kv // NX
    z = kv // NX
    x = kv % NX

    def local(src, dst, i):
        copy = pltpu.make_async_copy(src, dst, loc.at[i])
        copy.start()
        return copy

    def remote(src, dst, s, r, kv_to, tp_to):
        return pltpu.make_async_remote_copy(
            src_ref=src,
            dst_ref=dst,
            send_sem=s,
            recv_sem=r,
            device_id={"kv": kv_to, "tp": tp_to},
            device_id_type=pl.DeviceIdType.MESH,
        )

    in_tok = local(tok_hbm, tokx.at[x], 12)
    in_gain = local(ngain_hbm, gp.at[x], 13)
    in_w = [local(w, wst.at[i], i) for i, w in enumerate((qw_hbm, kw_hbm, vw_hbm, gw_hbm))]
    in_out = local(out_hbm, out_all.at[z], 6)
    in_up = local(up_hbm, up_all.at[z], 7)
    in_down = local(down_hbm, down_all.at[z], 8)
    lanes_z = pl.ds(pl.multiple_of(z * 256, 256), 256)
    in_b = [
        local(bw_hbm.at[:, lanes_z], bdw.at[0], 4),
        local(dw_hbm.at[:, lanes_z], bdw.at[1], 5),
    ]
    in_block = [
        local(bbeta_hbm, bbeta_ref, 14),
        local(bdecay_hbm, bdecay_ref, 15),
        local(live_hbm, live_ref, 16),
        local(keys_hbm, keys, 9),
        local(vals_hbm, vals, 10),
        local(state_hbm, state, 11),
    ]
    in_small = [
        local(rate_hbm, rate_ref, 17),
        local(hgain_hbm, hgain_ref, 18),
        local(mgain_hbm, mgain_ref, 19),
    ]

    barrier = pltpu.get_barrier_semaphore()

    def greet_kv(d, carry):
        pl.semaphore_signal(
            barrier,
            inc=1,
            device_id={"kv": (kv + d) % n_kv, "tp": tp},
            device_id_type=pl.DeviceIdType.MESH,
        )
        return carry

    def greet_tp(d, carry):
        pl.semaphore_signal(
            barrier,
            inc=1,
            device_id={"kv": kv, "tp": (tp + d) % n_tp},
            device_id_type=pl.DeviceIdType.MESH,
        )
        return carry

    lax.fori_loop(1, n_kv, greet_kv, 0)
    lax.fori_loop(1, n_tp, greet_tp, 0)

    in_tok.wait()
    in_gain.wait()
    tokl[...] = tokx[x].astype(F32).T.astype(BF16)
    tokt[z] = tokl[pl.ds(pl.multiple_of(z * 32, 32), 32), :]
    for copy in in_w:
        copy.wait()
    mine = pl.ds(pl.multiple_of(x * 64, 64), 64)
    wcat[mine, :] = wst[x]
    in_out.wait()
    in_up.wait()
    in_down.wait()

    pl.semaphore_wait(barrier, n_kv - 1 + n_tp - 1)

    sent_x = []
    for d in range(1, NX):
        to = (x + d) % NX
        peer = z * NX + to
        sent_x.append(remote(tokx.at[x], tokx.at[x], xs.at[0, d], xr.at[0, d], peer, tp))
        sent_x.append(remote(gp.at[x], gp.at[x], xs.at[1, d], xr.at[1, d], peer, tp))
        sent_x.append(
            remote(wst.at[to], wcat.at[mine, :], xs.at[2, d], xr.at[2, d], peer, tp)
        )
    for copy in sent_x:
        copy.start()

    sent_t = []
    for d in range(1, nz):
        to = (z + d) % nz
        sent_t.append(
            remote(
                tokl.at[pl.ds(pl.multiple_of(to * 32, 32), 32), :],
                tokt.at[z],
                ts.at[d],
                tr.at[d],
                to * NX + x,
                tp,
            )
        )
    for copy in sent_t:
        copy.start()

    def ring(way, step, what):
        to = (z + 1) % nz if way == 0 else (z + nz - 1) % nz
        block = (z + nz - (step - 1)) % nz if way == 0 else (z + step - 1) % nz
        ref = (out_all, up_all, down_all)[what].at[block]
        return remote(
            ref, ref, ring_s.at[way, step - 1, what], ring_r.at[way, step - 1, what], to * NX + x, tp
        )

    half = nz // 2
    plan = {}
    for step in range(1, half + 1):
        plan[step] = [
            (way, what)
            for what in range(3)
            for way in range(2)
            if step < half or way == (1 if what == 2 else 0)
        ]

    def ring_start(step):
        for way, what in plan[step]:
            ring(way, step, what).start()

    def ring_pass(step):
        for way, what in plan[step]:
            ring(way, step, what).wait_recv()
            if step < half and (way, what) in plan[step + 1]:
                ring(way, step + 1, what).start()

    ring_start(1)

    for copy in in_block:
        copy.wait()
    for i in range(4):
        pairs = [(2 * i + j // 2, slice(j % 2, j % 2 + 1)) for j in range(4)]
        bbeta[i] = jnp.concatenate([bbeta_ref[pair] for pair in pairs], axis=1)
        bdecay[i] = jnp.concatenate([bdecay_ref[pair] for pair in pairs], axis=1)

    def before(g, carry):
        state_before(g, keys, vals, state, bbeta, bdecay, live_ref)
        return carry

    lax.fori_loop(0, 2, before, 0)

    for copy in sent_x:
        copy.wait_recv()
    t = tokx[...].reshape(256, 256).astype(F32).T
    squares = jnp.sum(t * t, axis=1, keepdims=True)
    normed = (t * jnp.concatenate([gp[i] for i in range(NX)], axis=1)).astype(BF16)
    projected = dot(normed, wcat[...])
    for copy in in_b:
        copy.wait()
    small = jnp.concatenate(
        [bdw[...].astype(F32).reshape(32, 256), jnp.zeros((96, 256), F32)], axis=0
    ).astype(BF16)
    extra = dot_nt(normed, small)
    proj_s[...] = projected.reshape(n_kv, 8, 256).astype(BF16)
    lane = iota((256, 128), 1)
    high = squares.astype(BF16).astype(F32)
    extra = jnp.where(lane == 32, high, jnp.where(lane == 33, squares - high, extra))
    ex_s[...] = extra.reshape(n_kv, 8, 128).astype(BF16)
    proj_r[kv] = proj_s[kv]
    ex_r[z] = ex_s[kv]

    def send_proj(d, carry):
        to = (kv + d) % n_kv
        remote(proj_s.at[to], proj_r.at[kv], ps.at[0], pr.at[0], to, tp).start()
        return carry

    def send_extra(d, carry):
        to = ((z + d) % nz) * NX + x
        remote(ex_s.at[to], ex_r.at[z], ps.at[1], pr.at[1], to, tp).start()
        return carry

    lax.fori_loop(1, nz, send_extra, 0)
    lax.fori_loop(1, n_kv, send_proj, 0)

    ring_pass(1)
    lax.fori_loop(2, 4, before, 0)

    some = pl.ds(0, n_kv - 1)
    few = pl.ds(0, nz - 1)
    all_proj = remote(proj_s.at[some], proj_r.at[some], ps.at[0], pr.at[0], kv, tp)
    all_extra = remote(ex_s.at[few], ex_r.at[few], ps.at[1], pr.at[1], kv, tp)
    all_extra.wait_recv()
    all_proj.wait_recv()

    for copy in in_small:
        copy.wait()
    total = jnp.sum(proj_r[...].astype(F32).reshape(nz, NX, 8, 256), axis=0)
    extra = jnp.sum(ex_r[...].astype(F32), axis=0)
    inverse_rms = lax.rsqrt((extra[:, 32:33] + extra[:, 33:34]) / MODEL + EPS)
    extra = extra * inverse_rms
    queries, key_raw, value_raw, gate_raw = [total[i] * inverse_rms for i in range(4)]
    lane = iota((8, 128), 1)
    cols, heads = [], []
    for h in range(2):
        at = slice(128 * h, 128 * h + 128)
        k = key_raw[:, at]
        k = k * lax.rsqrt(jnp.sum(k * k, axis=1, keepdims=True) + EPS)
        k = k.astype(BF16).astype(F32)
        v = value_raw[:, at].astype(BF16).astype(F32)
        q = queries[:, at]
        b = jnp.sum(jnp.where(lane == 2 * tp + h, extra, 0.0), axis=1, keepdims=True)
        b = 1.0 / (1.0 + jnp.exp(-b))
        a = jnp.sum(jnp.where(lane == HEADS + 2 * tp + h, extra, 0.0), axis=1, keepdims=True)
        a = jnp.maximum(a, 0.0) + jnp.log1p(jnp.exp(-jnp.abs(a)))
        e = jnp.exp(-rate_ref[h] * a)
        qk = jnp.sum(q * k, axis=1, keepdims=True)
        cols += [k, q]
        heads.append((k, v, q, b, e, qk))
    columns = jnp.concatenate(cols + [jnp.zeros((96, 128), F32)], axis=0).T
    updates, readouts = {}, []
    for h in range(2):
        k, v, q, b, e, qk = heads[h]
        lines = []
        for s in range(8):
            old = state[s, h]
            one = slice(s, s + 1)
            kcol = columns[:, 16 * h + s : 16 * h + s + 1]
            qcol = columns[:, 16 * h + 8 + s : 16 * h + 9 + s]
            ks = jnp.sum(old * kcol, axis=0, keepdims=True)
            qs = jnp.sum(old * qcol, axis=0, keepdims=True)
            u = b[one] * (v[one] - e[one] * ks)
            updates[s, h] = u
            lines.append(e[one] * qs + qk[one] * u)
        readouts.append(jnp.concatenate(lines, axis=0))
    gated = []
    for h in range(2):
        rd = readouts[h]
        gate = gate_raw[:, 128 * h : 128 * h + 128]
        scaled = rd * lax.rsqrt(jnp.sum(rd * rd, axis=1, keepdims=True) / 128 + EPS) * hgain_ref[...]
        gated.append(scaled * (gate / (1.0 + jnp.exp(-gate))))
    mh[x] = jnp.concatenate(gated, axis=1).astype(BF16).astype(F32)
    sent_m = []
    for d in range(1, NX):
        peer = z * NX + (x + d) % NX
        sent_m.append(remote(mh.at[x], mh.at[x], ms.at[d], mr.at[d], peer, tp))
    for copy in sent_m:
        copy.start()
    ring_pass(2)

    for h in range(2):
        e = heads[h][4]
        for s in range(8):
            kcol = columns[:, 16 * h + s : 16 * h + s + 1]
            state[s, h] = e[s : s + 1] * state[s, h] + kcol * updates[s, h]
    put_state = local(state, nstate_hbm, 0)
    ring_pass(3)

    for copy in sent_m:
        copy.wait_recv()
    ring_pass(4)
    m = mh[...].reshape(32, 256)
    ar[tp] = dot_nt(m.astype(BF16), out_all[...].reshape(nz * 64, 256)).astype(BF16)

    def send_ar(d, carry):
        to = (tp + d) % n_tp
        remote(ar.at[tp], ar.at[tp], asem, arr, kv, to).start()
        return carry

    lax.fori_loop(1, n_tp, send_ar, 0)
    tps = pl.ds(0, n_tp - 1)
    all_ar = remote(ar.at[tps], ar.at[tps], asem, arr, kv, tp)
    for copy in sent_t:
        copy.wait_recv()
    tokens = jnp.concatenate([tokt[i].astype(F32) for i in range(nz)], axis=1)
    gains = []
    for p in range(nz):
        gain = mgain_ref[pl.ds(2 * p + x // 2, 1), :]
        gains.append(jnp.where(x % 2 == 0, gain[:, :64], gain[:, 64:]))
    gains = jnp.concatenate(gains, axis=1)
    all_ar.wait_recv()

    attended = jnp.sum(ar[...].astype(F32), axis=0)
    residual = (tokens + attended).astype(BF16).astype(F32)
    for i in range(nz):
        resid[i] = residual[:, 64 * i : 64 * i + 64]
    squares = jnp.sum(residual * residual, axis=1, keepdims=True)
    mlp_in = (residual * gains).astype(BF16)
    pre = dot(mlp_in, up_all[...].reshape(nz * 64, 1024))
    high = squares.astype(BF16).astype(F32)
    lane = iota((32, 128), 1)
    tail = jnp.where(lane == 0, high, jnp.where(lane == 1, squares - high, 0.0))
    ax[x] = jnp.concatenate([pre, tail], axis=1).astype(BF16)
    sent_u = []
    for d in range(1, NX):
        peer = z * NX + (x + d) % NX
        sent_u.append(remote(ax.at[x], ax.at[x], us.at[d], ur.at[d], peer, tp))
    for copy in sent_u:
        copy.start()
    for copy in sent_u:
        copy.wait_recv()
    total = jnp.sum(ax[...].astype(F32), axis=0)
    rms = lax.rsqrt((total[:, 1024:1025] + total[:, 1025:1026]) / MODEL + EPS)
    hidden = jnp.maximum(total[:, :1024] * rms, 0.0)
    hidden = (hidden * hidden).astype(BF16)
    output = dot_nt(hidden, down_all[...].reshape(nz * 64, 1024))
    for i in range(nz):
        rs_s[i] = output[:, 64 * i : 64 * i + 64].astype(BF16)
    rs_r[tp] = rs_s[tp]

    def send_rs(d, carry):
        to = (tp + d) % n_tp
        remote(rs_s.at[to], rs_r.at[tp], ds_, dr, kv, to).start()
        return carry

    lax.fori_loop(1, n_tp, send_rs, 0)
    all_rs = remote(rs_s.at[tps], rs_r.at[tps], ds_, dr, kv, tp)
    all_rs.wait_recv()
    fin_s[...] = (resid[tp] + jnp.sum(rs_r[...].astype(F32), axis=0)).astype(BF16)

    at_home = z == tp
    far = tp * NX + x

    def send_fin(t, carry):
        @pl.when(jnp.logical_or(jnp.logical_not(at_home), t != tp))
        def _():
            remote(fin_s, mx.at[z], fs, fr, far, t).start()

        return carry

    @pl.when(at_home)
    def _():
        mx[z] = fin_s[...]

    lax.fori_loop(0, n_tp, send_fin, 0)

    put_state.wait()
    for copy in sent_x + sent_t + sent_m + sent_u:
        copy.wait_send()
    for step in plan:
        for way, what in plan[step]:
            ring(way, step, what).wait_send()
    all_proj.wait_send()
    all_extra.wait_send()
    all_ar.wait_send()
    all_rs.wait_send()

    eight = remote(mx, mx, fs, fr, kv, tp)
    seven = remote(mx.at[few], mx.at[few], fs, fr, kv, tp)

    @pl.when(at_home)
    def _():
        seven.wait_recv()
        seven.wait_send()

    @pl.when(jnp.logical_not(at_home))
    def _():
        eight.wait_recv()
        eight.wait_send()

    mixed_ref[...] = mx[...].astype(F32).reshape(nz * 32, 64).T.astype(BF16)


def body(
    tokens,
    norm_gain,
    query_weight,
    key_weight,
    value_weight,
    gate_weight,
    beta_weight,
    decay_weight,
    decay_rate,
    head_gain,
    carried_state,
    block_keys,
    block_values,
    block_beta,
    block_decay,
    live_count,
    out_weight,
    mlp_gain,
    up_weight,
    down_weight,
):
    n_kv = lax.axis_size("kv")
    n_tp = lax.axis_size("tp")
    nz = n_kv // NX
    vmem = pl.BlockSpec(memory_space=pltpu.VMEM)
    hbm = pl.BlockSpec(memory_space=pl.ANY)
    dma = pltpu.SemaphoreType.DMA
    mixed, new_state = pl.pallas_call(
        functools.partial(kernel, n_kv=n_kv, n_tp=n_tp),
        out_shape=(
            jax.ShapeDtypeStruct(tokens.shape[::-1], BF16),
            jax.ShapeDtypeStruct(carried_state.shape, F32),
        ),
        in_specs=[hbm] * 20,
        out_specs=(vmem, hbm),
        scratch_shapes=[
            pltpu.VMEM((4, 64, 256), BF16),
            pltpu.VMEM((256, 256), BF16),
            pltpu.VMEM((2, 16, 256), BF16),
            pltpu.VMEM((NX, 64, 256), BF16),
            pltpu.VMEM((NX, 1, 64), F32),
            pltpu.VMEM((256, 64), BF16),
            pltpu.VMEM((nz, 32, 64), BF16),
            pltpu.SMEM((2,), F32),
            pltpu.VMEM((1, 128), F32),
            pltpu.VMEM((8, 2, 64), F32),
            pltpu.VMEM((8, 2, 64), F32),
            pltpu.SMEM((8,), jnp.int32),
            pltpu.VMEM((16, 128), F32),
            pltpu.VMEM((n_kv, 8, 256), BF16),
            pltpu.VMEM((n_kv, 8, 256), BF16),
            pltpu.VMEM((n_kv, 8, 128), BF16),
            pltpu.VMEM((nz, 8, 128), BF16),
            pltpu.VMEM((8, 2, 64, 128), BF16),
            pltpu.VMEM((8, 2, 64, 128), BF16),
            pltpu.VMEM((8, 2, 128, 128), F32),
            pltpu.VMEM((nz, 64, 1024), BF16),
            pltpu.VMEM((nz, 64, 1024), BF16),
            pltpu.VMEM((nz, 64, 256), BF16),
            pltpu.VMEM((4, 1, 256), F32),
            pltpu.VMEM((4, 1, 256), F32),
            pltpu.VMEM((NX, 8, 256), F32),
            pltpu.VMEM((n_tp, 32, 512), BF16),
            pltpu.VMEM((NX, 32, 1152), BF16),
            pltpu.VMEM((n_tp, 32, 64), BF16),
            pltpu.VMEM((n_tp, 32, 64), BF16),
            pltpu.VMEM((nz, 32, 64), F32),
            pltpu.VMEM((32, 64), BF16),
            pltpu.VMEM((nz, 32, 64), BF16),
            dma((20,)),
            dma((3, NX)),
            dma((3, NX)),
            dma((nz,)),
            dma((nz,)),
            dma((2,)),
            dma((2,)),
            dma((NX,)),
            dma((NX,)),
            dma,
            dma,
            dma((NX,)),
            dma((NX,)),
            dma,
            dma,
            dma,
            dma,
            dma((2, 4, 3)),
            dma((2, 4, 3)),
        ],
        compiler_params=pltpu.CompilerParams(
            collective_id=0, has_side_effects=True
        ),
        name="layer",
    )(
        tokens.T,
        norm_gain.reshape(1, -1),
        query_weight,
        key_weight,
        value_weight,
        gate_weight,
        beta_weight.T,
        decay_weight.T,
        decay_rate,
        head_gain.reshape(1, -1),
        carried_state,
        block_keys,
        block_values,
        block_beta,
        block_decay,
        live_count,
        out_weight.T,
        mlp_gain.reshape(-1, 128),
        up_weight,
        down_weight.T,
    )
    return mixed.T, new_state


def solution(mesh):
    placed = (
        P(None, "kv"),
        P("kv"),
        P("kv", "tp"),
        P("kv", "tp"),
        P("kv", "tp"),
        P("kv", "tp"),
        P(),
        P(),
        P("tp"),
        P(),
        P("kv", "tp", None, None),
        P("kv", "tp", None, None),
        P("kv", "tp", None, None),
        P("kv", "tp", None),
        P("kv", "tp", None),
        P("kv"),
        P("tp", "kv"),
        P(),
        P("kv", "tp"),
        P("tp", "kv"),
    )
    return jax.shard_map(
        body,
        mesh=mesh,
        in_specs=placed,
        out_specs=(P(None, "kv"), P("kv", "tp", None, None)),
        check_vma=False,
    )
```

```python
import functools

import jax
import jax.numpy as jnp
from jax import lax
from jax.experimental import pallas as pl
from jax.experimental.pallas import tpu as pltpu
from jax.sharding import PartitionSpec as P

MODEL = 2048
HEADS = 16
EPS = 1e-06
NX = 4
F32 = jnp.float32
BF16 = jnp.bfloat16


def dot(a, b):
    return jnp.dot(a, b, preferred_element_type=F32)


def split(a):
    high = a.astype(BF16)
    return high, (a - high.astype(F32)).astype(BF16)


def dot_nt(a, b):
    return lax.dot_general(a, b, (((1,), (1,)), ((), ())), preferred_element_type=F32)


def dot2(a, b):
    bh, bl = split(b)
    return dot(a, bh) + dot(a, bl)


def iota(shape, dim):
    return lax.broadcasted_iota(jnp.int32, shape, dim)


def dot3(a, b):
    ah, al = split(a)
    bh, bl = split(b)
    n = a.shape[0]
    both = dot(jnp.concatenate([ah, al], axis=0), bh)
    return both[:n] + both[n:] + dot(ah, bl)


def apart(a, mask):
    return jnp.concatenate([a] * 4, axis=0) * mask


def dot3_blocks(a, b, mask):
    ah, al = split(a)
    bh, bl = split(b)
    both = dot(jnp.concatenate([ah, al], axis=0), apart(bh, mask))
    return both[:64] + both[64:] + dot(ah, apart(bl, mask))


def unit_inverse(lower, r, c, mask):
    def same(bits):
        return (r >> bits) == (c >> bits)

    ident = jnp.where(r == c, 1.0, 0.0)
    power = jnp.where(same(3), -lower, 0.0)
    total = ident + power
    for _ in range(2):
        power = dot3_blocks(power, power, mask)
        total = total + dot3_blocks(total, power, mask)
    for bits in (3, 4, 5):
        off = jnp.where(same(bits + 1) & jnp.logical_not(same(bits)), lower, 0.0)
        total = total - dot3_blocks(total, dot3_blocks(off, total, mask), mask)
    return total


def state_before(g, keys, vals, state, bbeta, bdecay, live, mask_ref):
    mask = mask_ref[...]
    r = iota((64, 256), 0)
    lane = iota((64, 256), 1)
    c = lane & 63
    pair = lane >> 6
    n0, n1 = live[2 * g] - 1, live[2 * g + 1] - 1
    lane1 = iota((1, 256), 1)
    live_row = (lane1 & 63) < jnp.where(lane1 < 128, n0, n1)
    d_row = jnp.where(live_row, bdecay[g], 0.0)
    b_row = jnp.where(live_row, bbeta[g], 0.0)
    r1 = iota((256, 128), 0)
    live_col = (r1 & 63) < jnp.where(r1 < 128, n0, n1)
    k_all = jnp.where(live_col, keys[pl.ds(2 * g, 2)].astype(F32).reshape(256, 128), 0.0)
    v_all = jnp.where(live_col, vals[pl.ds(2 * g, 2)].astype(F32).reshape(256, 128), 0.0)
    kb = k_all.astype(BF16)
    kt = k_all.T.astype(BF16)
    b_diag = jnp.where(r == c, b_row, 0.0)
    d_tri = jnp.where(c <= r, d_row, 0.0)
    b_col, t_col = [], []
    for p in range(4):
        b_col.append(jnp.sum(jnp.where(pair == p, b_diag, 0.0), axis=1, keepdims=True))
        t_col.append(jnp.sum(jnp.where(pair == p, d_tri, 0.0), axis=1, keepdims=True))

    def side(columns):
        low = jnp.where(pair == 0, columns[0], columns[1])
        high = jnp.where(pair == 2, columns[2], columns[3])
        return jnp.where(pair < 2, low, high)

    tots = side(t_col)
    tot_row = jnp.sum(jnp.where(r == c, tots, 0.0), axis=0, keepdims=True)
    strict = c < r
    fade = jnp.exp(jnp.where(strict, tots - tot_row, 0.0))
    gram = dot(kb, kt)
    gram = side([gram[64 * p : 64 * p + 64] for p in range(4)])
    lower = jnp.where(strict, side(b_col) * gram * fade, 0.0)
    inverse = unit_inverse(lower, r, c, mask)
    zero = jnp.zeros((64, 128), F32)

    def spread(blocks):
        rows = [[blocks[p] if q == p else zero for q in range(4)] for p in range(4)]
        return jnp.concatenate([jnp.concatenate(row, axis=1) for row in rows], axis=0)

    right = []
    for p in range(4):
        at = slice(64 * p, 64 * p + 64)
        seen = dot2(kb[at], state[2 * g + p // 2, p % 2])
        right.append(b_col[p] * (v_all[at] - jnp.exp(t_col[p]) * seen))
    update = dot3(inverse, spread(right))
    faded = []
    for p in range(4):
        faded.append(update[:, 128 * p : 128 * p + 128] * jnp.exp(t_col[p][63:64] - t_col[p]))
    added = dot2(kt, spread(faded))
    for p in range(4):
        end = jnp.exp(t_col[p][63:64])
        at = (2 * g + p // 2, p % 2)
        state[at] = end * state[at] + added[:, 128 * p : 128 * p + 128]


def kernel(
    tok_hbm,
    ngain_hbm,
    qw_hbm,
    kw_hbm,
    vw_hbm,
    gw_hbm,
    bw_hbm,
    dw_hbm,
    rate_hbm,
    hgain_hbm,
    state_hbm,
    keys_hbm,
    vals_hbm,
    bbeta_hbm,
    bdecay_hbm,
    live_hbm,
    out_hbm,
    mgain_hbm,
    up_hbm,
    down_hbm,
    mixed_ref,
    state,
    wst,
    wcat,
    bdw,
    tokx,
    gp,
    tokl,
    tokt,
    rate_ref,
    hgain_ref,
    bbeta_ref,
    bdecay_ref,
    live_ref,
    mgain_ref,
    proj_s,
    proj_r,
    ex_s,
    ex_r,
    keys,
    vals,
    mask,
    up_all,
    down_all,
    out_all,
    bbeta,
    bdecay,
    mh,
    ar,
    ax,
    rs_s,
    rs_r,
    resid,
    fin_s,
    mx,
    loc,
    xs,
    xr,
    ts,
    tr,
    ps,
    pr,
    ms,
    mr,
    asem,
    arr,
    us,
    ur,
    ds_,
    dr,
    fs,
    fr,
    ring_s,
    ring_r,
    round_r,
    *,
    n_kv,
    n_tp,
):
    kv = lax.axis_index("kv")
    tp = lax.axis_index("tp")
    nz = n_kv // NX
    z = kv // NX
    x = kv % NX

    def local(src, dst, i):
        copy = pltpu.make_async_copy(src, dst, loc.at[i])
        copy.start()
        return copy

    def remote(src, dst, s, r, kv_to, tp_to):
        return pltpu.make_async_remote_copy(
            src_ref=src,
            dst_ref=dst,
            send_sem=s,
            recv_sem=r,
            device_id={"kv": kv_to, "tp": tp_to},
            device_id_type=pl.DeviceIdType.MESH,
        )

    in_tok = local(tok_hbm, tokx.at[x], 12)
    in_gain = local(ngain_hbm, gp.at[x], 13)
    in_w = [local(w, wst.at[i], i) for i, w in enumerate((qw_hbm, kw_hbm, vw_hbm, gw_hbm))]
    in_out = local(out_hbm, out_all.at[z], 6)
    in_up = local(up_hbm, up_all.at[z], 7)
    in_down = local(down_hbm, down_all.at[z], 8)
    lanes_z = pl.ds(pl.multiple_of(z * 256, 256), 256)
    in_b = [
        local(bw_hbm.at[:, lanes_z], bdw.at[0], 4),
        local(dw_hbm.at[:, lanes_z], bdw.at[1], 5),
    ]
    in_block = [
        local(bbeta_hbm, bbeta_ref, 14),
        local(bdecay_hbm, bdecay_ref, 15),
        local(live_hbm, live_ref, 16),
        local(keys_hbm, keys, 9),
        local(vals_hbm, vals, 10),
        local(state_hbm, state, 11),
    ]
    in_small = [
        local(rate_hbm, rate_ref, 17),
        local(hgain_hbm, hgain_ref, 18),
        local(mgain_hbm, mgain_ref, 19),
    ]

    up_z = ((z + 1) % nz) * NX + x
    down_z = ((z + nz - 1) % nz) * NX + x
    barrier = pltpu.get_barrier_semaphore()

    def greet(sem, kv_to, tp_to):
        pl.semaphore_signal(
            sem,
            inc=1,
            device_id={"kv": kv_to, "tp": tp_to},
            device_id_type=pl.DeviceIdType.MESH,
        )

    greet(barrier, up_z, tp)
    greet(barrier, down_z, tp)
    for d in range(1, NX):
        greet(barrier, z * NX + (x + d) % NX, tp)

    def greet_tp(d, carry):
        greet(barrier, kv, (tp + d) % n_tp)
        return carry

    lax.fori_loop(1, n_tp, greet_tp, 0)

    def round_send(i):
        greet(round_r.at[i], up_z, tp)
        greet(round_r.at[i], down_z, tp)

    def round_wait(i):
        pl.semaphore_wait(round_r.at[i], 2)

    mask[...] = jnp.where((iota((256, 256), 0) >> 6) == (iota((256, 256), 1) >> 6), 1.0, 0.0).astype(
        BF16
    )
    in_tok.wait()
    in_gain.wait()
    tokl[...] = tokx[x].astype(F32).T.astype(BF16)
    tokt[z] = tokl[pl.ds(pl.multiple_of(z * 32, 32), 32), :]
    for copy in in_w:
        copy.wait()
    mine = pl.ds(pl.multiple_of(x * 64, 64), 64)
    wcat[mine, :] = wst[x]
    in_out.wait()
    in_up.wait()
    in_down.wait()

    pl.semaphore_wait(barrier, 2 + NX - 1 + n_tp - 1)

    sent_x = []
    for d in range(1, NX):
        to = (x + d) % NX
        peer = z * NX + to
        sent_x.append(remote(tokx.at[x], tokx.at[x], xs.at[0, d], xr.at[0, d], peer, tp))
        sent_x.append(remote(gp.at[x], gp.at[x], xs.at[1, d], xr.at[1, d], peer, tp))
        sent_x.append(
            remote(wst.at[to], wcat.at[mine, :], xs.at[2, d], xr.at[2, d], peer, tp)
        )
    for copy in sent_x:
        copy.start()

    sent_t = []
    for d in range(1, nz):
        to = (z + d) % nz
        sent_t.append(
            remote(
                tokl.at[pl.ds(pl.multiple_of(to * 32, 32), 32), :],
                tokt.at[z],
                ts.at[d],
                tr.at[d],
                to * NX + x,
                tp,
            )
        )
    def ring(way, step, what):
        to = up_z if way == 0 else down_z
        block = (z + nz - (step - 1)) % nz if way == 0 else (z + step - 1) % nz
        ref = (out_all, up_all, down_all)[what].at[block]
        return remote(
            ref, ref, ring_s.at[way, step - 1, what], ring_r.at[way, step - 1, what], to, tp
        )

    half = nz // 2
    plan = {}
    for step in range(1, half + 1):
        plan[step] = [
            (way, what)
            for what in range(3)
            for way in range(2)
            if step < half or way == (1 if what == 2 else 0)
        ]

    OUT, UP, DOWN = 0, 1, 2

    def ways(step, what):
        return [way for way in range(2) if (way, what) in plan.get(step, ())]

    def ring_start(step, what):
        for way in ways(step, what):
            ring(way, step, what).start()

    def ring_pass(step, what):
        for way in ways(step, what):
            ring(way, step, what).wait_recv()
            if way in ways(step + 1, what):
                ring(way, step + 1, what).start()

    ring_start(1, OUT)
    ring_start(1, UP)
    round_send(0)

    for copy in in_block:
        copy.wait()
    for i in range(4):
        pairs = [(2 * i + j // 2, slice(j % 2, j % 2 + 1)) for j in range(4)]
        bbeta[i] = jnp.concatenate([bbeta_ref[pair] for pair in pairs], axis=1)
        bdecay[i] = jnp.concatenate([bdecay_ref[pair] for pair in pairs], axis=1)

    def before(g, carry):
        state_before(g, keys, vals, state, bbeta, bdecay, live_ref, mask)
        return carry

    lax.fori_loop(0, 1, before, 0)
    round_wait(0)
    round_send(1)
    ring_pass(1, OUT)
    ring_start(1, DOWN)
    lax.fori_loop(1, 2, before, 0)
    round_wait(1)
    round_send(2)

    for copy in sent_x:
        copy.wait_recv()
    round_wait(2)
    round_send(3)
    t = tokx[...].reshape(256, 256).astype(F32).T
    squares = jnp.sum(t * t, axis=1, keepdims=True)
    normed = (t * jnp.concatenate([gp[i] for i in range(NX)], axis=1)).astype(BF16)
    projected = dot(normed, wcat[...])
    for copy in in_b:
        copy.wait()
    small = jnp.concatenate(
        [bdw[...].astype(F32).reshape(32, 256), jnp.zeros((96, 256), F32)], axis=0
    ).astype(BF16)
    extra = dot_nt(normed, small)
    proj_s[...] = projected.reshape(n_kv, 8, 256).astype(BF16)
    lane = iota((256, 128), 1)
    high = squares.astype(BF16).astype(F32)
    extra = jnp.where(lane == 32, high, jnp.where(lane == 33, squares - high, extra))
    ex_s[...] = extra.reshape(n_kv, 8, 128).astype(BF16)
    proj_r[kv] = proj_s[kv]
    ex_r[z] = ex_s[kv]

    def send_proj(d, carry):
        to = (kv + d) % n_kv
        remote(proj_s.at[to], proj_r.at[kv], ps.at[0], pr.at[0], to, tp).start()
        return carry

    def send_extra(d, carry):
        to = ((z + d) % nz) * NX + x
        remote(ex_s.at[to], ex_r.at[z], ps.at[1], pr.at[1], to, tp).start()
        return carry

    round_wait(3)
    lax.fori_loop(1, nz, send_extra, 0)
    lax.fori_loop(1, n_kv, send_proj, 0)
    for copy in sent_t:
        copy.start()

    ring_pass(1, UP)
    ring_pass(2, OUT)
    lax.fori_loop(2, 3, before, 0)
    ring_pass(1, DOWN)
    lax.fori_loop(3, 4, before, 0)
    ring_pass(2, UP)
    ring_pass(3, OUT)

    some = pl.ds(0, n_kv - 1)
    few = pl.ds(0, nz - 1)
    all_proj = remote(proj_s.at[some], proj_r.at[some], ps.at[0], pr.at[0], kv, tp)
    all_extra = remote(ex_s.at[few], ex_r.at[few], ps.at[1], pr.at[1], kv, tp)
    all_extra.wait_recv()
    all_proj.wait_recv()

    for copy in in_small:
        copy.wait()
    total = jnp.sum(proj_r[...].astype(F32).reshape(nz, NX, 8, 256), axis=0)
    extra = jnp.sum(ex_r[...].astype(F32), axis=0)
    inverse_rms = lax.rsqrt((extra[:, 32:33] + extra[:, 33:34]) / MODEL + EPS)
    extra = extra * inverse_rms
    queries, key_raw, value_raw, gate_raw = [total[i] * inverse_rms for i in range(4)]
    lane = iota((8, 128), 1)
    cols, heads = [], []
    for h in range(2):
        at = slice(128 * h, 128 * h + 128)
        k = key_raw[:, at]
        k = k * lax.rsqrt(jnp.sum(k * k, axis=1, keepdims=True) + EPS)
        k = k.astype(BF16).astype(F32)
        v = value_raw[:, at].astype(BF16).astype(F32)
        q = queries[:, at]
        b = jnp.sum(jnp.where(lane == 2 * tp + h, extra, 0.0), axis=1, keepdims=True)
        b = 1.0 / (1.0 + jnp.exp(-b))
        a = jnp.sum(jnp.where(lane == HEADS + 2 * tp + h, extra, 0.0), axis=1, keepdims=True)
        a = jnp.maximum(a, 0.0) + jnp.log1p(jnp.exp(-jnp.abs(a)))
        e = jnp.exp(-rate_ref[h] * a)
        qk = jnp.sum(q * k, axis=1, keepdims=True)
        cols += [k, q]
        heads.append((k, v, q, b, e, qk))
    columns = jnp.concatenate(cols + [jnp.zeros((96, 128), F32)], axis=0).T
    updates, readouts = {}, []
    for h in range(2):
        k, v, q, b, e, qk = heads[h]
        lines = []
        for s in range(8):
            old = state[s, h]
            one = slice(s, s + 1)
            kcol = columns[:, 16 * h + s : 16 * h + s + 1]
            qcol = columns[:, 16 * h + 8 + s : 16 * h + 9 + s]
            ks = jnp.sum(old * kcol, axis=0, keepdims=True)
            qs = jnp.sum(old * qcol, axis=0, keepdims=True)
            u = b[one] * (v[one] - e[one] * ks)
            updates[s, h] = u
            lines.append(e[one] * qs + qk[one] * u)
        readouts.append(jnp.concatenate(lines, axis=0))
    gated = []
    for h in range(2):
        rd = readouts[h]
        gate = gate_raw[:, 128 * h : 128 * h + 128]
        scaled = rd * lax.rsqrt(jnp.sum(rd * rd, axis=1, keepdims=True) / 128 + EPS) * hgain_ref[...]
        gated.append(scaled * (gate / (1.0 + jnp.exp(-gate))))
    mh[x] = jnp.concatenate(gated, axis=1).astype(BF16).astype(F32)
    sent_m = []
    for d in range(1, NX):
        peer = z * NX + (x + d) % NX
        sent_m.append(remote(mh.at[x], mh.at[x], ms.at[d], mr.at[d], peer, tp))
    for copy in sent_m:
        copy.start()
    ring_pass(2, DOWN)

    for h in range(2):
        e = heads[h][4]
        for s in range(8):
            kcol = columns[:, 16 * h + s : 16 * h + s + 1]
            state[s, h] = e[s : s + 1] * state[s, h] + kcol * updates[s, h]
    ring_pass(3, UP)

    for copy in sent_m:
        copy.wait_recv()
    ring_pass(4, OUT)
    m = mh[...].reshape(32, 256)
    ar[tp] = dot_nt(m.astype(BF16), out_all[...].reshape(nz * 64, 256)).astype(BF16)

    def send_ar(d, carry):
        to = (tp + d) % n_tp
        remote(ar.at[tp], ar.at[tp], asem, arr, kv, to).start()
        return carry

    lax.fori_loop(1, n_tp, send_ar, 0)
    ring_pass(3, DOWN)
    tps = pl.ds(0, n_tp - 1)
    all_ar = remote(ar.at[tps], ar.at[tps], asem, arr, kv, tp)
    for copy in sent_t:
        copy.wait_recv()
    tokens = jnp.concatenate([tokt[i].astype(F32) for i in range(nz)], axis=1)
    gains = []
    for p in range(nz):
        gain = mgain_ref[pl.ds(2 * p + x // 2, 1), :]
        gains.append(jnp.where(x % 2 == 0, gain[:, :64], gain[:, 64:]))
    gains = jnp.concatenate(gains, axis=1)
    all_ar.wait_recv()

    attended = jnp.sum(ar[...].astype(F32), axis=0)
    residual = (tokens + attended).astype(BF16).astype(F32)
    for i in range(nz):
        resid[i] = residual[:, 64 * i : 64 * i + 64]
    squares = jnp.sum(residual * residual, axis=1, keepdims=True)
    mlp_in = (residual * gains).astype(BF16)
    ring_pass(4, UP)
    pre = dot(mlp_in, up_all[...].reshape(nz * 64, 1024))
    high = squares.astype(BF16).astype(F32)
    lane = iota((32, 128), 1)
    tail = jnp.where(lane == 0, high, jnp.where(lane == 1, squares - high, 0.0))
    ax[x] = jnp.concatenate([pre, tail], axis=1).astype(BF16)
    sent_u = []
    for d in range(1, NX):
        peer = z * NX + (x + d) % NX
        sent_u.append(remote(ax.at[x], ax.at[x], us.at[d], ur.at[d], peer, tp))
    for copy in sent_u:
        copy.start()
    ring_pass(4, DOWN)
    for copy in sent_u:
        copy.wait_recv()
    total = jnp.sum(ax[...].astype(F32), axis=0)
    rms = lax.rsqrt((total[:, 1024:1025] + total[:, 1025:1026]) / MODEL + EPS)
    hidden = jnp.maximum(total[:, :1024] * rms, 0.0)
    hidden = (hidden * hidden).astype(BF16)
    output = dot_nt(hidden, down_all[...].reshape(nz * 64, 1024))
    for i in range(nz):
        rs_s[i] = output[:, 64 * i : 64 * i + 64].astype(BF16)
    rs_r[tp] = rs_s[tp]

    def send_rs(d, carry):
        to = (tp + d) % n_tp
        remote(rs_s.at[to], rs_r.at[tp], ds_, dr, kv, to).start()
        return carry

    lax.fori_loop(1, n_tp, send_rs, 0)
    all_rs = remote(rs_s.at[tps], rs_r.at[tps], ds_, dr, kv, tp)
    all_rs.wait_recv()
    fin_s[...] = (resid[tp] + jnp.sum(rs_r[...].astype(F32), axis=0)).astype(BF16)

    at_home = z == tp
    far = tp * NX + x

    def send_fin(t, carry):
        @pl.when(jnp.logical_or(jnp.logical_not(at_home), t != tp))
        def _():
            remote(fin_s, mx.at[z], fs, fr, far, t).start()

        return carry

    @pl.when(at_home)
    def _():
        mx[z] = fin_s[...]

    lax.fori_loop(0, n_tp, send_fin, 0)

    for copy in sent_x + sent_t + sent_m + sent_u:
        copy.wait_send()
    for step in plan:
        for way, what in plan[step]:
            ring(way, step, what).wait_send()
    all_proj.wait_send()
    all_extra.wait_send()
    all_ar.wait_send()
    all_rs.wait_send()

    eight = remote(mx, mx, fs, fr, kv, tp)
    seven = remote(mx.at[few], mx.at[few], fs, fr, kv, tp)

    @pl.when(at_home)
    def _():
        seven.wait_recv()
        seven.wait_send()

    @pl.when(jnp.logical_not(at_home))
    def _():
        eight.wait_recv()
        eight.wait_send()

    mixed_ref[...] = mx[...].astype(F32).reshape(nz * 32, 64).T.astype(BF16)


def body(
    tokens,
    norm_gain,
    query_weight,
    key_weight,
    value_weight,
    gate_weight,
    beta_weight,
    decay_weight,
    decay_rate,
    head_gain,
    carried_state,
    block_keys,
    block_values,
    block_beta,
    block_decay,
    live_count,
    out_weight,
    mlp_gain,
    up_weight,
    down_weight,
):
    n_kv = lax.axis_size("kv")
    n_tp = lax.axis_size("tp")
    nz = n_kv // NX
    vmem = pl.BlockSpec(memory_space=pltpu.VMEM)
    hbm = pl.BlockSpec(memory_space=pltpu.HBM)
    dma = pltpu.SemaphoreType.DMA
    operands = (
        tokens.T,
        norm_gain.reshape(1, -1),
        query_weight,
        key_weight,
        value_weight,
        gate_weight,
        beta_weight.T,
        decay_weight.T,
        decay_rate,
        head_gain.reshape(1, -1),
        carried_state,
        block_keys,
        block_values,
        block_beta,
        block_decay,
        live_count,
        out_weight.T,
        mlp_gain.reshape(-1, 128),
        up_weight,
        down_weight.T,
    )
    mixed, new_state = pl.pallas_call(
        functools.partial(kernel, n_kv=n_kv, n_tp=n_tp),
        out_shape=(
            jax.ShapeDtypeStruct(tokens.shape[::-1], BF16),
            jax.ShapeDtypeStruct(carried_state.shape, F32),
        ),
        in_specs=[hbm] * 20,
        out_specs=(vmem, vmem),
        scratch_shapes=[
            pltpu.VMEM((4, 64, 256), BF16),
            pltpu.VMEM((256, 256), BF16),
            pltpu.VMEM((2, 16, 256), BF16),
            pltpu.VMEM((NX, 64, 256), BF16),
            pltpu.VMEM((NX, 1, 64), F32),
            pltpu.VMEM((256, 64), BF16),
            pltpu.VMEM((nz, 32, 64), BF16),
            pltpu.SMEM((2,), F32),
            pltpu.VMEM((1, 128), F32),
            pltpu.VMEM((8, 2, 64), F32),
            pltpu.VMEM((8, 2, 64), F32),
            pltpu.SMEM((8,), jnp.int32),
            pltpu.VMEM((16, 128), F32),
            pltpu.VMEM((n_kv, 8, 256), BF16),
            pltpu.VMEM((n_kv, 8, 256), BF16),
            pltpu.VMEM((n_kv, 8, 128), BF16),
            pltpu.VMEM((nz, 8, 128), BF16),
            pltpu.VMEM((8, 2, 64, 128), BF16),
            pltpu.VMEM((8, 2, 64, 128), BF16),
            pltpu.VMEM((256, 256), BF16),
            pltpu.VMEM((nz, 64, 1024), BF16),
            pltpu.VMEM((nz, 64, 1024), BF16),
            pltpu.VMEM((nz, 64, 256), BF16),
            pltpu.VMEM((4, 1, 256), F32),
            pltpu.VMEM((4, 1, 256), F32),
            pltpu.VMEM((NX, 8, 256), F32),
            pltpu.VMEM((n_tp, 32, 512), BF16),
            pltpu.VMEM((NX, 32, 1152), BF16),
            pltpu.VMEM((n_tp, 32, 64), BF16),
            pltpu.VMEM((n_tp, 32, 64), BF16),
            pltpu.VMEM((nz, 32, 64), F32),
            pltpu.VMEM((32, 64), BF16),
            pltpu.VMEM((nz, 32, 64), BF16),
            dma((20,)),
            dma((3, NX)),
            dma((3, NX)),
            dma((nz,)),
            dma((nz,)),
            dma((2,)),
            dma((2,)),
            dma((NX,)),
            dma((NX,)),
            dma,
            dma,
            dma((NX,)),
            dma((NX,)),
            dma,
            dma,
            dma,
            dma,
            dma((2, 4, 3)),
            dma((2, 4, 3)),
            pltpu.SemaphoreType.REGULAR((4,)),
        ],
        compiler_params=pltpu.CompilerParams(
            collective_id=0, has_side_effects=True, vmem_limit_bytes=40 * 1024 * 1024
        ),
        name="layer",
    )(*[pltpu.with_memory_space_constraint(a, pltpu.HBM) for a in operands])
    return mixed.T, new_state


def solution(mesh):
    placed = (
        P(None, "kv"),
        P("kv"),
        P("kv", "tp"),
        P("kv", "tp"),
        P("kv", "tp"),
        P("kv", "tp"),
        P(),
        P(),
        P("tp"),
        P(),
        P("kv", "tp", None, None),
        P("kv", "tp", None, None),
        P("kv", "tp", None, None),
        P("kv", "tp", None),
        P("kv", "tp", None),
        P("kv"),
        P("tp", "kv"),
        P(),
        P("kv", "tp"),
        P("tp", "kv"),
    )
    return jax.shard_map(
        body,
        mesh=mesh,
        in_specs=placed,
        out_specs=(P(None, "kv"), P("kv", "tp", None, None)),
        check_vma=False,
    )
```

```python
import functools

import jax
import jax.numpy as jnp
from jax import lax
from jax.experimental import pallas as pl
from jax.experimental.pallas import tpu as pltpu
from jax.sharding import PartitionSpec as P

MODEL = 2048
HEADS = 16
EPS = 1e-06
NX = 4
F32 = jnp.float32
BF16 = jnp.bfloat16


def dot(a, b):
    return jnp.dot(a, b, preferred_element_type=F32)


def split(a):
    high = a.astype(BF16)
    return high, (a - high.astype(F32)).astype(BF16)


def dot_nt(a, b):
    return lax.dot_general(a, b, (((1,), (1,)), ((), ())), preferred_element_type=F32)


def dot2(a, b):
    bh, bl = split(b)
    return dot(a, bh) + dot(a, bl)


def iota(shape, dim):
    return lax.broadcasted_iota(jnp.int32, shape, dim)


def dot3(a, b):
    ah, al = split(a)
    bh, bl = split(b)
    n = a.shape[0]
    both = dot(jnp.concatenate([ah, al], axis=0), bh)
    return both[:n] + both[n:] + dot(ah, bl)


def apart(a, mask):
    return jnp.concatenate([a] * 4, axis=0) * mask


def dot3_blocks(a, b, mask):
    ah, al = split(a)
    bh, bl = split(b)
    both = dot(jnp.concatenate([ah, al], axis=0), apart(bh, mask))
    return both[:64] + both[64:] + dot(ah, apart(bl, mask))


def unit_inverse(lower, r, c, mask):
    def same(bits):
        return (r >> bits) == (c >> bits)

    ident = jnp.where(r == c, 1.0, 0.0)
    power = jnp.where(same(3), -lower, 0.0)
    total = ident + power
    for _ in range(2):
        power = dot3_blocks(power, power, mask)
        total = total + dot3_blocks(total, power, mask)
    for bits in (3, 4, 5):
        off = jnp.where(same(bits + 1) & jnp.logical_not(same(bits)), lower, 0.0)
        total = total - dot3_blocks(total, dot3_blocks(off, total, mask), mask)
    return total


def state_before(g, keys, vals, state, bbeta, bdecay, live, mask_ref):
    mask = mask_ref[...]
    r = iota((64, 256), 0)
    lane = iota((64, 256), 1)
    c = lane & 63
    pair = lane >> 6
    n0, n1 = live[2 * g] - 1, live[2 * g + 1] - 1
    lane1 = iota((1, 256), 1)
    live_row = (lane1 & 63) < jnp.where(lane1 < 128, n0, n1)
    d_row = jnp.where(live_row, bdecay[g], 0.0)
    b_row = jnp.where(live_row, bbeta[g], 0.0)
    r1 = iota((256, 128), 0)
    live_col = (r1 & 63) < jnp.where(r1 < 128, n0, n1)
    k_all = jnp.where(live_col, keys[pl.ds(2 * g, 2)].astype(F32).reshape(256, 128), 0.0)
    v_all = jnp.where(live_col, vals[pl.ds(2 * g, 2)].astype(F32).reshape(256, 128), 0.0)
    kb = k_all.astype(BF16)
    kt = k_all.T.astype(BF16)
    b_diag = jnp.where(r == c, b_row, 0.0)
    d_tri = jnp.where(c <= r, d_row, 0.0)
    b_col, t_col = [], []
    for p in range(4):
        b_col.append(jnp.sum(jnp.where(pair == p, b_diag, 0.0), axis=1, keepdims=True))
        t_col.append(jnp.sum(jnp.where(pair == p, d_tri, 0.0), axis=1, keepdims=True))

    def side(columns):
        low = jnp.where(pair == 0, columns[0], columns[1])
        high = jnp.where(pair == 2, columns[2], columns[3])
        return jnp.where(pair < 2, low, high)

    tots = side(t_col)
    tot_row = jnp.sum(jnp.where(r == c, tots, 0.0), axis=0, keepdims=True)
    strict = c < r
    fade = jnp.exp(jnp.where(strict, tots - tot_row, 0.0))
    gram = dot(kb, kt)
    gram = side([gram[64 * p : 64 * p + 64] for p in range(4)])
    lower = jnp.where(strict, side(b_col) * gram * fade, 0.0)
    inverse = unit_inverse(lower, r, c, mask)
    zero = jnp.zeros((64, 128), F32)

    def spread(blocks):
        rows = [[blocks[p] if q == p else zero for q in range(4)] for p in range(4)]
        return jnp.concatenate([jnp.concatenate(row, axis=1) for row in rows], axis=0)

    right = []
    for p in range(4):
        at = slice(64 * p, 64 * p + 64)
        seen = dot2(kb[at], state[2 * g + p // 2, p % 2])
        right.append(b_col[p] * (v_all[at] - jnp.exp(t_col[p]) * seen))
    update = dot3(inverse, spread(right))
    faded = []
    for p in range(4):
        faded.append(update[:, 128 * p : 128 * p + 128] * jnp.exp(t_col[p][63:64] - t_col[p]))
    added = dot2(kt, spread(faded))
    for p in range(4):
        end = jnp.exp(t_col[p][63:64])
        at = (2 * g + p // 2, p % 2)
        state[at] = end * state[at] + added[:, 128 * p : 128 * p + 128]


def kernel(
    tok_hbm,
    ngain_hbm,
    qw_hbm,
    kw_hbm,
    vw_hbm,
    gw_hbm,
    bw_hbm,
    dw_hbm,
    rate_hbm,
    hgain_hbm,
    state_hbm,
    keys_hbm,
    vals_hbm,
    bbeta_hbm,
    bdecay_hbm,
    live_hbm,
    out_hbm,
    mgain_hbm,
    up_hbm,
    down_hbm,
    mixed_ref,
    state,
    wst,
    wcat,
    bdw,
    tokx,
    gp,
    tokl,
    tokt,
    rate_ref,
    hgain_ref,
    bbeta_ref,
    bdecay_ref,
    live_ref,
    mgain_ref,
    proj_s,
    proj_r,
    ex_s,
    ex_r,
    keys,
    vals,
    mask,
    up_all,
    down_all,
    out_all,
    bbeta,
    bdecay,
    mh,
    ar,
    ax,
    rs,
    resid,
    fin_s,
    mx,
    loc,
    xs,
    xr,
    ts,
    tr,
    ps,
    pr,
    ms,
    mr,
    asem,
    arr,
    us,
    ur,
    ds_,
    dr,
    fs,
    fr,
    ring_s,
    ring_r,
    round_r,
    *,
    n_kv,
    n_tp,
):
    kv = lax.axis_index("kv")
    tp = lax.axis_index("tp")
    nz = n_kv // NX
    z = kv // NX
    x = kv % NX

    def local(src, dst, i):
        copy = pltpu.make_async_copy(src, dst, loc.at[i])
        copy.start()
        return copy

    def remote(src, dst, s, r, kv_to, tp_to):
        return pltpu.make_async_remote_copy(
            src_ref=src,
            dst_ref=dst,
            send_sem=s,
            recv_sem=r,
            device_id={"kv": kv_to, "tp": tp_to},
            device_id_type=pl.DeviceIdType.MESH,
        )

    in_tok = local(tok_hbm, tokx.at[x], 12)
    in_gain = local(ngain_hbm, gp.at[x], 13)
    in_w = [local(w, wst.at[i], i) for i, w in enumerate((qw_hbm, kw_hbm, vw_hbm, gw_hbm))]
    in_out = local(out_hbm, out_all.at[z], 6)
    in_up = local(up_hbm, up_all.at[z], 7)
    in_down = local(down_hbm, down_all.at[z], 8)
    lanes_z = pl.ds(pl.multiple_of(z * 256, 256), 256)
    in_b = [
        local(bw_hbm.at[:, lanes_z], bdw.at[0], 4),
        local(dw_hbm.at[:, lanes_z], bdw.at[1], 5),
    ]
    in_block = [
        local(bbeta_hbm, bbeta_ref, 14),
        local(bdecay_hbm, bdecay_ref, 15),
        local(live_hbm, live_ref, 16),
        local(keys_hbm, keys, 9),
        local(vals_hbm, vals, 10),
        local(state_hbm, state, 11),
    ]
    in_small = [
        local(rate_hbm, rate_ref, 17),
        local(hgain_hbm, hgain_ref, 18),
        local(mgain_hbm, mgain_ref, 19),
    ]

    up_z = ((z + 1) % nz) * NX + x
    down_z = ((z + nz - 1) % nz) * NX + x
    barrier = pltpu.get_barrier_semaphore()

    def greet(sem, kv_to, tp_to):
        pl.semaphore_signal(
            sem,
            inc=1,
            device_id={"kv": kv_to, "tp": tp_to},
            device_id_type=pl.DeviceIdType.MESH,
        )

    near_z = [((z + d) % nz) * NX + x for d in (1, nz - 1, 2, nz - 2)]
    for to in near_z:
        greet(barrier, to, tp)
    for d in range(1, NX):
        greet(barrier, z * NX + (x + d) % NX, tp)

    def greet_tp(d, carry):
        greet(barrier, kv, (tp + d) % n_tp)
        return carry

    lax.fori_loop(1, n_tp, greet_tp, 0)

    def round_send(i):
        for to in near_z:
            greet(round_r.at[i], to, tp)

    def round_wait(i):
        pl.semaphore_wait(round_r.at[i], 4)

    mask[...] = jnp.where((iota((256, 256), 0) >> 6) == (iota((256, 256), 1) >> 6), 1.0, 0.0).astype(
        BF16
    )
    in_tok.wait()
    in_gain.wait()
    tokl[...] = tokx[x].astype(F32).T.astype(BF16)
    tokt[z] = tokl[pl.ds(pl.multiple_of(z * 32, 32), 32), :]
    for copy in in_w:
        copy.wait()
    mine = pl.ds(pl.multiple_of(x * 64, 64), 64)
    wcat[mine, :] = wst[x]
    in_out.wait()
    in_up.wait()
    in_down.wait()

    pl.semaphore_wait(barrier, 4 + NX - 1 + n_tp - 1)

    sent_x = []
    for d in range(1, NX):
        to = (x + d) % NX
        peer = z * NX + to
        sent_x.append(remote(tokx.at[x], tokx.at[x], xs.at[0, d], xr.at[0, d], peer, tp))
        sent_x.append(remote(gp.at[x], gp.at[x], xs.at[1, d], xr.at[1, d], peer, tp))
        sent_x.append(
            remote(wst.at[to], wcat.at[mine, :], xs.at[2, d], xr.at[2, d], peer, tp)
        )
    for copy in sent_x:
        copy.start()

    sent_t = []
    for d in range(1, nz):
        to = (z + d) % nz
        sent_t.append(
            remote(
                tokl.at[pl.ds(pl.multiple_of(to * 32, 32), 32), :],
                tokt.at[z],
                ts.at[d],
                tr.at[d],
                to * NX + x,
                tp,
            )
        )
    def ring(way, step, what):
        to = up_z if way == 0 else down_z
        block = (z + nz - (step - 1)) % nz if way == 0 else (z + step - 1) % nz
        ref = (out_all, up_all, down_all, down_all)[what].at[block]
        first, rows = (0, 64) if what < 2 else (32 * (what - 2), 32)
        if step == nz // 2:
            first, rows = first + rows // 2 * way, rows // 2
        ref = ref.at[pl.ds(first, rows)]
        return remote(
            ref, ref, ring_s.at[way, step - 1, what], ring_r.at[way, step - 1, what], to, tp
        )

    half = nz // 2

    def ring_start(step, what):
        for way in range(2):
            ring(way, step, what).start()

    def ring_pass(step, what):
        for way in range(2):
            ring(way, step, what).wait_recv()
            if step < half:
                ring(way, step + 1, what).start()

    OUT, UP, LOW, HIGH = 0, 1, 2, 3

    round_send(0)
    ring_start(1, OUT)
    ring_start(1, UP)
    ring_start(1, LOW)

    for copy in in_block:
        copy.wait()
    for i in range(4):
        pairs = [(2 * i + j // 2, slice(j % 2, j % 2 + 1)) for j in range(4)]
        bbeta[i] = jnp.concatenate([bbeta_ref[pair] for pair in pairs], axis=1)
        bdecay[i] = jnp.concatenate([bdecay_ref[pair] for pair in pairs], axis=1)

    def before(g, carry):
        state_before(g, keys, vals, state, bbeta, bdecay, live_ref, mask)
        return carry

    lax.fori_loop(0, 1, before, 0)
    round_wait(0)
    round_send(1)
    ring_pass(1, OUT)
    lax.fori_loop(1, 2, before, 0)

    for copy in sent_x:
        copy.wait_recv()
    t = tokx[...].reshape(256, 256).astype(F32).T
    squares = jnp.sum(t * t, axis=1, keepdims=True)
    normed = (t * jnp.concatenate([gp[i] for i in range(NX)], axis=1)).astype(BF16)
    projected = dot(normed, wcat[...])
    for copy in in_b:
        copy.wait()
    small = jnp.concatenate(
        [bdw[...].astype(F32).reshape(32, 256), jnp.zeros((96, 256), F32)], axis=0
    ).astype(BF16)
    extra = dot_nt(normed, small)
    proj_s[...] = projected.reshape(n_kv, 8, 256).astype(BF16)
    lane = iota((256, 128), 1)
    high = squares.astype(BF16).astype(F32)
    extra = jnp.where(lane == 32, high, jnp.where(lane == 33, squares - high, extra))
    ex_s[...] = extra.reshape(n_kv, 8, 128).astype(BF16)
    proj_r[kv] = proj_s[kv]
    ex_r[z] = ex_s[kv]

    def send_proj(d, carry):
        far = d // NX
        far = nz // 2 + (far + 1) // 2 * (1 - 2 * (far % 2))
        to = ((z + far) % nz) * NX + (x + NX - 1 - d % NX) % NX
        remote(proj_s.at[to], proj_r.at[kv], ps.at[0], pr.at[0], to, tp).start()
        return carry

    def send_extra(d, carry):
        to = ((z + d) % nz) * NX + x
        remote(ex_s.at[to], ex_r.at[z], ps.at[1], pr.at[1], to, tp).start()
        return carry

    round_wait(1)
    lax.fori_loop(1, nz, send_extra, 0)
    lax.fori_loop(0, n_kv - 1, send_proj, 0)
    ring_pass(1, UP)
    lax.fori_loop(2, 3, before, 0)
    ring_pass(2, OUT)
    ring_pass(1, LOW)
    ring_start(1, HIGH)
    lax.fori_loop(3, 4, before, 0)
    ring_pass(3, OUT)
    ring_pass(2, UP)
    for copy in sent_t:
        copy.start()

    some = pl.ds(0, n_kv - 1)
    few = pl.ds(0, nz - 1)
    all_proj = remote(proj_s.at[some], proj_r.at[some], ps.at[0], pr.at[0], kv, tp)
    all_extra = remote(ex_s.at[few], ex_r.at[few], ps.at[1], pr.at[1], kv, tp)
    all_extra.wait_recv()
    all_proj.wait_recv()

    for copy in in_small:
        copy.wait()
    total = jnp.sum(proj_r[...].astype(F32).reshape(nz, NX, 8, 256), axis=0)
    extra = jnp.sum(ex_r[...].astype(F32), axis=0)
    inverse_rms = lax.rsqrt((extra[:, 32:33] + extra[:, 33:34]) / MODEL + EPS)
    extra = extra * inverse_rms
    queries, key_raw, value_raw, gate_raw = [total[i] * inverse_rms for i in range(4)]
    lane = iota((8, 128), 1)
    cols, heads = [], []
    for h in range(2):
        at = slice(128 * h, 128 * h + 128)
        k = key_raw[:, at]
        k = k * lax.rsqrt(jnp.sum(k * k, axis=1, keepdims=True) + EPS)
        k = k.astype(BF16).astype(F32)
        v = value_raw[:, at].astype(BF16).astype(F32)
        q = queries[:, at]
        b = jnp.sum(jnp.where(lane == 2 * tp + h, extra, 0.0), axis=1, keepdims=True)
        b = 1.0 / (1.0 + jnp.exp(-b))
        a = jnp.sum(jnp.where(lane == HEADS + 2 * tp + h, extra, 0.0), axis=1, keepdims=True)
        a = jnp.maximum(a, 0.0) + jnp.log1p(jnp.exp(-jnp.abs(a)))
        e = jnp.exp(-rate_ref[h] * a)
        qk = jnp.sum(q * k, axis=1, keepdims=True)
        cols += [k, q]
        heads.append((k, v, q, b, e, qk))
    columns = jnp.concatenate(cols + [jnp.zeros((96, 128), F32)], axis=0).T
    updates, readouts = {}, []
    for h in range(2):
        k, v, q, b, e, qk = heads[h]
        lines = []
        for s in range(8):
            old = state[s, h]
            one = slice(s, s + 1)
            kcol = columns[:, 16 * h + s : 16 * h + s + 1]
            qcol = columns[:, 16 * h + 8 + s : 16 * h + 9 + s]
            ks = jnp.sum(old * kcol, axis=0, keepdims=True)
            qs = jnp.sum(old * qcol, axis=0, keepdims=True)
            u = b[one] * (v[one] - e[one] * ks)
            updates[s, h] = u
            lines.append(e[one] * qs + qk[one] * u)
        readouts.append(jnp.concatenate(lines, axis=0))
    gated = []
    for h in range(2):
        rd = readouts[h]
        gate = gate_raw[:, 128 * h : 128 * h + 128]
        scaled = rd * lax.rsqrt(jnp.sum(rd * rd, axis=1, keepdims=True) / 128 + EPS) * hgain_ref[...]
        gated.append(scaled * (gate / (1.0 + jnp.exp(-gate))))
    mh[x] = jnp.concatenate(gated, axis=1).astype(BF16).astype(F32)
    sent_m = []
    for d in range(1, NX):
        peer = z * NX + (x + d) % NX
        sent_m.append(remote(mh.at[x], mh.at[x], ms.at[d], mr.at[d], peer, tp))
    for copy in sent_m:
        copy.start()
    ring_pass(2, LOW)
    for h in range(2):
        e = heads[h][4]
        for s in range(8):
            kcol = columns[:, 16 * h + s : 16 * h + s + 1]
            state[s, h] = e[s : s + 1] * state[s, h] + kcol * updates[s, h]

    ring_pass(1, HIGH)

    for copy in sent_m:
        copy.wait_recv()
    ring_pass(4, OUT)
    m = mh[...].reshape(32, 256)
    ar[tp] = dot_nt(m.astype(BF16), out_all[...].reshape(nz * 64, 256)).astype(BF16)

    def send_ar(d, carry):
        to = (tp + d) % n_tp
        remote(ar.at[tp], ar.at[tp], asem, arr, kv, to).start()
        return carry

    lax.fori_loop(1, n_tp, send_ar, 0)
    ring_pass(3, UP)
    tps = pl.ds(0, n_tp - 1)
    all_ar = remote(ar.at[tps], ar.at[tps], asem, arr, kv, tp)
    for copy in sent_t:
        copy.wait_recv()
    tokens = jnp.concatenate([tokt[i].astype(F32) for i in range(nz)], axis=1)
    gains = []
    for p in range(nz):
        gain = mgain_ref[pl.ds(2 * p + x // 2, 1), :]
        gains.append(jnp.where(x % 2 == 0, gain[:, :64], gain[:, 64:]))
    gains = jnp.concatenate(gains, axis=1)
    ring_pass(3, LOW)
    all_ar.wait_recv()
    ring_pass(2, HIGH)

    attended = jnp.sum(ar[...].astype(F32), axis=0)
    residual = (tokens + attended).astype(BF16).astype(F32)
    resid[...] = residual
    squares = jnp.sum(residual * residual, axis=1, keepdims=True)
    mlp_in = (residual * gains).astype(BF16)
    ring_pass(4, UP)
    pre = dot(mlp_in, up_all[...].reshape(nz * 64, 1024))
    high = squares.astype(BF16).astype(F32)
    lane = iota((32, 128), 1)
    tail = jnp.where(lane == 0, high, jnp.where(lane == 1, squares - high, 0.0))
    ax[x] = jnp.concatenate([pre, tail], axis=1).astype(BF16)
    sent_u = []
    for d in range(1, NX):
        peer = z * NX + (x + d) % NX
        sent_u.append(remote(ax.at[x], ax.at[x], us.at[d], ur.at[d], peer, tp))
    for copy in sent_u:
        copy.start()
    ring_pass(3, HIGH)
    for copy in sent_u:
        copy.wait_recv()
    ring_pass(4, LOW)
    ring_pass(4, HIGH)
    total = jnp.sum(ax[...].astype(F32), axis=0)
    rms = lax.rsqrt((total[:, 1024:1025] + total[:, 1025:1026]) / MODEL + EPS)
    hidden = jnp.maximum(total[:, :1024] * rms, 0.0)
    hidden = (hidden * hidden).astype(BF16)
    output = dot_nt(hidden, down_all[...].reshape(nz * 64, 1024))
    rs[tp] = output.astype(BF16)

    def send_rs(d, carry):
        to = (tp + d) % n_tp
        remote(rs.at[tp], rs.at[tp], ds_, dr, kv, to).start()
        return carry

    lax.fori_loop(1, n_tp, send_rs, 0)
    all_rs = remote(rs.at[tps], rs.at[tps], ds_, dr, kv, tp)
    all_rs.wait_recv()
    final = resid[...] + jnp.sum(rs[...].astype(F32), axis=0)
    for i in range(nz):
        fin_s[i] = final[:, 64 * i : 64 * i + 64].astype(BF16)
    mx[z] = fin_s[z]

    sent_f = []
    for d in range(1, nz):
        to = (z + d) % nz
        sent_f.append(remote(fin_s.at[to], mx.at[z], fs.at[d], fr.at[d], to * NX + x, tp))
    for copy in sent_f:
        copy.start()

    for copy in sent_x + sent_t + sent_m + sent_u + sent_f:
        copy.wait_send()
    for step in range(1, half + 1):
        for way in range(2):
            for what in (OUT, UP, LOW, HIGH):
                ring(way, step, what).wait_send()
    all_proj.wait_send()
    all_extra.wait_send()
    all_ar.wait_send()
    all_rs.wait_send()

    for copy in sent_f:
        copy.wait_recv()
    mixed_ref[...] = mx[...].astype(F32).reshape(nz * 32, 64).T.astype(BF16)


def put(mixed, state, mixed_hbm, state_hbm, sem):
    copies = [
        pltpu.make_async_copy(state, state_hbm, sem.at[0]),
        pltpu.make_async_copy(mixed, mixed_hbm, sem.at[1]),
    ]
    for copy in copies:
        copy.start()
    for copy in copies:
        copy.wait()


def body(
    tokens,
    norm_gain,
    query_weight,
    key_weight,
    value_weight,
    gate_weight,
    beta_weight,
    decay_weight,
    decay_rate,
    head_gain,
    carried_state,
    block_keys,
    block_values,
    block_beta,
    block_decay,
    live_count,
    out_weight,
    mlp_gain,
    up_weight,
    down_weight,
):
    n_kv = lax.axis_size("kv")
    n_tp = lax.axis_size("tp")
    nz = n_kv // NX
    vmem = pl.BlockSpec(memory_space=pltpu.VMEM)
    hbm = pl.BlockSpec(memory_space=pltpu.HBM)
    dma = pltpu.SemaphoreType.DMA
    operands = (
        tokens.T,
        norm_gain.reshape(1, -1),
        query_weight,
        key_weight,
        value_weight,
        gate_weight,
        beta_weight.T,
        decay_weight.T,
        decay_rate,
        head_gain.reshape(1, -1),
        carried_state,
        block_keys,
        block_values,
        block_beta,
        block_decay,
        live_count,
        out_weight.T,
        mlp_gain.reshape(-1, 128),
        up_weight,
        down_weight.T,
    )
    mixed, new_state = pl.pallas_call(
        functools.partial(kernel, n_kv=n_kv, n_tp=n_tp),
        out_shape=(
            jax.ShapeDtypeStruct(tokens.shape[::-1], BF16),
            jax.ShapeDtypeStruct(carried_state.shape, F32),
        ),
        in_specs=[hbm] * 20,
        out_specs=(vmem, vmem),
        scratch_shapes=[
            pltpu.VMEM((4, 64, 256), BF16),
            pltpu.VMEM((256, 256), BF16),
            pltpu.VMEM((2, 16, 256), BF16),
            pltpu.VMEM((NX, 64, 256), BF16),
            pltpu.VMEM((NX, 1, 64), F32),
            pltpu.VMEM((256, 64), BF16),
            pltpu.VMEM((nz, 32, 64), BF16),
            pltpu.SMEM((2,), F32),
            pltpu.VMEM((1, 128), F32),
            pltpu.VMEM((8, 2, 64), F32),
            pltpu.VMEM((8, 2, 64), F32),
            pltpu.SMEM((8,), jnp.int32),
            pltpu.VMEM((16, 128), F32),
            pltpu.VMEM((n_kv, 8, 256), BF16),
            pltpu.VMEM((n_kv, 8, 256), BF16),
            pltpu.VMEM((n_kv, 8, 128), BF16),
            pltpu.VMEM((nz, 8, 128), BF16),
            pltpu.VMEM((8, 2, 64, 128), BF16),
            pltpu.VMEM((8, 2, 64, 128), BF16),
            pltpu.VMEM((256, 256), BF16),
            pltpu.VMEM((nz, 64, 1024), BF16),
            pltpu.VMEM((nz, 64, 1024), BF16),
            pltpu.VMEM((nz, 64, 256), BF16),
            pltpu.VMEM((4, 1, 256), F32),
            pltpu.VMEM((4, 1, 256), F32),
            pltpu.VMEM((NX, 8, 256), F32),
            pltpu.VMEM((n_tp, 32, 512), BF16),
            pltpu.VMEM((NX, 32, 1152), BF16),
            pltpu.VMEM((n_tp, 32, 512), BF16),
            pltpu.VMEM((32, 512), F32),
            pltpu.VMEM((nz, 32, 64), BF16),
            pltpu.VMEM((nz, 32, 64), BF16),
            dma((20,)),
            dma((3, NX)),
            dma((3, NX)),
            dma((nz,)),
            dma((nz,)),
            dma((2,)),
            dma((2,)),
            dma((NX,)),
            dma((NX,)),
            dma,
            dma,
            dma((NX,)),
            dma((NX,)),
            dma,
            dma,
            dma((nz,)),
            dma((nz,)),
            dma((2, 4, 4)),
            dma((2, 4, 4)),
            pltpu.SemaphoreType.REGULAR((2,)),
        ],
        compiler_params=pltpu.CompilerParams(
            collective_id=0, has_side_effects=True, vmem_limit_bytes=40 * 1024 * 1024
        ),
        name="layer",
    )(*[pltpu.with_memory_space_constraint(a, pltpu.HBM) for a in operands])
    mixed, new_state = pl.pallas_call(
        put,
        out_shape=(
            jax.ShapeDtypeStruct(mixed.shape, BF16),
            jax.ShapeDtypeStruct(new_state.shape, F32),
        ),
        in_specs=[vmem, vmem],
        out_specs=(hbm, hbm),
        scratch_shapes=[dma((2,))],
        compiler_params=pltpu.CompilerParams(vmem_limit_bytes=16 * 1024 * 1024),
        name="put",
    )(mixed, new_state)
    return mixed.T, new_state


def solution(mesh):
    placed = (
        P(None, "kv"),
        P("kv"),
        P("kv", "tp"),
        P("kv", "tp"),
        P("kv", "tp"),
        P("kv", "tp"),
        P(),
        P(),
        P("tp"),
        P(),
        P("kv", "tp", None, None),
        P("kv", "tp", None, None),
        P("kv", "tp", None, None),
        P("kv", "tp", None),
        P("kv", "tp", None),
        P("kv"),
        P("tp", "kv"),
        P(),
        P("kv", "tp"),
        P("tp", "kv"),
    )
    return jax.shard_map(
        body,
        mesh=mesh,
        in_specs=placed,
        out_specs=(P(None, "kv"), P("kv", "tp", None, None)),
        check_vma=False,
    )
```

```python
import functools

import jax
import jax.numpy as jnp
from jax import lax
from jax.experimental import pallas as pl
from jax.experimental.pallas import tpu as pltpu
from jax.sharding import PartitionSpec as P

MODEL = 2048
HEADS = 16
EPS = 1e-06
NX = 4
F32 = jnp.float32
BF16 = jnp.bfloat16


def dot(a, b):
    return jnp.dot(a, b, preferred_element_type=F32)


def split(a):
    high = a.astype(BF16)
    return high, (a - high.astype(F32)).astype(BF16)


def dot_nt(a, b):
    return lax.dot_general(a, b, (((1,), (1,)), ((), ())), preferred_element_type=F32)


def dot2(a, b):
    bh, bl = split(b)
    return dot(a, bh) + dot(a, bl)


def iota(shape, dim):
    return lax.broadcasted_iota(jnp.int32, shape, dim)


def dot3(a, b):
    ah, al = split(a)
    bh, bl = split(b)
    n = a.shape[0]
    both = dot(jnp.concatenate([ah, al], axis=0), bh)
    return both[:n] + both[n:] + dot(ah, bl)


def apart(a, mask):
    return jnp.concatenate([a] * 4, axis=0) * mask


def dot3_blocks(a, b, mask):
    ah, al = split(a)
    bh, bl = split(b)
    both = dot(jnp.concatenate([ah, al], axis=0), apart(bh, mask))
    return both[:64] + both[64:] + dot(ah, apart(bl, mask))


def state_before(gs, between, keys, vals, state, bbeta, bdecay, live, mask_ref):
    r = iota((64, 256), 0)
    lane = iota((64, 256), 1)
    c = lane & 63
    pair = lane >> 6
    strict = c < r
    lane1 = iota((1, 256), 1)
    r1 = iota((256, 128), 0)
    zero = jnp.zeros((64, 128), F32)

    def side(columns):
        low = jnp.where(pair == 0, columns[0], columns[1])
        high = jnp.where(pair == 2, columns[2], columns[3])
        return jnp.where(pair < 2, low, high)

    def spread(blocks):
        rows = [[blocks[p] if q == p else zero for q in range(4)] for p in range(4)]
        return jnp.concatenate([jnp.concatenate(row, axis=1) for row in rows], axis=0)

    def prepare(g):
        n0, n1 = live[2 * g] - 1, live[2 * g + 1] - 1
        live_row = (lane1 & 63) < jnp.where(lane1 < 128, n0, n1)
        d_row = jnp.where(live_row, bdecay[g], 0.0)
        b_row = jnp.where(live_row, bbeta[g], 0.0)
        live_col = (r1 & 63) < jnp.where(r1 < 128, n0, n1)
        k_all = jnp.where(live_col, keys[2 * g : 2 * g + 2].astype(F32).reshape(256, 128), 0.0)
        kb = k_all.astype(BF16)
        kt = k_all.T.astype(BF16)
        b_diag = jnp.where(r == c, b_row, 0.0)
        d_tri = jnp.where(c <= r, d_row, 0.0)
        b_col, t_col = [], []
        for p in range(4):
            b_col.append(jnp.sum(jnp.where(pair == p, b_diag, 0.0), axis=1, keepdims=True))
            t_col.append(jnp.sum(jnp.where(pair == p, d_tri, 0.0), axis=1, keepdims=True))
        tots = side(t_col)
        tot_row = jnp.sum(jnp.where(r == c, tots, 0.0), axis=0, keepdims=True)
        fade = jnp.exp(jnp.where(strict, tots - tot_row, 0.0))
        gram = dot(kb, kt)
        gram = side([gram[64 * p : 64 * p + 64] for p in range(4)])
        lower = jnp.where(strict, side(b_col) * gram * fade, 0.0)
        return kb, kt, live_col, b_col, t_col, lower

    def same(bits):
        return (r >> bits) == (c >> bits)

    prepared = [prepare(g) for g in gs]
    lowers = [one[5] for one in prepared]
    mask = mask_ref[...]
    ident = jnp.where(r == c, 1.0, 0.0)
    powers = [jnp.where(same(3), -lower, 0.0) for lower in lowers]
    totals = [ident + power for power in powers]
    for _ in range(2):
        powers = [dot3_blocks(power, power, mask) for power in powers]
        more = [dot3_blocks(total, power, mask) for total, power in zip(totals, powers)]
        totals = [total + one for total, one in zip(totals, more)]
    between()
    for bits in (3, 4, 5):
        off = same(bits + 1) & jnp.logical_not(same(bits))
        offs = [jnp.where(off, lower, 0.0) for lower in lowers]
        offs = [dot3_blocks(one, total, mask) for one, total in zip(offs, totals)]
        more = [dot3_blocks(total, one, mask) for one, total in zip(offs, totals)]
        totals = [total - one for total, one in zip(totals, more)]
    rights = []
    for g, (kb, _, live_col, b_col, t_col, _) in zip(gs, prepared):
        v_all = jnp.where(live_col, vals[2 * g : 2 * g + 2].astype(F32).reshape(256, 128), 0.0)
        right = []
        for p in range(4):
            at = slice(64 * p, 64 * p + 64)
            seen = dot2(kb[at], state[2 * g + p // 2, p % 2])
            right.append(b_col[p] * (v_all[at] - jnp.exp(t_col[p]) * seen))
        rights.append(spread(right))
    updates = [dot3(total, right) for total, right in zip(totals, rights)]
    added = []
    for update, (_, kt, _, _, t_col, _) in zip(updates, prepared):
        faded = []
        for p in range(4):
            faded.append(update[:, 128 * p : 128 * p + 128] * jnp.exp(t_col[p][63:64] - t_col[p]))
        added.append(dot2(kt, spread(faded)))
    for g, one, (_, _, _, _, t_col, _) in zip(gs, added, prepared):
        for p in range(4):
            end = jnp.exp(t_col[p][63:64])
            at = (2 * g + p // 2, p % 2)
            state[at] = end * state[at] + one[:, 128 * p : 128 * p + 128]


def kernel(
    tok_hbm,
    ngain_hbm,
    qw_hbm,
    kw_hbm,
    vw_hbm,
    gw_hbm,
    bw_hbm,
    dw_hbm,
    rate_hbm,
    hgain_hbm,
    state_hbm,
    keys_hbm,
    vals_hbm,
    bbeta_hbm,
    bdecay_hbm,
    live_hbm,
    out_hbm,
    mgain_hbm,
    up_hbm,
    down_hbm,
    mixed_ref,
    state,
    wst,
    wcat,
    bdw,
    tokx,
    gp,
    tokl,
    tokt,
    rate_ref,
    hgain_ref,
    bbeta_ref,
    bdecay_ref,
    live_ref,
    mgain_ref,
    proj_s,
    proj_r,
    ex_s,
    ex_r,
    keys,
    vals,
    mask,
    up_all,
    down_all,
    out_all,
    bbeta,
    bdecay,
    mh,
    ar,
    ax,
    rs,
    resid,
    fin_s,
    mx,
    loc,
    xs,
    xr,
    ts,
    tr,
    ps,
    pr,
    ms,
    mr,
    asem,
    arr,
    us,
    ur,
    ds_,
    dr,
    fs,
    fr,
    ring_s,
    ring_r,
    round_r,
    *,
    n_kv,
    n_tp,
):
    kv = lax.axis_index("kv")
    tp = lax.axis_index("tp")
    nz = n_kv // NX
    z = kv // NX
    x = kv % NX

    def local(src, dst, i):
        copy = pltpu.make_async_copy(src, dst, loc.at[i])
        copy.start()
        return copy

    def remote(src, dst, s, r, kv_to, tp_to):
        return pltpu.make_async_remote_copy(
            src_ref=src,
            dst_ref=dst,
            send_sem=s,
            recv_sem=r,
            device_id={"kv": kv_to, "tp": tp_to},
            device_id_type=pl.DeviceIdType.MESH,
        )

    up_z = ((z + 1) % nz) * NX + x
    down_z = ((z + nz - 1) % nz) * NX + x
    barrier = pltpu.get_barrier_semaphore()

    def greet(sem, kv_to, tp_to):
        pl.semaphore_signal(
            sem,
            inc=1,
            device_id={"kv": kv_to, "tp": tp_to},
            device_id_type=pl.DeviceIdType.MESH,
        )

    near_z = [((z + d) % nz) * NX + x for d in (1, nz - 1, 2, nz - 2)]
    for to in near_z:
        greet(barrier, to, tp)
    for d in range(1, NX):
        greet(barrier, z * NX + (x + d) % NX, tp)

    def greet_tp(d, carry):
        greet(barrier, kv, (tp + d) % n_tp)
        return carry

    lax.fori_loop(1, n_tp, greet_tp, 0)

    in_tok = local(tok_hbm, tokx.at[x], 12)
    in_gain = local(ngain_hbm, gp.at[x], 13)
    in_w = [local(w, wst.at[i], i) for i, w in enumerate((qw_hbm, kw_hbm, vw_hbm, gw_hbm))]
    in_out = local(out_hbm, out_all.at[z], 6)
    in_up = local(up_hbm, up_all.at[z], 7)
    in_down = local(down_hbm, down_all.at[z], 8)
    lanes_z = pl.ds(pl.multiple_of(z * 256, 256), 256)
    in_b = [
        local(bw_hbm.at[:, lanes_z], bdw.at[0], 4),
        local(dw_hbm.at[:, lanes_z], bdw.at[1], 5),
    ]
    in_block = [
        local(bbeta_hbm, bbeta_ref, 14),
        local(bdecay_hbm, bdecay_ref, 15),
        local(live_hbm, live_ref, 16),
        local(keys_hbm, keys, 9),
        local(vals_hbm, vals, 10),
        local(state_hbm, state, 11),
    ]
    in_small = [
        local(rate_hbm, rate_ref, 17),
        local(hgain_hbm, hgain_ref, 18),
        local(mgain_hbm, mgain_ref, 19),
    ]

    def round_send(i):
        for to in near_z:
            greet(round_r.at[i], to, tp)

    def round_wait(i):
        pl.semaphore_wait(round_r.at[i], 4)

    in_tok.wait()
    in_gain.wait()
    for copy in in_w:
        copy.wait()
    mine = pl.ds(pl.multiple_of(x * 64, 64), 64)
    pl.semaphore_wait(barrier, 4 + NX - 1 + n_tp - 1)

    sent_x = []
    for d in range(1, NX):
        to = (x + d) % NX
        peer = z * NX + to
        sent_x.append(remote(tokx.at[x], tokx.at[x], xs.at[0, d], xr.at[0, d], peer, tp))
        sent_x.append(remote(gp.at[x], gp.at[x], xs.at[1, d], xr.at[1, d], peer, tp))
        sent_x.append(
            remote(wst.at[to], wcat.at[mine, :], xs.at[2, d], xr.at[2, d], peer, tp)
        )
    for copy in sent_x:
        copy.start()

    sent_t = []
    for d in range(1, nz):
        to = (z + d) % nz
        part = tokl.at[pl.ds(pl.multiple_of(to * 32, 32), 32), :]
        sent_t.append(remote(part, tokt, ts.at[d], tr, to * NX + x, tp))

    def ring(way, step, what):
        to = up_z if way == 0 else down_z
        block = (z + nz - (step - 1)) % nz if way == 0 else (z + step - 1) % nz
        ref = (out_all, up_all, down_all, down_all)[what].at[block]
        first, rows = (0, 64) if what < 2 else (32 * (what - 2), 32)
        if step == nz // 2:
            first, rows = first + rows // 2 * way, rows // 2
        ref = ref.at[pl.ds(first, rows)]
        return remote(
            ref, ref, ring_s.at[way, step - 1, what], ring_r.at[way, step - 1, what], to, tp
        )

    half = nz // 2

    def ring_start(step, what):
        for way in range(2):
            ring(way, step, what).start()

    def ring_pass(step, what):
        for way in range(2):
            ring(way, step, what).wait_recv()
            if step < half:
                ring(way, step + 1, what).start()

    OUT, UP, LOW, HIGH = 0, 1, 2, 3

    round_send(0)
    in_out.wait()
    in_up.wait()
    in_down.wait()
    ring_start(1, OUT)
    ring_start(1, UP)
    ring_start(1, LOW)

    for copy in in_block:
        copy.wait()
    for i in range(4):
        pairs = [(2 * i + j // 2, slice(j % 2, j % 2 + 1)) for j in range(4)]
        bbeta[i] = jnp.concatenate([bbeta_ref[pair] for pair in pairs], axis=1)
        bdecay[i] = jnp.concatenate([bdecay_ref[pair] for pair in pairs], axis=1)

    mask[...] = jnp.where((iota((256, 256), 0) >> 6) == (iota((256, 256), 1) >> 6), 1.0, 0.0).astype(
        BF16
    )
    wcat[mine, :] = wst[x]
    tokl[...] = tokx[x].astype(F32).T.astype(BF16)

    @pl.when(z == tp)
    def _():
        tokt[...] = tokl[pl.ds(pl.multiple_of(z * 32, 32), 32), :]


    def before(gs, between):
        state_before(gs, between, keys, vals, state, bbeta, bdecay, live_ref, mask)

    def early():
        round_wait(0)
        round_send(1)
        ring_pass(1, OUT)

    before((0, 1), early)

    for copy in sent_x:
        copy.wait_recv()
    t = tokx[...].reshape(256, 256).astype(F32).T
    squares = jnp.sum(t * t, axis=1, keepdims=True)
    normed = (t * jnp.concatenate([gp[i] for i in range(NX)], axis=1)).astype(BF16)
    projected = dot(normed, wcat[...])
    for copy in in_b:
        copy.wait()
    small = jnp.concatenate(
        [bdw[...].astype(F32).reshape(32, 256), jnp.zeros((96, 256), F32)], axis=0
    ).astype(BF16)
    extra = dot_nt(normed, small)
    proj_s[...] = projected.reshape(n_kv, 8, 256).astype(BF16)
    lane = iota((256, 128), 1)
    high = squares.astype(BF16).astype(F32)
    extra = jnp.where(lane == 32, high, jnp.where(lane == 33, squares - high, extra))
    ex_s[...] = extra.reshape(n_kv, 8, 128).astype(BF16)
    proj_r[kv] = proj_s[kv]
    ex_r[z] = ex_s[kv]

    sent_p = []
    for far in (4, 3, 5, 2, 6, 1, 7, 0):
        row = ((z + far) % nz) * NX
        for side in range(NX):
            if far or side:
                to = row + (x + side) % NX
                sent_p.append(remote(proj_s.at[to], proj_r.at[kv], ps.at[0], pr.at[0], to, tp))

    def send_extra(d, carry):
        to = ((z + d) % nz) * NX + x
        remote(ex_s.at[to], ex_r.at[z], ps.at[1], pr.at[1], to, tp).start()
        return carry

    round_wait(1)
    lax.fori_loop(1, nz, send_extra, 0)
    for copy in sent_p:
        copy.start()
    ring_pass(2, OUT)
    ring_pass(1, UP)
    ring_start(1, HIGH)
    before((2, 3), lambda: None)

    @pl.when(z == tp)
    def _():
        for copy in sent_t:
            copy.start()

    ring_pass(3, OUT)
    ring_pass(1, LOW)

    some = pl.ds(0, n_kv - 1)
    few = pl.ds(0, nz - 1)
    all_proj = remote(proj_s.at[some], proj_r.at[some], ps.at[0], pr.at[0], kv, tp)
    all_extra = remote(ex_s.at[few], ex_r.at[few], ps.at[1], pr.at[1], kv, tp)
    all_extra.wait_recv()
    all_proj.wait_recv()

    for copy in in_small:
        copy.wait()
    total = jnp.sum(proj_r[...].astype(F32).reshape(nz, NX, 8, 256), axis=0)
    extra = jnp.sum(ex_r[...].astype(F32), axis=0)
    inverse_rms = lax.rsqrt((extra[:, 32:33] + extra[:, 33:34]) / MODEL + EPS)
    extra = extra * inverse_rms
    queries, key_raw, value_raw, gate_raw = [total[i] * inverse_rms for i in range(4)]
    lane = iota((8, 128), 1)
    cols, heads = [], []
    for h in range(2):
        at = slice(128 * h, 128 * h + 128)
        k = key_raw[:, at]
        k = k * lax.rsqrt(jnp.sum(k * k, axis=1, keepdims=True) + EPS)
        k = k.astype(BF16).astype(F32)
        v = value_raw[:, at].astype(BF16).astype(F32)
        q = queries[:, at]
        b = jnp.sum(jnp.where(lane == 2 * tp + h, extra, 0.0), axis=1, keepdims=True)
        b = 1.0 / (1.0 + jnp.exp(-b))
        a = jnp.sum(jnp.where(lane == HEADS + 2 * tp + h, extra, 0.0), axis=1, keepdims=True)
        a = jnp.maximum(a, 0.0) + jnp.log1p(jnp.exp(-jnp.abs(a)))
        e = jnp.exp(-rate_ref[h] * a)
        qk = jnp.sum(q * k, axis=1, keepdims=True)
        cols += [k, q]
        heads.append((k, v, q, b, e, qk))
    columns = jnp.concatenate(cols + [jnp.zeros((96, 128), F32)], axis=0).T
    updates, readouts = {}, []
    for h in range(2):
        k, v, q, b, e, qk = heads[h]
        lines = []
        for s in range(8):
            old = state[s, h]
            one = slice(s, s + 1)
            kcol = columns[:, 16 * h + s : 16 * h + s + 1]
            qcol = columns[:, 16 * h + 8 + s : 16 * h + 9 + s]
            ks = jnp.sum(old * kcol, axis=0, keepdims=True)
            qs = jnp.sum(old * qcol, axis=0, keepdims=True)
            u = b[one] * (v[one] - e[one] * ks)
            updates[s, h] = u
            lines.append(e[one] * qs + qk[one] * u)
        readouts.append(jnp.concatenate(lines, axis=0))
    gated = []
    for h in range(2):
        rd = readouts[h]
        gate = gate_raw[:, 128 * h : 128 * h + 128]
        scaled = rd * lax.rsqrt(jnp.sum(rd * rd, axis=1, keepdims=True) / 128 + EPS) * hgain_ref[...]
        gated.append(scaled * (gate / (1.0 + jnp.exp(-gate))))
    mh[x] = jnp.concatenate(gated, axis=1).astype(BF16).astype(F32)
    sent_m = []
    for d in range(1, NX):
        peer = z * NX + (x + d) % NX
        sent_m.append(remote(mh.at[x], mh.at[x], ms.at[d], mr.at[d], peer, tp))
    for copy in sent_m:
        copy.start()
    ring_pass(2, UP)
    for h in range(2):
        e = heads[h][4]
        for s in range(8):
            kcol = columns[:, 16 * h + s : 16 * h + s + 1]
            state[s, h] = e[s : s + 1] * state[s, h] + kcol * updates[s, h]

    ring_pass(1, HIGH)

    for copy in sent_m:
        copy.wait_recv()
    ring_pass(4, OUT)
    m = mh[...].reshape(32, 256)
    partial = dot_nt(m.astype(BF16), out_all[...].reshape(nz * 64, 256))

    @pl.when(z != tp)
    def _():
        sent_t[0].wait_recv()

    tokens = jnp.concatenate([tokt[...].astype(F32)] * nz, axis=1)
    partial = partial + jnp.where((iota((32, 64 * nz), 1) >> 6) == tp, tokens, 0.0)
    ar[tp] = partial.astype(BF16)

    def send_ar(d, carry):
        to = (tp + d) % n_tp
        remote(ar.at[tp], ar.at[tp], asem, arr, kv, to).start()
        return carry

    lax.fori_loop(1, n_tp, send_ar, 0)
    ring_pass(3, UP)
    tps = pl.ds(0, n_tp - 1)
    all_ar = remote(ar.at[tps], ar.at[tps], asem, arr, kv, tp)
    gains = []
    for p in range(nz):
        gain = mgain_ref[pl.ds(2 * p + x // 2, 1), :]
        gains.append(jnp.where(x % 2 == 0, gain[:, :64], gain[:, 64:]))
    gains = jnp.concatenate(gains, axis=1)
    ring_pass(2, LOW)
    all_ar.wait_recv()
    ring_pass(2, HIGH)

    attended = jnp.sum(ar[...].astype(F32), axis=0)
    residual = attended.astype(BF16).astype(F32)
    resid[...] = residual
    squares = jnp.sum(residual * residual, axis=1, keepdims=True)
    mlp_in = (residual * gains).astype(BF16)
    ring_pass(4, UP)
    pre = dot(mlp_in, up_all[...].reshape(nz * 64, 1024))
    high = squares.astype(BF16).astype(F32)
    lane = iota((32, 128), 1)
    tail = jnp.where(lane == 0, high, jnp.where(lane == 1, squares - high, 0.0))
    ax[x] = jnp.concatenate([pre, tail], axis=1).astype(BF16)
    sent_u = []
    for d in range(1, NX):
        peer = z * NX + (x + d) % NX
        sent_u.append(remote(ax.at[x], ax.at[x], us.at[d], ur.at[d], peer, tp))
    for copy in sent_u:
        copy.start()
    ring_pass(3, LOW)
    ring_pass(3, HIGH)
    for copy in sent_u:
        copy.wait_recv()
    ring_pass(4, LOW)
    ring_pass(4, HIGH)
    total = jnp.sum(ax[...].astype(F32), axis=0)
    rms = lax.rsqrt((total[:, 1024:1025] + total[:, 1025:1026]) / MODEL + EPS)
    hidden = jnp.maximum(total[:, :1024] * rms, 0.0)
    hidden = (hidden * hidden).astype(BF16)
    output = dot_nt(hidden, down_all[...].reshape(nz * 64, 1024))
    rs[tp] = output.astype(BF16)

    def send_rs(d, carry):
        to = (tp + d) % n_tp
        remote(rs.at[tp], rs.at[tp], ds_, dr, kv, to).start()
        return carry

    lax.fori_loop(1, n_tp, send_rs, 0)
    all_rs = remote(rs.at[tps], rs.at[tps], ds_, dr, kv, tp)
    for copy in sent_x + sent_m + sent_u:
        copy.wait_send()

    @pl.when(z == tp)
    def _():
        for copy in sent_t:
            copy.wait_send()

    for step in range(1, half + 1):
        for way in range(2):
            for what in (OUT, UP, LOW, HIGH):
                ring(way, step, what).wait_send()
    all_proj.wait_send()
    all_extra.wait_send()
    all_ar.wait_send()

    all_rs.wait_recv()
    final = resid[...] + jnp.sum(rs[...].astype(F32), axis=0)
    for i in range(nz):
        fin_s[i] = final[:, 64 * i : 64 * i + 64].astype(BF16)
    mx[z] = fin_s[z]

    sent_f = []
    for d in range(1, nz):
        to = (z + d) % nz
        sent_f.append(remote(fin_s.at[to], mx.at[z], fs.at[d], fr.at[d], to * NX + x, tp))
    for copy in sent_f:
        copy.start()

    all_rs.wait_send()
    for copy in sent_f:
        copy.wait()
    mixed_ref[...] = mx[...].astype(F32).reshape(nz * 32, 64).T.astype(BF16)


def put(mixed, state, mixed_hbm, state_hbm, sem):
    copies = [pltpu.make_async_copy(mixed, mixed_hbm, sem.at[8])]
    for i in range(8):
        copies.append(pltpu.make_async_copy(state.at[i], state_hbm.at[i], sem.at[i]))
    for copy in copies:
        copy.start()
    for copy in copies:
        copy.wait()


def body(
    tokens,
    norm_gain,
    query_weight,
    key_weight,
    value_weight,
    gate_weight,
    beta_weight,
    decay_weight,
    decay_rate,
    head_gain,
    carried_state,
    block_keys,
    block_values,
    block_beta,
    block_decay,
    live_count,
    out_weight,
    mlp_gain,
    up_weight,
    down_weight,
):
    n_kv = lax.axis_size("kv")
    n_tp = lax.axis_size("tp")
    nz = n_kv // NX
    vmem = pl.BlockSpec(memory_space=pltpu.VMEM)
    hbm = pl.BlockSpec(memory_space=pltpu.HBM)
    dma = pltpu.SemaphoreType.DMA
    operands = (
        tokens.T,
        norm_gain.reshape(1, -1),
        query_weight,
        key_weight,
        value_weight,
        gate_weight,
        beta_weight.T,
        decay_weight.T,
        decay_rate,
        head_gain.reshape(1, -1),
        carried_state,
        block_keys,
        block_values,
        block_beta,
        block_decay,
        live_count,
        out_weight.T,
        mlp_gain.reshape(-1, 128),
        up_weight,
        down_weight.T,
    )
    mixed, new_state = pl.pallas_call(
        functools.partial(kernel, n_kv=n_kv, n_tp=n_tp),
        out_shape=(
            jax.ShapeDtypeStruct(tokens.shape[::-1], BF16),
            jax.ShapeDtypeStruct(carried_state.shape, F32),
        ),
        in_specs=[hbm] * 20,
        out_specs=(vmem, vmem),
        scratch_shapes=[
            pltpu.VMEM((4, 64, 256), BF16),
            pltpu.VMEM((256, 256), BF16),
            pltpu.VMEM((2, 16, 256), BF16),
            pltpu.VMEM((NX, 64, 256), BF16),
            pltpu.VMEM((NX, 1, 64), F32),
            pltpu.VMEM((256, 64), BF16),
            pltpu.VMEM((32, 64), BF16),
            pltpu.SMEM((2,), F32),
            pltpu.VMEM((1, 128), F32),
            pltpu.VMEM((8, 2, 64), F32),
            pltpu.VMEM((8, 2, 64), F32),
            pltpu.SMEM((8,), jnp.int32),
            pltpu.VMEM((16, 128), F32),
            pltpu.VMEM((n_kv, 8, 256), BF16),
            pltpu.VMEM((n_kv, 8, 256), BF16),
            pltpu.VMEM((n_kv, 8, 128), BF16),
            pltpu.VMEM((nz, 8, 128), BF16),
            pltpu.VMEM((8, 2, 64, 128), BF16),
            pltpu.VMEM((8, 2, 64, 128), BF16),
            pltpu.VMEM((256, 256), BF16),
            pltpu.VMEM((nz, 64, 1024), BF16),
            pltpu.VMEM((nz, 64, 1024), BF16),
            pltpu.VMEM((nz, 64, 256), BF16),
            pltpu.VMEM((4, 1, 256), F32),
            pltpu.VMEM((4, 1, 256), F32),
            pltpu.VMEM((NX, 8, 256), F32),
            pltpu.VMEM((n_tp, 32, 512), BF16),
            pltpu.VMEM((NX, 32, 1152), BF16),
            pltpu.VMEM((n_tp, 32, 512), BF16),
            pltpu.VMEM((32, 512), F32),
            pltpu.VMEM((nz, 32, 64), BF16),
            pltpu.VMEM((nz, 32, 64), BF16),
            dma((20,)),
            dma((3, NX)),
            dma((3, NX)),
            dma((nz,)),
            dma,
            dma((2,)),
            dma((2,)),
            dma((NX,)),
            dma((NX,)),
            dma,
            dma,
            dma((NX,)),
            dma((NX,)),
            dma,
            dma,
            dma((nz,)),
            dma((nz,)),
            dma((2, 4, 4)),
            dma((2, 4, 4)),
            pltpu.SemaphoreType.REGULAR((2,)),
        ],
        compiler_params=pltpu.CompilerParams(
            collective_id=0, has_side_effects=True, vmem_limit_bytes=40 * 1024 * 1024
        ),
        name="layer",
    )(*[pltpu.with_memory_space_constraint(a, pltpu.HBM) for a in operands])
    mixed, new_state = pl.pallas_call(
        put,
        out_shape=(
            jax.ShapeDtypeStruct(mixed.shape, BF16),
            jax.ShapeDtypeStruct(new_state.shape, F32),
        ),
        in_specs=[vmem, vmem],
        out_specs=(hbm, hbm),
        scratch_shapes=[dma((9,))],
        compiler_params=pltpu.CompilerParams(vmem_limit_bytes=16 * 1024 * 1024),
        name="put",
    )(mixed, new_state)
    return mixed.T, new_state


def solution(mesh):
    placed = (
        P(None, "kv"),
        P("kv"),
        P("kv", "tp"),
        P("kv", "tp"),
        P("kv", "tp"),
        P("kv", "tp"),
        P(),
        P(),
        P("tp"),
        P(),
        P("kv", "tp", None, None),
        P("kv", "tp", None, None),
        P("kv", "tp", None, None),
        P("kv", "tp", None),
        P("kv", "tp", None),
        P("kv"),
        P("tp", "kv"),
        P(),
        P("kv", "tp"),
        P("tp", "kv"),
    )
    return jax.shard_map(
        body,
        mesh=mesh,
        in_specs=placed,
        out_specs=(P(None, "kv"), P("kv", "tp", None, None)),
        check_vma=False,
    )
```

```python
import functools

import jax
import jax.numpy as jnp
from jax import lax
from jax.experimental import pallas as pl
from jax.experimental.pallas import tpu as pltpu
from jax.sharding import PartitionSpec as P

MODEL = 2048
HEADS = 16
EPS = 1e-06
NX = 4
F32 = jnp.float32
BF16 = jnp.bfloat16


def dot(a, b):
    return jnp.dot(a, b, preferred_element_type=F32)


def split(a):
    high = a.astype(BF16)
    return high, (a - high.astype(F32)).astype(BF16)


def dot_nt(a, b):
    return lax.dot_general(a, b, (((1,), (1,)), ((), ())), preferred_element_type=F32)


def dot2(a, b):
    bh, bl = split(b)
    return dot(a, bh) + dot(a, bl)


def iota(shape, dim):
    return lax.broadcasted_iota(jnp.int32, shape, dim)


def dot3(a, b):
    ah, al = split(a)
    bh, bl = split(b)
    n = a.shape[0]
    both = dot(jnp.concatenate([ah, al], axis=0), bh)
    return both[:n] + both[n:] + dot(ah, bl)


def apart(a, mask):
    return jnp.concatenate([a] * 4, axis=0) * mask


def dot3_blocks(a, b, mask):
    ah, al = split(a)
    bh, bl = split(b)
    both = dot(jnp.concatenate([ah, al], axis=0), apart(bh, mask))
    return both[:64] + both[64:] + dot(ah, apart(bl, mask))


def state_before(gs, between, keys, vals, state, bbeta, bdecay, live, mask_ref):
    r = iota((64, 256), 0)
    lane = iota((64, 256), 1)
    c = lane & 63
    pair = lane >> 6
    strict = c < r
    lane1 = iota((1, 256), 1)
    r1 = iota((256, 128), 0)
    zero = jnp.zeros((64, 128), F32)

    def side(columns):
        low = jnp.where(pair == 0, columns[0], columns[1])
        high = jnp.where(pair == 2, columns[2], columns[3])
        return jnp.where(pair < 2, low, high)

    def spread(blocks):
        rows = [[blocks[p] if q == p else zero for q in range(4)] for p in range(4)]
        return jnp.concatenate([jnp.concatenate(row, axis=1) for row in rows], axis=0)

    def prepare(g):
        n0, n1 = live[2 * g] - 1, live[2 * g + 1] - 1
        live_row = (lane1 & 63) < jnp.where(lane1 < 128, n0, n1)
        d_row = jnp.where(live_row, bdecay[g], 0.0)
        b_row = jnp.where(live_row, bbeta[g], 0.0)
        live_col = (r1 & 63) < jnp.where(r1 < 128, n0, n1)
        k_all = jnp.where(live_col, keys[2 * g : 2 * g + 2].astype(F32).reshape(256, 128), 0.0)
        kb = k_all.astype(BF16)
        kt = k_all.T.astype(BF16)
        b_diag = jnp.where(r == c, b_row, 0.0)
        d_tri = jnp.where(c <= r, d_row, 0.0)
        b_col, t_col = [], []
        for p in range(4):
            b_col.append(jnp.sum(jnp.where(pair == p, b_diag, 0.0), axis=1, keepdims=True))
            t_col.append(jnp.sum(jnp.where(pair == p, d_tri, 0.0), axis=1, keepdims=True))
        tots = side(t_col)
        tot_row = jnp.sum(jnp.where(r == c, tots, 0.0), axis=0, keepdims=True)
        fade = jnp.exp(jnp.where(strict, tots - tot_row, 0.0))
        gram = dot(kb, kt)
        gram = side([gram[64 * p : 64 * p + 64] for p in range(4)])
        lower = jnp.where(strict, side(b_col) * gram * fade, 0.0)
        return kb, kt, live_col, b_col, t_col, lower

    def same(bits):
        return (r >> bits) == (c >> bits)

    prepared = [prepare(g) for g in gs]
    lowers = [one[5] for one in prepared]
    mask = mask_ref[...]
    ident = jnp.where(r == c, 1.0, 0.0)
    powers = [jnp.where(same(3), -lower, 0.0) for lower in lowers]
    totals = [ident + power for power in powers]
    for _ in range(2):
        powers = [dot3_blocks(power, power, mask) for power in powers]
        more = [dot3_blocks(total, power, mask) for total, power in zip(totals, powers)]
        totals = [total + one for total, one in zip(totals, more)]
    between()
    for bits in (3, 4, 5):
        off = same(bits + 1) & jnp.logical_not(same(bits))
        offs = [jnp.where(off, lower, 0.0) for lower in lowers]
        offs = [dot3_blocks(one, total, mask) for one, total in zip(offs, totals)]
        more = [dot3_blocks(total, one, mask) for one, total in zip(offs, totals)]
        totals = [total - one for total, one in zip(totals, more)]
    rights = []
    for g, (kb, _, live_col, b_col, t_col, _) in zip(gs, prepared):
        v_all = jnp.where(live_col, vals[2 * g : 2 * g + 2].astype(F32).reshape(256, 128), 0.0)
        right = []
        for p in range(4):
            at = slice(64 * p, 64 * p + 64)
            seen = dot2(kb[at], state[2 * g + p // 2, p % 2])
            right.append(b_col[p] * (v_all[at] - jnp.exp(t_col[p]) * seen))
        rights.append(spread(right))
    updates = [dot3(total, right) for total, right in zip(totals, rights)]
    added = []
    for update, (_, kt, _, _, t_col, _) in zip(updates, prepared):
        faded = []
        for p in range(4):
            faded.append(update[:, 128 * p : 128 * p + 128] * jnp.exp(t_col[p][63:64] - t_col[p]))
        added.append(dot2(kt, spread(faded)))
    for g, one, (_, _, _, _, t_col, _) in zip(gs, added, prepared):
        for p in range(4):
            end = jnp.exp(t_col[p][63:64])
            at = (2 * g + p // 2, p % 2)
            state[at] = end * state[at] + one[:, 128 * p : 128 * p + 128]


def kernel(
    tok_hbm,
    ngain_hbm,
    qw_hbm,
    kw_hbm,
    vw_hbm,
    gw_hbm,
    bw_hbm,
    dw_hbm,
    rate_hbm,
    hgain_hbm,
    state_hbm,
    keys_hbm,
    vals_hbm,
    bbeta_hbm,
    bdecay_hbm,
    live_hbm,
    out_hbm,
    mgain_hbm,
    up_hbm,
    down_hbm,
    mixed_ref,
    state,
    wst,
    wcat,
    bdw,
    tokx,
    gp,
    tokl,
    tokt,
    rate_ref,
    hgain_ref,
    bbeta_ref,
    bdecay_ref,
    live_ref,
    mgain_ref,
    proj_s,
    proj_r,
    ex_s,
    ex_r,
    keys,
    vals,
    mask,
    up_all,
    down_all,
    out_all,
    bbeta,
    bdecay,
    mh,
    ar,
    ax,
    rs,
    resid,
    fin_s,
    mx,
    loc,
    xs,
    xr,
    ts,
    tr,
    ps,
    pr,
    ms,
    mr,
    asem,
    arr,
    us,
    ur,
    ds_,
    dr,
    fs,
    fr,
    ring_s,
    ring_r,
    round_r,
    *,
    n_kv,
    n_tp,
):
    kv = lax.axis_index("kv")
    tp = lax.axis_index("tp")
    nz = n_kv // NX
    z = kv // NX
    x = kv % NX

    def local(src, dst, i):
        copy = pltpu.make_async_copy(src, dst, loc.at[i])
        copy.start()
        return copy

    def remote(src, dst, s, r, kv_to, tp_to):
        return pltpu.make_async_remote_copy(
            src_ref=src,
            dst_ref=dst,
            send_sem=s,
            recv_sem=r,
            device_id={"kv": kv_to, "tp": tp_to},
            device_id_type=pl.DeviceIdType.MESH,
        )

    up_z = ((z + 1) % nz) * NX + x
    down_z = ((z + nz - 1) % nz) * NX + x
    barrier = pltpu.get_barrier_semaphore()

    def greet(sem, kv_to, tp_to):
        pl.semaphore_signal(
            sem,
            inc=1,
            device_id={"kv": kv_to, "tp": tp_to},
            device_id_type=pl.DeviceIdType.MESH,
        )

    near_z = [((z + d) % nz) * NX + x for d in (1, nz - 1, 2, nz - 2)]
    for to in near_z:
        greet(barrier, to, tp)
    for d in range(1, NX):
        greet(barrier, z * NX + (x + d) % NX, tp)

    def greet_tp(d, carry):
        greet(barrier, kv, (tp + d) % n_tp)
        return carry

    lax.fori_loop(1, n_tp, greet_tp, 0)

    in_tok = local(tok_hbm, tokx.at[x], 2)
    in_gain = local(ngain_hbm, gp.at[x], 3)
    in_w = [local(w, wst.at[i], 0) for i, w in enumerate((qw_hbm, kw_hbm, vw_hbm, gw_hbm))]
    in_out = local(out_hbm, out_all.at[z], 4)
    in_up = local(up_hbm, up_all.at[z], 5)
    in_down = local(down_hbm, down_all.at[z], 6)
    lanes_z = pl.ds(pl.multiple_of(z * 256, 256), 256)
    in_b = [
        local(bw_hbm.at[:, lanes_z], bdw.at[0], 1),
        local(dw_hbm.at[:, lanes_z], bdw.at[1], 1),
    ]
    in_block = [
        local(bbeta_hbm, bbeta_ref, 7),
        local(bdecay_hbm, bdecay_ref, 8),
        local(live_hbm, live_ref, 9),
        local(keys_hbm, keys, 10),
        local(vals_hbm, vals, 11),
        local(state_hbm, state, 12),
    ]
    in_small = [
        local(rate_hbm, rate_ref, 13),
        local(hgain_hbm, hgain_ref, 14),
        local(mgain_hbm, mgain_ref, 15),
    ]

    def round_send(i):
        for to in near_z:
            greet(round_r.at[i], to, tp)

    def round_wait(i):
        pl.semaphore_wait(round_r.at[i], 4)

    in_tok.wait()
    in_gain.wait()
    pltpu.make_async_copy(wst, wst, loc.at[0]).wait()
    mine = pl.ds(pl.multiple_of(x * 64, 64), 64)
    pl.semaphore_wait(barrier, 4 + NX - 1 + n_tp - 1)

    sent_x = []
    for d in range(1, NX):
        to = (x + d) % NX
        peer = z * NX + to
        sent_x.append(remote(tokx.at[x], tokx.at[x], xs.at[0], xr.at[0], peer, tp))
        sent_x.append(remote(gp.at[x], gp.at[x], xs.at[1], xr.at[1], peer, tp))
        sent_x.append(remote(wst.at[to], wcat.at[mine, :], xs.at[2], xr.at[2], peer, tp))
    for copy in sent_x:
        copy.start()

    sent_t = []
    for d in range(1, nz):
        to = (z + d) % nz
        part = tokl.at[pl.ds(pl.multiple_of(to * 32, 32), 32), :]
        sent_t.append(remote(part, tokt, ts, tr, to * NX + x, tp))

    def ring(way, step, what):
        to = up_z if way == 0 else down_z
        block = (z + nz - (step - 1)) % nz if way == 0 else (z + step - 1) % nz
        ref = (out_all, up_all, down_all, down_all)[what].at[block]
        first, rows = (0, 64) if what < 2 else (32 * (what - 2), 32)
        if step == nz // 2:
            first, rows = first + rows // 2 * way, rows // 2
        ref = ref.at[pl.ds(first, rows)]
        return remote(
            ref, ref, ring_s.at[min(what, 2)], ring_r.at[way, step - 1, what], to, tp
        )

    half = nz // 2

    def ring_start(step, what):
        for way in range(2):
            ring(way, step, what).start()

    def ring_pass(step, what):
        for way in range(2):
            ring(way, step, what).wait_recv()
            if step < half:
                ring(way, step + 1, what).start()

    OUT, UP, LOW, HIGH = 0, 1, 2, 3

    round_send(0)
    in_out.wait()
    in_up.wait()
    in_down.wait()
    ring_start(1, OUT)
    ring_start(1, UP)
    ring_start(1, LOW)

    for copy in in_block:
        copy.wait()
    for i in range(4):
        pairs = [(2 * i + j // 2, slice(j % 2, j % 2 + 1)) for j in range(4)]
        bbeta[i] = jnp.concatenate([bbeta_ref[pair] for pair in pairs], axis=1)
        bdecay[i] = jnp.concatenate([bdecay_ref[pair] for pair in pairs], axis=1)

    mask[...] = jnp.where((iota((256, 256), 0) >> 6) == (iota((256, 256), 1) >> 6), 1.0, 0.0).astype(
        BF16
    )
    wcat[mine, :] = wst[x]
    tokl[...] = tokx[x].astype(F32).T.astype(BF16)

    @pl.when(z == tp)
    def _():
        tokt[...] = tokl[pl.ds(pl.multiple_of(z * 32, 32), 32), :]


    def before(gs, between):
        state_before(gs, between, keys, vals, state, bbeta, bdecay, live_ref, mask)

    def early():
        round_wait(0)
        round_send(1)
        ring_pass(1, OUT)

    before((0, 1), early)

    three = pl.ds(0, NX - 1)

    def whole(ref, s, r):
        return remote(ref, ref, s, r, kv, tp)

    all_x = [
        whole(tokx.at[three], xs.at[0], xr.at[0]),
        whole(gp.at[three], xs.at[1], xr.at[1]),
        whole(wst.at[three], xs.at[2], xr.at[2]),
    ]
    for copy in all_x:
        copy.wait_recv()
    t = tokx[...].reshape(256, 256).astype(F32).T
    squares = jnp.sum(t * t, axis=1, keepdims=True)
    normed = (t * jnp.concatenate([gp[i] for i in range(NX)], axis=1)).astype(BF16)
    projected = dot(normed, wcat[...])
    pltpu.make_async_copy(bdw, bdw, loc.at[1]).wait()
    small = jnp.concatenate(
        [bdw[...].astype(F32).reshape(32, 256), jnp.zeros((96, 256), F32)], axis=0
    ).astype(BF16)
    extra = dot_nt(normed, small)
    proj_s[...] = projected.reshape(n_kv, 8, 256).astype(BF16)
    lane = iota((256, 128), 1)
    high = squares.astype(BF16).astype(F32)
    extra = jnp.where(lane == 32, high, jnp.where(lane == 33, squares - high, extra))
    ex_s[...] = extra.reshape(n_kv, 8, 128).astype(BF16)
    proj_r[kv] = proj_s[kv]
    ex_r[z] = ex_s[kv]

    sent_p = []
    for far in (4, 3, 5, 2, 6, 1, 7, 0):
        row = ((z + far) % nz) * NX
        for side in range(NX):
            if far or side:
                to = row + (x + side) % NX
                sent_p.append(remote(proj_s.at[to], proj_r.at[kv], ps.at[0], pr.at[0], to, tp))

    def send_extra(d, carry):
        to = ((z + d) % nz) * NX + x
        remote(ex_s.at[to], ex_r.at[z], ps.at[1], pr.at[1], to, tp).start()
        return carry

    round_wait(1)
    lax.fori_loop(1, nz, send_extra, 0)
    for copy in sent_p:
        copy.start()
    ring_pass(2, OUT)
    ring_pass(1, UP)
    ring_start(1, HIGH)
    before((2, 3), lambda: None)

    @pl.when(z == tp)
    def _():
        for copy in sent_t:
            copy.start()

    ring_pass(3, OUT)
    ring_pass(1, LOW)

    some = pl.ds(0, n_kv - 1)
    few = pl.ds(0, nz - 1)
    all_proj = remote(proj_s.at[some], proj_r.at[some], ps.at[0], pr.at[0], kv, tp)
    all_extra = remote(ex_s.at[few], ex_r.at[few], ps.at[1], pr.at[1], kv, tp)
    all_extra.wait_recv()
    all_proj.wait_recv()

    for copy in in_small:
        copy.wait()
    total = jnp.sum(proj_r[...].astype(F32).reshape(nz, NX, 8, 256), axis=0)
    extra = jnp.sum(ex_r[...].astype(F32), axis=0)
    inverse_rms = lax.rsqrt((extra[:, 32:33] + extra[:, 33:34]) / MODEL + EPS)
    extra = extra * inverse_rms
    queries, key_raw, value_raw, gate_raw = [total[i] * inverse_rms for i in range(4)]
    lane = iota((8, 128), 1)
    cols, heads = [], []
    for h in range(2):
        at = slice(128 * h, 128 * h + 128)
        k = key_raw[:, at]
        k = k * lax.rsqrt(jnp.sum(k * k, axis=1, keepdims=True) + EPS)
        k = k.astype(BF16).astype(F32)
        v = value_raw[:, at].astype(BF16).astype(F32)
        q = queries[:, at]
        b = jnp.sum(jnp.where(lane == 2 * tp + h, extra, 0.0), axis=1, keepdims=True)
        b = 1.0 / (1.0 + jnp.exp(-b))
        a = jnp.sum(jnp.where(lane == HEADS + 2 * tp + h, extra, 0.0), axis=1, keepdims=True)
        a = jnp.maximum(a, 0.0) + jnp.log1p(jnp.exp(-jnp.abs(a)))
        e = jnp.exp(-rate_ref[h] * a)
        qk = jnp.sum(q * k, axis=1, keepdims=True)
        cols += [k, q]
        heads.append((k, v, q, b, e, qk))
    columns = jnp.concatenate(cols + [jnp.zeros((96, 128), F32)], axis=0).T
    updates, readouts = {}, []
    for h in range(2):
        k, v, q, b, e, qk = heads[h]
        lines = []
        for s in range(8):
            old = state[s, h]
            one = slice(s, s + 1)
            kcol = columns[:, 16 * h + s : 16 * h + s + 1]
            qcol = columns[:, 16 * h + 8 + s : 16 * h + 9 + s]
            ks = jnp.sum(old * kcol, axis=0, keepdims=True)
            qs = jnp.sum(old * qcol, axis=0, keepdims=True)
            u = b[one] * (v[one] - e[one] * ks)
            updates[s, h] = u
            lines.append(e[one] * qs + qk[one] * u)
        readouts.append(jnp.concatenate(lines, axis=0))
    gated = []
    for h in range(2):
        rd = readouts[h]
        gate = gate_raw[:, 128 * h : 128 * h + 128]
        scaled = rd * lax.rsqrt(jnp.sum(rd * rd, axis=1, keepdims=True) / 128 + EPS) * hgain_ref[...]
        gated.append(scaled * (gate / (1.0 + jnp.exp(-gate))))
    mh[x] = jnp.concatenate(gated, axis=1).astype(BF16).astype(F32)
    sent_m = []
    for d in range(1, NX):
        peer = z * NX + (x + d) % NX
        sent_m.append(remote(mh.at[x], mh.at[x], ms, mr, peer, tp))
    for copy in sent_m:
        copy.start()
    ring_pass(2, UP)
    for h in range(2):
        e = heads[h][4]
        for s in range(8):
            kcol = columns[:, 16 * h + s : 16 * h + s + 1]
            state[s, h] = e[s : s + 1] * state[s, h] + kcol * updates[s, h]

    ring_pass(1, HIGH)

    all_m = whole(mh.at[three], ms, mr)
    all_m.wait_recv()
    ring_pass(4, OUT)
    m = mh[...].reshape(32, 256)
    partial = dot_nt(m.astype(BF16), out_all[...].reshape(nz * 64, 256))

    @pl.when(z != tp)
    def _():
        sent_t[0].wait_recv()

    tokens = jnp.concatenate([tokt[...].astype(F32)] * nz, axis=1)
    partial = partial + jnp.where((iota((32, 64 * nz), 1) >> 6) == tp, tokens, 0.0)
    ar[tp] = partial.astype(BF16)

    def send_ar(d, carry):
        to = (tp + d) % n_tp
        remote(ar.at[tp], ar.at[tp], asem, arr, kv, to).start()
        return carry

    lax.fori_loop(1, n_tp, send_ar, 0)
    ring_pass(3, UP)
    tps = pl.ds(0, n_tp - 1)
    all_ar = remote(ar.at[tps], ar.at[tps], asem, arr, kv, tp)
    gains = []
    for p in range(nz):
        gain = mgain_ref[pl.ds(2 * p + x // 2, 1), :]
        gains.append(jnp.where(x % 2 == 0, gain[:, :64], gain[:, 64:]))
    gains = jnp.concatenate(gains, axis=1)
    ring_pass(2, LOW)
    all_ar.wait_recv()
    ring_pass(2, HIGH)

    attended = jnp.sum(ar[...].astype(F32), axis=0)
    residual = attended.astype(BF16).astype(F32)
    for i in range(nz):
        resid[i] = residual[:, 64 * i : 64 * i + 64]
    squares = jnp.sum(residual * residual, axis=1, keepdims=True)
    mlp_in = (residual * gains).astype(BF16)
    ring_pass(4, UP)
    pre = dot(mlp_in, up_all[...].reshape(nz * 64, 1024))
    high = squares.astype(BF16).astype(F32)
    lane = iota((32, 128), 1)
    tail = jnp.where(lane == 0, high, jnp.where(lane == 1, squares - high, 0.0))
    ax[x] = jnp.concatenate([pre, tail], axis=1).astype(BF16)
    sent_u = []
    for d in range(1, NX):
        peer = z * NX + (x + d) % NX
        sent_u.append(remote(ax.at[x], ax.at[x], us, ur, peer, tp))
    for copy in sent_u:
        copy.start()
    ring_pass(3, LOW)
    ring_pass(3, HIGH)
    all_u = whole(ax.at[three], us, ur)
    all_u.wait_recv()
    total = jnp.sum(ax[...].astype(F32), axis=0)
    rms = lax.rsqrt((total[:, 1024:1025] + total[:, 1025:1026]) / MODEL + EPS)
    hidden = jnp.maximum(total[:, :1024] * rms, 0.0)
    hidden = (hidden * hidden).astype(BF16)
    near, distant = (0, 1, 7, 2), (6, 3, 5, 4)

    def project(half, places):
        for i in range(0, 4, 2):
            pair = [down_all[(z + places[j]) % nz] for j in (i, i + 1)]
            part = dot_nt(hidden, jnp.concatenate(pair, axis=0))
            rs[half, tp, :, 64 * i : 64 * i + 128] = part.astype(BF16)

        def send_rs(d, carry):
            to = (tp + d) % n_tp
            remote(rs.at[half, tp], rs.at[half, tp], ds_.at[half], dr.at[half], kv, to).start()
            return carry

        lax.fori_loop(1, n_tp, send_rs, 0)

    project(0, near)
    ring_pass(4, LOW)
    ring_pass(4, HIGH)
    project(1, distant)
    all_rs = [
        remote(rs.at[i, tps], rs.at[i, tps], ds_.at[i], dr.at[i], kv, tp) for i in range(2)
    ]

    for copy in all_x + [all_m, all_u]:
        copy.wait_send()

    @pl.when(z == tp)
    def _():
        whole(tokl.at[pl.ds(0, 32 * (nz - 1)), :], ts, tr).wait_send()

    for ref, sem in zip((out_all, up_all, down_all), range(3)):
        whole(ref.at[few], ring_s.at[sem], tr).wait_send()
    all_proj.wait_send()
    all_extra.wait_send()
    all_ar.wait_send()

    sent_f = []
    for half, places in enumerate((near, distant)):
        all_rs[half].wait_recv()
        added = jnp.sum(rs[half].astype(F32), axis=0)
        for i, place in enumerate(places):
            to = (z + place) % nz
            row = resid[to] + added[:, 64 * i : 64 * i + 64]
            fin_s[to] = row.astype(BF16)
            if place:
                copy = remote(fin_s.at[to], mx.at[z], fs, fr, to * NX + x, tp)
                copy.start()
                sent_f.append(copy)
            else:
                mx[z] = fin_s[z]
    all_f = whole(fin_s.at[few], fs, fr)
    for copy in all_rs:
        copy.wait_send()
    all_f.wait()
    mixed_ref[...] = mx[...].astype(F32).reshape(nz * 32, 64).T.astype(BF16)


def put(mixed, state, mixed_hbm, state_hbm, sem):
    copies = [pltpu.make_async_copy(mixed, mixed_hbm, sem.at[8])]
    for i in range(8):
        copies.append(pltpu.make_async_copy(state.at[i], state_hbm.at[i], sem.at[i]))
    for copy in copies:
        copy.start()
    for copy in copies:
        copy.wait()


def body(
    tokens,
    norm_gain,
    query_weight,
    key_weight,
    value_weight,
    gate_weight,
    beta_weight,
    decay_weight,
    decay_rate,
    head_gain,
    carried_state,
    block_keys,
    block_values,
    block_beta,
    block_decay,
    live_count,
    out_weight,
    mlp_gain,
    up_weight,
    down_weight,
):
    n_kv = lax.axis_size("kv")
    n_tp = lax.axis_size("tp")
    nz = n_kv // NX
    vmem = pl.BlockSpec(memory_space=pltpu.VMEM)
    hbm = pl.BlockSpec(memory_space=pltpu.HBM)
    dma = pltpu.SemaphoreType.DMA
    operands = (
        tokens.T,
        norm_gain.reshape(1, -1),
        query_weight,
        key_weight,
        value_weight,
        gate_weight,
        beta_weight.T,
        decay_weight.T,
        decay_rate,
        head_gain.reshape(1, -1),
        carried_state,
        block_keys,
        block_values,
        block_beta,
        block_decay,
        live_count,
        out_weight.T,
        mlp_gain.reshape(-1, 128),
        up_weight,
        down_weight.T,
    )
    mixed, new_state = pl.pallas_call(
        functools.partial(kernel, n_kv=n_kv, n_tp=n_tp),
        out_shape=(
            jax.ShapeDtypeStruct(tokens.shape[::-1], BF16),
            jax.ShapeDtypeStruct(carried_state.shape, F32),
        ),
        in_specs=[hbm] * 20,
        out_specs=(vmem, vmem),
        scratch_shapes=[
            pltpu.VMEM((4, 64, 256), BF16),
            pltpu.VMEM((256, 256), BF16),
            pltpu.VMEM((2, 16, 256), BF16),
            pltpu.VMEM((NX, 64, 256), BF16),
            pltpu.VMEM((NX, 1, 64), F32),
            pltpu.VMEM((256, 64), BF16),
            pltpu.VMEM((32, 64), BF16),
            pltpu.SMEM((2,), F32),
            pltpu.VMEM((1, 128), F32),
            pltpu.VMEM((8, 2, 64), F32),
            pltpu.VMEM((8, 2, 64), F32),
            pltpu.SMEM((8,), jnp.int32),
            pltpu.VMEM((16, 128), F32),
            pltpu.VMEM((n_kv, 8, 256), BF16),
            pltpu.VMEM((n_kv, 8, 256), BF16),
            pltpu.VMEM((n_kv, 8, 128), BF16),
            pltpu.VMEM((nz, 8, 128), BF16),
            pltpu.VMEM((8, 2, 64, 128), BF16),
            pltpu.VMEM((8, 2, 64, 128), BF16),
            pltpu.VMEM((256, 256), BF16),
            pltpu.VMEM((nz, 64, 1024), BF16),
            pltpu.VMEM((nz, 64, 1024), BF16),
            pltpu.VMEM((nz, 64, 256), BF16),
            pltpu.VMEM((4, 1, 256), F32),
            pltpu.VMEM((4, 1, 256), F32),
            pltpu.VMEM((NX, 8, 256), F32),
            pltpu.VMEM((n_tp, 32, 512), BF16),
            pltpu.VMEM((NX, 32, 1152), BF16),
            pltpu.VMEM((2, n_tp, 32, 256), BF16),
            pltpu.VMEM((nz, 32, 64), F32),
            pltpu.VMEM((nz, 32, 64), BF16),
            pltpu.VMEM((nz, 32, 64), BF16),
            dma((16,)),
            dma((3,)),
            dma((3,)),
            dma,
            dma,
            dma((2,)),
            dma((2,)),
            dma,
            dma,
            dma,
            dma,
            dma,
            dma,
            dma((2,)),
            dma((2,)),
            dma,
            dma,
            dma((3,)),
            dma((2, 4, 4)),
            pltpu.SemaphoreType.REGULAR((2,)),
        ],
        compiler_params=pltpu.CompilerParams(
            collective_id=0, has_side_effects=True, vmem_limit_bytes=40 * 1024 * 1024
        ),
        name="layer",
    )(*[pltpu.with_memory_space_constraint(a, pltpu.HBM) for a in operands])
    mixed, new_state = pl.pallas_call(
        put,
        out_shape=(
            jax.ShapeDtypeStruct(mixed.shape, BF16),
            jax.ShapeDtypeStruct(new_state.shape, F32),
        ),
        in_specs=[vmem, vmem],
        out_specs=(hbm, hbm),
        scratch_shapes=[dma((9,))],
        compiler_params=pltpu.CompilerParams(vmem_limit_bytes=16 * 1024 * 1024),
        name="put",
    )(mixed, new_state)
    return mixed.T, new_state


def solution(mesh):
    placed = (
        P(None, "kv"),
        P("kv"),
        P("kv", "tp"),
        P("kv", "tp"),
        P("kv", "tp"),
        P("kv", "tp"),
        P(),
        P(),
        P("tp"),
        P(),
        P("kv", "tp", None, None),
        P("kv", "tp", None, None),
        P("kv", "tp", None, None),
        P("kv", "tp", None),
        P("kv", "tp", None),
        P("kv"),
        P("tp", "kv"),
        P(),
        P("kv", "tp"),
        P("tp", "kv"),
    )
    return jax.shard_map(
        body,
        mesh=mesh,
        in_specs=placed,
        out_specs=(P(None, "kv"), P("kv", "tp", None, None)),
        check_vma=False,
    )
```

```python
import functools

import jax
import jax.numpy as jnp
from jax import lax
from jax.experimental import pallas as pl
from jax.experimental.pallas import tpu as pltpu
from jax.sharding import PartitionSpec as P

MODEL = 2048
HEADS = 16
EPS = 1e-06
NX = 4
F32 = jnp.float32
BF16 = jnp.bfloat16


def dot(a, b):
    return jnp.dot(a, b, preferred_element_type=F32)


def split(a):
    high = a.astype(BF16)
    return high, (a - high.astype(F32)).astype(BF16)


def dot_nt(a, b):
    return lax.dot_general(a, b, (((1,), (1,)), ((), ())), preferred_element_type=F32)


def dot2(a, b):
    bh, bl = split(b)
    return dot(a, bh) + dot(a, bl)


def iota(shape, dim):
    return lax.broadcasted_iota(jnp.int32, shape, dim)


def dot3(a, b):
    ah, al = split(a)
    bh, bl = split(b)
    n = a.shape[0]
    both = dot(jnp.concatenate([ah, al], axis=0), bh)
    return both[:n] + both[n:] + dot(ah, bl)


def apart(a, mask):
    return jnp.concatenate([a] * 4, axis=0) * mask


def dot3_blocks(a, b, mask):
    ah, al = split(a)
    bh, bl = split(b)
    both = dot(jnp.concatenate([ah, al], axis=0), apart(bh, mask))
    return both[:64] + both[64:] + dot(ah, apart(bl, mask))


def state_before(gs, between, keys, vals, state, bbeta, bdecay, live, mask_ref):
    r = iota((64, 256), 0)
    lane = iota((64, 256), 1)
    c = lane & 63
    pair = lane >> 6
    strict = c < r
    lane1 = iota((1, 256), 1)
    r1 = iota((256, 128), 0)
    zero = jnp.zeros((64, 128), F32)

    def side(columns):
        low = jnp.where(pair == 0, columns[0], columns[1])
        high = jnp.where(pair == 2, columns[2], columns[3])
        return jnp.where(pair < 2, low, high)

    def spread(blocks):
        rows = [[blocks[p] if q == p else zero for q in range(4)] for p in range(4)]
        return jnp.concatenate([jnp.concatenate(row, axis=1) for row in rows], axis=0)

    def prepare(g):
        n0, n1 = live[2 * g] - 1, live[2 * g + 1] - 1
        live_row = (lane1 & 63) < jnp.where(lane1 < 128, n0, n1)
        d_row = jnp.where(live_row, bdecay[g], 0.0)
        b_row = jnp.where(live_row, bbeta[g], 0.0)
        live_col = (r1 & 63) < jnp.where(r1 < 128, n0, n1)
        k_all = jnp.where(live_col, keys[2 * g : 2 * g + 2].astype(F32).reshape(256, 128), 0.0)
        kb = k_all.astype(BF16)
        kt = k_all.T.astype(BF16)
        b_diag = jnp.where(r == c, b_row, 0.0)
        d_tri = jnp.where(c <= r, d_row, 0.0)
        b_col, t_col = [], []
        for p in range(4):
            b_col.append(jnp.sum(jnp.where(pair == p, b_diag, 0.0), axis=1, keepdims=True))
            t_col.append(jnp.sum(jnp.where(pair == p, d_tri, 0.0), axis=1, keepdims=True))
        tots = side(t_col)
        tot_row = jnp.sum(jnp.where(r == c, tots, 0.0), axis=0, keepdims=True)
        fade = jnp.exp(jnp.where(strict, tots - tot_row, 0.0))
        gram = dot(kb, kt)
        gram = side([gram[64 * p : 64 * p + 64] for p in range(4)])
        lower = jnp.where(strict, side(b_col) * gram * fade, 0.0)
        return kb, kt, live_col, b_col, t_col, lower

    def same(bits):
        return (r >> bits) == (c >> bits)

    prepared = [prepare(g) for g in gs]
    lowers = [one[5] for one in prepared]
    mask = mask_ref[...]
    ident = jnp.where(r == c, 1.0, 0.0)
    powers = [jnp.where(same(3), -lower, 0.0) for lower in lowers]
    totals = [ident + power for power in powers]
    for _ in range(2):
        powers = [dot3_blocks(power, power, mask) for power in powers]
        more = [dot3_blocks(total, power, mask) for total, power in zip(totals, powers)]
        totals = [total + one for total, one in zip(totals, more)]
    between()
    for bits in (3, 4, 5):
        off = same(bits + 1) & jnp.logical_not(same(bits))
        offs = [jnp.where(off, lower, 0.0) for lower in lowers]
        offs = [dot3_blocks(one, total, mask) for one, total in zip(offs, totals)]
        more = [dot3_blocks(total, one, mask) for one, total in zip(offs, totals)]
        totals = [total - one for total, one in zip(totals, more)]
    rights = []
    for g, (kb, _, live_col, b_col, t_col, _) in zip(gs, prepared):
        v_all = jnp.where(live_col, vals[2 * g : 2 * g + 2].astype(F32).reshape(256, 128), 0.0)
        right = []
        for p in range(4):
            at = slice(64 * p, 64 * p + 64)
            seen = dot2(kb[at], state[2 * g + p // 2, p % 2])
            right.append(b_col[p] * (v_all[at] - jnp.exp(t_col[p]) * seen))
        rights.append(spread(right))
    updates = [dot3(total, right) for total, right in zip(totals, rights)]
    added = []
    for update, (_, kt, _, _, t_col, _) in zip(updates, prepared):
        faded = []
        for p in range(4):
            faded.append(update[:, 128 * p : 128 * p + 128] * jnp.exp(t_col[p][63:64] - t_col[p]))
        added.append(dot2(kt, spread(faded)))
    for g, one, (_, _, _, _, t_col, _) in zip(gs, added, prepared):
        for p in range(4):
            end = jnp.exp(t_col[p][63:64])
            at = (2 * g + p // 2, p % 2)
            state[at] = end * state[at] + one[:, 128 * p : 128 * p + 128]


def kernel(
    tok_hbm,
    ngain_hbm,
    qw_hbm,
    kw_hbm,
    vw_hbm,
    gw_hbm,
    bw_hbm,
    dw_hbm,
    rate_hbm,
    hgain_hbm,
    state_hbm,
    keys_hbm,
    vals_hbm,
    bbeta_hbm,
    bdecay_hbm,
    live_hbm,
    out_hbm,
    mgain_hbm,
    up_hbm,
    down_hbm,
    mixed_ref,
    state,
    wst,
    wcat,
    bdw,
    tokx,
    gp,
    tokl,
    tokt,
    rate_ref,
    hgain_ref,
    bbeta_ref,
    bdecay_ref,
    live_ref,
    mgain_ref,
    proj_s,
    proj_r,
    ex_s,
    ex_r,
    keys,
    vals,
    mask,
    up_all,
    down_all,
    out_all,
    bbeta,
    bdecay,
    mh,
    ar,
    ax,
    rs,
    resid,
    fin_s,
    mx,
    loc,
    xs,
    xr,
    ts,
    tr,
    ps,
    pr,
    ms,
    mr,
    asem,
    arr,
    us,
    ur,
    ds_,
    dr,
    fs,
    fr,
    ring_s,
    ring_r,
    round_r,
    *,
    n_kv,
    n_tp,
):
    kv = lax.axis_index("kv")
    tp = lax.axis_index("tp")
    nz = n_kv // NX
    z = kv // NX
    x = kv % NX

    def local(src, dst, i):
        copy = pltpu.make_async_copy(src, dst, loc.at[i])
        copy.start()
        return copy

    def remote(src, dst, s, r, kv_to, tp_to):
        return pltpu.make_async_remote_copy(
            src_ref=src,
            dst_ref=dst,
            send_sem=s,
            recv_sem=r,
            device_id={"kv": kv_to, "tp": tp_to},
            device_id_type=pl.DeviceIdType.MESH,
        )

    up_z = ((z + 1) % nz) * NX + x
    down_z = ((z + nz - 1) % nz) * NX + x
    barrier = pltpu.get_barrier_semaphore()

    def greet(sem, kv_to, tp_to):
        pl.semaphore_signal(
            sem,
            inc=1,
            device_id={"kv": kv_to, "tp": tp_to},
            device_id_type=pl.DeviceIdType.MESH,
        )

    near_z = [((z + d) % nz) * NX + x for d in (1, nz - 1, 2, nz - 2)]
    for to in near_z:
        greet(barrier, to, tp)
    for d in range(1, NX):
        greet(barrier, z * NX + (x + d) % NX, tp)

    def greet_tp(d, carry):
        greet(barrier, kv, (tp + d) % n_tp)
        return carry

    lax.fori_loop(1, n_tp, greet_tp, 0)

    in_tok = local(tok_hbm, tokx.at[x], 2)
    in_gain = local(ngain_hbm, gp.at[x], 3)
    in_w = [local(w, wst.at[i], 0) for i, w in enumerate((qw_hbm, kw_hbm, vw_hbm, gw_hbm))]
    in_out = local(out_hbm, out_all.at[z], 4)
    in_up = local(up_hbm, up_all.at[z], 5)
    in_down = local(down_hbm, down_all.at[z], 6)
    lanes_z = pl.ds(pl.multiple_of(z * 256, 256), 256)
    in_b = [
        local(bw_hbm.at[:, lanes_z], bdw.at[0], 1),
        local(dw_hbm.at[:, lanes_z], bdw.at[1], 1),
    ]
    in_block = [
        local(bbeta_hbm, bbeta_ref, 7),
        local(bdecay_hbm, bdecay_ref, 8),
        local(live_hbm, live_ref, 9),
        local(keys_hbm, keys, 10),
        local(vals_hbm, vals, 11),
        local(state_hbm, state, 12),
    ]
    in_small = [
        local(rate_hbm, rate_ref, 13),
        local(hgain_hbm, hgain_ref, 14),
        local(mgain_hbm, mgain_ref, 15),
    ]

    def round_send(i):
        for to in near_z:
            greet(round_r.at[i], to, tp)

    def round_wait(i):
        pl.semaphore_wait(round_r.at[i], 4)

    in_tok.wait()
    in_gain.wait()
    pltpu.make_async_copy(wst, wst, loc.at[0]).wait()
    mine = pl.ds(pl.multiple_of(x * 64, 64), 64)
    pl.semaphore_wait(barrier, 4 + NX - 1 + n_tp - 1)

    sent_x = []
    for d in range(1, NX):
        to = (x + d) % NX
        peer = z * NX + to
        sent_x.append(remote(tokx.at[x], tokx.at[x], xs.at[0], xr.at[0], peer, tp))
        sent_x.append(remote(gp.at[x], gp.at[x], xs.at[1], xr.at[1], peer, tp))
        sent_x.append(remote(wst.at[to], wcat.at[mine, :], xs.at[2], xr.at[2], peer, tp))
    for copy in sent_x:
        copy.start()

    sent_t = []
    for d in range(1, nz):
        to = (z + d) % nz
        part = tokl.at[pl.ds(pl.multiple_of(to * 32, 32), 32), :]
        sent_t.append(remote(part, tokt, ts, tr, to * NX + x, tp))

    def ring(way, step, what):
        to = up_z if way == 0 else down_z
        block = (z + nz - (step - 1)) % nz if way == 0 else (z + step - 1) % nz
        ref = (out_all, up_all, down_all, down_all)[what].at[block]
        first, rows = (0, 64) if what < 2 else (32 * (what - 2), 32)
        if step == nz // 2:
            first, rows = first + rows // 2 * way, rows // 2
        ref = ref.at[pl.ds(first, rows)]
        return remote(
            ref, ref, ring_s.at[min(what, 2)], ring_r.at[way, step - 1, what], to, tp
        )

    half = nz // 2

    def ring_start(step, what):
        for way in range(2):
            ring(way, step, what).start()

    def ring_pass(step, what):
        for way in range(2):
            ring(way, step, what).wait_recv()
            if step < half:
                ring(way, step + 1, what).start()

    OUT, UP, LOW, HIGH = 0, 1, 2, 3

    round_send(0)
    in_out.wait()
    in_up.wait()
    in_down.wait()
    ring_start(1, OUT)
    ring_start(1, UP)
    ring_start(1, LOW)

    for copy in in_block:
        copy.wait()
    for i in range(4):
        pairs = [(2 * i + j // 2, slice(j % 2, j % 2 + 1)) for j in range(4)]
        bbeta[i] = jnp.concatenate([bbeta_ref[pair] for pair in pairs], axis=1)
        bdecay[i] = jnp.concatenate([bdecay_ref[pair] for pair in pairs], axis=1)

    mask[...] = jnp.where((iota((256, 256), 0) >> 6) == (iota((256, 256), 1) >> 6), 1.0, 0.0).astype(
        BF16
    )
    wcat[mine, :] = wst[x]
    tokl[...] = tokx[x].astype(F32).T.astype(BF16)

    @pl.when(z == tp)
    def _():
        tokt[...] = tokl[pl.ds(pl.multiple_of(z * 32, 32), 32), :]


    def before(gs, between):
        state_before(gs, between, keys, vals, state, bbeta, bdecay, live_ref, mask)

    def early():
        round_wait(0)
        round_send(1)

        @pl.when(z == tp)
        def _():
            for copy in sent_t:
                copy.start()

        ring_pass(1, OUT)

    before((0, 1), early)

    three = pl.ds(0, NX - 1)

    def whole(ref, s, r):
        return remote(ref, ref, s, r, kv, tp)

    all_x = [
        whole(tokx.at[three], xs.at[0], xr.at[0]),
        whole(gp.at[three], xs.at[1], xr.at[1]),
        whole(wst.at[three], xs.at[2], xr.at[2]),
    ]
    for copy in all_x:
        copy.wait_recv()
    t = tokx[...].reshape(256, 256).astype(F32).T
    squares = jnp.sum(t * t, axis=1, keepdims=True)
    normed = (t * jnp.concatenate([gp[i] for i in range(NX)], axis=1)).astype(BF16)
    projected = dot(normed, wcat[...])
    pltpu.make_async_copy(bdw, bdw, loc.at[1]).wait()
    small = jnp.concatenate(
        [bdw[...].astype(F32).reshape(32, 256), jnp.zeros((96, 256), F32)], axis=0
    ).astype(BF16)
    extra = dot_nt(normed, small)
    proj_s[...] = projected.reshape(n_kv, 8, 256).astype(BF16)
    lane = iota((256, 128), 1)
    high = squares.astype(BF16).astype(F32)
    extra = jnp.where(lane == 32, high, jnp.where(lane == 33, squares - high, extra))
    ex_s[...] = extra.reshape(n_kv, 8, 128).astype(BF16)
    proj_r[kv] = proj_s[kv]
    ex_r[z] = ex_s[kv]

    sent_p = []
    for far in (4, 3, 5, 2, 6, 1, 7, 0):
        row = ((z + far) % nz) * NX
        for side in range(NX):
            if far or side:
                to = row + (x + side) % NX
                sent_p.append(remote(proj_s.at[to], proj_r.at[kv], ps.at[0], pr.at[0], to, tp))

    def send_extra(d, carry):
        to = ((z + d) % nz) * NX + x
        remote(ex_s.at[to], ex_r.at[z], ps.at[1], pr.at[1], to, tp).start()
        return carry

    round_wait(1)
    lax.fori_loop(1, nz, send_extra, 0)
    for copy in sent_p:
        copy.start()
    ring_pass(2, OUT)
    ring_pass(1, UP)
    ring_start(1, HIGH)
    before((2, 3), lambda: None)

    ring_pass(3, OUT)
    ring_pass(1, LOW)

    some = pl.ds(0, n_kv - 1)
    few = pl.ds(0, nz - 1)
    all_proj = remote(proj_s.at[some], proj_r.at[some], ps.at[0], pr.at[0], kv, tp)
    all_extra = remote(ex_s.at[few], ex_r.at[few], ps.at[1], pr.at[1], kv, tp)
    all_extra.wait_recv()
    all_proj.wait_recv()

    for copy in in_small:
        copy.wait()
    total = jnp.sum(proj_r[...].astype(F32).reshape(nz, NX, 8, 256), axis=0)
    extra = jnp.sum(ex_r[...].astype(F32), axis=0)
    inverse_rms = lax.rsqrt((extra[:, 32:33] + extra[:, 33:34]) / MODEL + EPS)
    extra = extra * inverse_rms
    queries, key_raw, value_raw, gate_raw = [total[i] * inverse_rms for i in range(4)]
    lane = iota((8, 128), 1)
    cols, heads = [], []
    for h in range(2):
        at = slice(128 * h, 128 * h + 128)
        k = key_raw[:, at]
        k = k * lax.rsqrt(jnp.sum(k * k, axis=1, keepdims=True) + EPS)
        k = k.astype(BF16).astype(F32)
        v = value_raw[:, at].astype(BF16).astype(F32)
        q = queries[:, at]
        b = jnp.sum(jnp.where(lane == 2 * tp + h, extra, 0.0), axis=1, keepdims=True)
        b = 1.0 / (1.0 + jnp.exp(-b))
        a = jnp.sum(jnp.where(lane == HEADS + 2 * tp + h, extra, 0.0), axis=1, keepdims=True)
        a = jnp.maximum(a, 0.0) + jnp.log1p(jnp.exp(-jnp.abs(a)))
        e = jnp.exp(-rate_ref[h] * a)
        qk = jnp.sum(q * k, axis=1, keepdims=True)
        cols += [k, q]
        heads.append((k, v, q, b, e, qk))
    columns = jnp.concatenate(cols + [jnp.zeros((96, 128), F32)], axis=0).T
    updates, readouts = {}, []
    for h in range(2):
        k, v, q, b, e, qk = heads[h]
        lines = []
        for s in range(8):
            old = state[s, h]
            one = slice(s, s + 1)
            kcol = columns[:, 16 * h + s : 16 * h + s + 1]
            qcol = columns[:, 16 * h + 8 + s : 16 * h + 9 + s]
            ks = jnp.sum(old * kcol, axis=0, keepdims=True)
            qs = jnp.sum(old * qcol, axis=0, keepdims=True)
            u = b[one] * (v[one] - e[one] * ks)
            updates[s, h] = u
            lines.append(e[one] * qs + qk[one] * u)
        readouts.append(jnp.concatenate(lines, axis=0))
    gated = []
    for h in range(2):
        rd = readouts[h]
        gate = gate_raw[:, 128 * h : 128 * h + 128]
        scaled = rd * lax.rsqrt(jnp.sum(rd * rd, axis=1, keepdims=True) / 128 + EPS) * hgain_ref[...]
        gated.append(scaled * (gate / (1.0 + jnp.exp(-gate))))
    mh[x] = jnp.concatenate(gated, axis=1).astype(BF16).astype(F32)
    sent_m = []
    for d in range(1, NX):
        peer = z * NX + (x + d) % NX
        sent_m.append(remote(mh.at[x], mh.at[x], ms, mr, peer, tp))
    for copy in sent_m:
        copy.start()
    ring_pass(2, UP)
    for h in range(2):
        e = heads[h][4]
        for s in range(8):
            kcol = columns[:, 16 * h + s : 16 * h + s + 1]
            state[s, h] = e[s : s + 1] * state[s, h] + kcol * updates[s, h]

    ring_pass(1, HIGH)

    all_m = whole(mh.at[three], ms, mr)
    all_m.wait_recv()
    ring_pass(4, OUT)
    m = mh[...].reshape(32, 256)
    partial = dot_nt(m.astype(BF16), out_all[...].reshape(nz * 64, 256))

    @pl.when(z != tp)
    def _():
        sent_t[0].wait_recv()

    tokens = jnp.concatenate([tokt[...].astype(F32)] * nz, axis=1)
    partial = partial + jnp.where((iota((32, 64 * nz), 1) >> 6) == tp, tokens, 0.0)
    ar[tp] = partial.astype(BF16)

    def send_ar(d, carry):
        to = (tp + d) % n_tp
        remote(ar.at[tp], ar.at[tp], asem, arr, kv, to).start()
        return carry

    lax.fori_loop(1, n_tp, send_ar, 0)
    ring_pass(3, UP)
    tps = pl.ds(0, n_tp - 1)
    all_ar = remote(ar.at[tps], ar.at[tps], asem, arr, kv, tp)
    gains = []
    for p in range(nz):
        gain = mgain_ref[pl.ds(2 * p + x // 2, 1), :]
        gains.append(jnp.where(x % 2 == 0, gain[:, :64], gain[:, 64:]))
    gains = jnp.concatenate(gains, axis=1)
    ring_pass(2, LOW)
    all_ar.wait_recv()
    ring_pass(2, HIGH)

    attended = jnp.sum(ar[...].astype(F32), axis=0)
    residual = attended.astype(BF16).astype(F32)
    for i in range(nz):
        resid[i] = residual[:, 64 * i : 64 * i + 64]
    squares = jnp.sum(residual * residual, axis=1, keepdims=True)
    mlp_in = (residual * gains).astype(BF16)
    ring_pass(4, UP)
    pre = dot(mlp_in, up_all[...].reshape(nz * 64, 1024))
    high = squares.astype(BF16).astype(F32)
    lane = iota((32, 128), 1)
    tail = jnp.where(lane == 0, high, jnp.where(lane == 1, squares - high, 0.0))
    ax[x] = jnp.concatenate([pre, tail], axis=1).astype(BF16)
    sent_u = []
    for d in range(1, NX):
        peer = z * NX + (x + d) % NX
        sent_u.append(remote(ax.at[x], ax.at[x], us, ur, peer, tp))
    for copy in sent_u:
        copy.start()
    ring_pass(3, LOW)
    ring_pass(3, HIGH)
    all_u = whole(ax.at[three], us, ur)
    all_u.wait_recv()
    total = jnp.sum(ax[...].astype(F32), axis=0)
    rms = lax.rsqrt((total[:, 1024:1025] + total[:, 1025:1026]) / MODEL + EPS)
    hidden = jnp.maximum(total[:, :1024] * rms, 0.0)
    hidden = (hidden * hidden).astype(BF16)
    near, distant = (0, 1, 7, 2), (6, 3, 5, 4)

    def project(half, places):
        for i in range(0, 4, 2):
            pair = [down_all[(z + places[j]) % nz] for j in (i, i + 1)]
            part = dot_nt(hidden, jnp.concatenate(pair, axis=0))
            rs[half, tp, :, 64 * i : 64 * i + 128] = part.astype(BF16)

        def send_rs(d, carry):
            to = (tp + d) % n_tp
            remote(rs.at[half, tp], rs.at[half, tp], ds_.at[half], dr.at[half], kv, to).start()
            return carry

        lax.fori_loop(1, n_tp, send_rs, 0)

    project(0, near)
    ring_pass(4, LOW)
    ring_pass(4, HIGH)
    project(1, distant)
    all_rs = [
        remote(rs.at[i, tps], rs.at[i, tps], ds_.at[i], dr.at[i], kv, tp) for i in range(2)
    ]

    for copy in all_x + [all_m, all_u]:
        copy.wait_send()

    @pl.when(z == tp)
    def _():
        whole(tokl.at[pl.ds(0, 32 * (nz - 1)), :], ts, tr).wait_send()

    for ref, sem in zip((out_all, up_all, down_all), range(3)):
        whole(ref.at[few], ring_s.at[sem], tr).wait_send()
    all_proj.wait_send()
    all_extra.wait_send()
    all_ar.wait_send()

    sent_f = []
    for half, places in enumerate((near, distant)):
        all_rs[half].wait_recv()
        added = jnp.sum(rs[half].astype(F32), axis=0)
        for i, place in enumerate(places):
            to = (z + place) % nz
            row = resid[to] + added[:, 64 * i : 64 * i + 64]
            fin_s[to] = row.astype(BF16)
            if place:
                copy = remote(fin_s.at[to], mx.at[z], fs, fr, to * NX + x, tp)
                copy.start()
                sent_f.append(copy)
            else:
                mx[z] = fin_s[z]
    all_f = whole(fin_s.at[few], fs, fr)
    for copy in all_rs:
        copy.wait_send()
    all_f.wait()
    mixed_ref[...] = mx[...].astype(F32).reshape(nz * 32, 64).T.astype(BF16)


def put(mixed, state, mixed_hbm, state_hbm, sem):
    copies = [pltpu.make_async_copy(mixed, mixed_hbm, sem.at[8])]
    for i in range(8):
        copies.append(pltpu.make_async_copy(state.at[i], state_hbm.at[i], sem.at[i]))
    for copy in copies:
        copy.start()
    for copy in copies:
        copy.wait()


def body(
    tokens,
    norm_gain,
    query_weight,
    key_weight,
    value_weight,
    gate_weight,
    beta_weight,
    decay_weight,
    decay_rate,
    head_gain,
    carried_state,
    block_keys,
    block_values,
    block_beta,
    block_decay,
    live_count,
    out_weight,
    mlp_gain,
    up_weight,
    down_weight,
):
    n_kv = lax.axis_size("kv")
    n_tp = lax.axis_size("tp")
    nz = n_kv // NX
    vmem = pl.BlockSpec(memory_space=pltpu.VMEM)
    hbm = pl.BlockSpec(memory_space=pltpu.HBM)
    dma = pltpu.SemaphoreType.DMA
    operands = (
        tokens.T,
        norm_gain.reshape(1, -1),
        query_weight,
        key_weight,
        value_weight,
        gate_weight,
        beta_weight.T,
        decay_weight.T,
        decay_rate,
        head_gain.reshape(1, -1),
        carried_state,
        block_keys,
        block_values,
        block_beta,
        block_decay,
        live_count,
        out_weight.T,
        mlp_gain.reshape(-1, 128),
        up_weight,
        down_weight.T,
    )
    mixed, new_state = pl.pallas_call(
        functools.partial(kernel, n_kv=n_kv, n_tp=n_tp),
        out_shape=(
            jax.ShapeDtypeStruct(tokens.shape[::-1], BF16),
            jax.ShapeDtypeStruct(carried_state.shape, F32),
        ),
        in_specs=[hbm] * 20,
        out_specs=(vmem, vmem),
        scratch_shapes=[
            pltpu.VMEM((4, 64, 256), BF16),
            pltpu.VMEM((256, 256), BF16),
            pltpu.VMEM((2, 16, 256), BF16),
            pltpu.VMEM((NX, 64, 256), BF16),
            pltpu.VMEM((NX, 1, 64), F32),
            pltpu.VMEM((256, 64), BF16),
            pltpu.VMEM((32, 64), BF16),
            pltpu.SMEM((2,), F32),
            pltpu.VMEM((1, 128), F32),
            pltpu.VMEM((8, 2, 64), F32),
            pltpu.VMEM((8, 2, 64), F32),
            pltpu.SMEM((8,), jnp.int32),
            pltpu.VMEM((16, 128), F32),
            pltpu.VMEM((n_kv, 8, 256), BF16),
            pltpu.VMEM((n_kv, 8, 256), BF16),
            pltpu.VMEM((n_kv, 8, 128), BF16),
            pltpu.VMEM((nz, 8, 128), BF16),
            pltpu.VMEM((8, 2, 64, 128), BF16),
            pltpu.VMEM((8, 2, 64, 128), BF16),
            pltpu.VMEM((256, 256), BF16),
            pltpu.VMEM((nz, 64, 1024), BF16),
            pltpu.VMEM((nz, 64, 1024), BF16),
            pltpu.VMEM((nz, 64, 256), BF16),
            pltpu.VMEM((4, 1, 256), F32),
            pltpu.VMEM((4, 1, 256), F32),
            pltpu.VMEM((NX, 8, 256), F32),
            pltpu.VMEM((n_tp, 32, 512), BF16),
            pltpu.VMEM((NX, 32, 1152), BF16),
            pltpu.VMEM((2, n_tp, 32, 256), BF16),
            pltpu.VMEM((nz, 32, 64), F32),
            pltpu.VMEM((nz, 32, 64), BF16),
            pltpu.VMEM((nz, 32, 64), BF16),
            dma((16,)),
            dma((3,)),
            dma((3,)),
            dma,
            dma,
            dma((2,)),
            dma((2,)),
            dma,
            dma,
            dma,
            dma,
            dma,
            dma,
            dma((2,)),
            dma((2,)),
            dma,
            dma,
            dma((3,)),
            dma((2, 4, 4)),
            pltpu.SemaphoreType.REGULAR((2,)),
        ],
        compiler_params=pltpu.CompilerParams(
            collective_id=0, has_side_effects=True, vmem_limit_bytes=40 * 1024 * 1024
        ),
        name="layer",
    )(*[pltpu.with_memory_space_constraint(a, pltpu.HBM) for a in operands])
    mixed, new_state = pl.pallas_call(
        put,
        out_shape=(
            jax.ShapeDtypeStruct(mixed.shape, BF16),
            jax.ShapeDtypeStruct(new_state.shape, F32),
        ),
        in_specs=[vmem, vmem],
        out_specs=(hbm, hbm),
        scratch_shapes=[dma((9,))],
        compiler_params=pltpu.CompilerParams(vmem_limit_bytes=16 * 1024 * 1024),
        name="put",
    )(mixed, new_state)
    return mixed.T, new_state


def solution(mesh):
    placed = (
        P(None, "kv"),
        P("kv"),
        P("kv", "tp"),
        P("kv", "tp"),
        P("kv", "tp"),
        P("kv", "tp"),
        P(),
        P(),
        P("tp"),
        P(),
        P("kv", "tp", None, None),
        P("kv", "tp", None, None),
        P("kv", "tp", None, None),
        P("kv", "tp", None),
        P("kv", "tp", None),
        P("kv"),
        P("tp", "kv"),
        P(),
        P("kv", "tp"),
        P("tp", "kv"),
    )
    return jax.shard_map(
        body,
        mesh=mesh,
        in_specs=placed,
        out_specs=(P(None, "kv"), P("kv", "tp", None, None)),
        check_vma=False,
    )
```

```python
import functools

import jax
import jax.numpy as jnp
from jax import lax
from jax.experimental import pallas as pl
from jax.experimental.pallas import tpu as pltpu
from jax.sharding import PartitionSpec as P

MODEL = 2048
HEADS = 16
EPS = 1e-06
NX = 4
F32 = jnp.float32
BF16 = jnp.bfloat16


def dot(a, b):
    return jnp.dot(a, b, preferred_element_type=F32)


def split(a):
    high = a.astype(BF16)
    return high, (a - high.astype(F32)).astype(BF16)


def dot_nt(a, b):
    return lax.dot_general(a, b, (((1,), (1,)), ((), ())), preferred_element_type=F32)


def dot2(a, b):
    bh, bl = split(b)
    return dot(a, bh) + dot(a, bl)


def iota(shape, dim):
    return lax.broadcasted_iota(jnp.int32, shape, dim)


def dot3(a, b):
    ah, al = split(a)
    bh, bl = split(b)
    n = a.shape[0]
    both = dot(jnp.concatenate([ah, al], axis=0), bh)
    return both[:n] + both[n:] + dot(ah, bl)


def apart(a, mask):
    return jnp.concatenate([a] * 4, axis=0) * mask


def dot3_blocks(a, b, mask):
    ah, al = split(a)
    bh, bl = split(b)
    both = dot(jnp.concatenate([ah, al], axis=0), apart(bh, mask))
    return both[:64] + both[64:] + dot(ah, apart(bl, mask))


def state_before(gs, between, keys, vals, state, bbeta, bdecay, live, mask_ref):
    r = iota((64, 256), 0)
    lane = iota((64, 256), 1)
    c = lane & 63
    pair = lane >> 6
    strict = c < r
    lane1 = iota((1, 256), 1)
    r1 = iota((256, 128), 0)
    zero = jnp.zeros((64, 128), F32)

    def side(columns):
        low = jnp.where(pair == 0, columns[0], columns[1])
        high = jnp.where(pair == 2, columns[2], columns[3])
        return jnp.where(pair < 2, low, high)

    def spread(blocks):
        rows = [[blocks[p] if q == p else zero for q in range(4)] for p in range(4)]
        return jnp.concatenate([jnp.concatenate(row, axis=1) for row in rows], axis=0)

    def prepare(g):
        n0, n1 = live[2 * g] - 1, live[2 * g + 1] - 1
        live_row = (lane1 & 63) < jnp.where(lane1 < 128, n0, n1)
        d_row = jnp.where(live_row, bdecay[g], 0.0)
        b_row = jnp.where(live_row, bbeta[g], 0.0)
        live_col = (r1 & 63) < jnp.where(r1 < 128, n0, n1)
        k_all = jnp.where(live_col, keys[2 * g : 2 * g + 2].astype(F32).reshape(256, 128), 0.0)
        kb = k_all.astype(BF16)
        kt = k_all.T.astype(BF16)
        b_diag = jnp.where(r == c, b_row, 0.0)
        d_tri = jnp.where(c <= r, d_row, 0.0)
        b_col, t_col = [], []
        for p in range(4):
            b_col.append(jnp.sum(jnp.where(pair == p, b_diag, 0.0), axis=1, keepdims=True))
            t_col.append(jnp.sum(jnp.where(pair == p, d_tri, 0.0), axis=1, keepdims=True))
        tots = side(t_col)
        tot_row = jnp.sum(jnp.where(r == c, tots, 0.0), axis=0, keepdims=True)
        fade = jnp.exp(jnp.where(strict, tots - tot_row, 0.0))
        gram = dot(kb, kt)
        gram = side([gram[64 * p : 64 * p + 64] for p in range(4)])
        lower = jnp.where(strict, side(b_col) * gram * fade, 0.0)
        return kb, kt, live_col, b_col, t_col, lower

    def same(bits):
        return (r >> bits) == (c >> bits)

    prepared = [prepare(g) for g in gs]
    lowers = [one[5] for one in prepared]
    mask = mask_ref[...]
    ident = jnp.where(r == c, 1.0, 0.0)
    powers = [jnp.where(same(3), -lower, 0.0) for lower in lowers]
    totals = [ident + power for power in powers]
    for _ in range(2):
        powers = [dot3_blocks(power, power, mask) for power in powers]
        more = [dot3_blocks(total, power, mask) for total, power in zip(totals, powers)]
        totals = [total + one for total, one in zip(totals, more)]
    between()
    for bits in (3, 4, 5):
        off = same(bits + 1) & jnp.logical_not(same(bits))
        offs = [jnp.where(off, lower, 0.0) for lower in lowers]
        offs = [dot3_blocks(one, total, mask) for one, total in zip(offs, totals)]
        more = [dot3_blocks(total, one, mask) for one, total in zip(offs, totals)]
        totals = [total - one for total, one in zip(totals, more)]
    rights = []
    for g, (kb, _, live_col, b_col, t_col, _) in zip(gs, prepared):
        v_all = jnp.where(live_col, vals[2 * g : 2 * g + 2].astype(F32).reshape(256, 128), 0.0)
        right = []
        for p in range(4):
            at = slice(64 * p, 64 * p + 64)
            seen = dot2(kb[at], state[2 * g + p // 2, p % 2])
            right.append(b_col[p] * (v_all[at] - jnp.exp(t_col[p]) * seen))
        rights.append(spread(right))
    updates = [dot3(total, right) for total, right in zip(totals, rights)]
    added = []
    for update, (_, kt, _, _, t_col, _) in zip(updates, prepared):
        faded = []
        for p in range(4):
            faded.append(update[:, 128 * p : 128 * p + 128] * jnp.exp(t_col[p][63:64] - t_col[p]))
        added.append(dot2(kt, spread(faded)))
    for g, one, (_, _, _, _, t_col, _) in zip(gs, added, prepared):
        for p in range(4):
            end = jnp.exp(t_col[p][63:64])
            at = (2 * g + p // 2, p % 2)
            state[at] = end * state[at] + one[:, 128 * p : 128 * p + 128]


def kernel(
    tok_hbm,
    ngain_hbm,
    qw_hbm,
    kw_hbm,
    vw_hbm,
    gw_hbm,
    bw_hbm,
    dw_hbm,
    rate_hbm,
    hgain_hbm,
    state_hbm,
    keys_hbm,
    vals_hbm,
    bbeta_hbm,
    bdecay_hbm,
    live_hbm,
    out_hbm,
    mgain_hbm,
    up_hbm,
    down_hbm,
    mixed_ref,
    state,
    wst,
    wcat,
    bdw,
    tokx,
    gp,
    tokl,
    tokt,
    rate_ref,
    hgain_ref,
    bbeta_ref,
    bdecay_ref,
    live_ref,
    mgain_ref,
    proj_s,
    proj_r,
    ex_s,
    ex_r,
    keys,
    vals,
    mask,
    up_all,
    down_all,
    out_all,
    bbeta,
    bdecay,
    mh,
    ar,
    ax,
    sq,
    rs,
    resid,
    fin_s,
    mx,
    loc,
    xs,
    xr,
    ts,
    tr,
    ps,
    pr,
    ms,
    mr,
    asem,
    arr,
    us,
    ur,
    sqs,
    sqr,
    ds_,
    dr,
    fs,
    fr,
    ring_s,
    ring_r,
    round_r,
    *,
    n_kv,
    n_tp,
):
    kv = lax.axis_index("kv")
    tp = lax.axis_index("tp")
    nz = n_kv // NX
    z = kv // NX
    x = kv % NX

    def local(src, dst, i):
        copy = pltpu.make_async_copy(src, dst, loc.at[i])
        copy.start()
        return copy

    def remote(src, dst, s, r, kv_to, tp_to):
        return pltpu.make_async_remote_copy(
            src_ref=src,
            dst_ref=dst,
            send_sem=s,
            recv_sem=r,
            device_id={"kv": kv_to, "tp": tp_to},
            device_id_type=pl.DeviceIdType.MESH,
        )

    up_z = ((z + 1) % nz) * NX + x
    down_z = ((z + nz - 1) % nz) * NX + x
    barrier = pltpu.get_barrier_semaphore()

    def greet(sem, kv_to, tp_to):
        pl.semaphore_signal(
            sem,
            inc=1,
            device_id={"kv": kv_to, "tp": tp_to},
            device_id_type=pl.DeviceIdType.MESH,
        )

    near_z = [((z + d) % nz) * NX + x for d in (1, nz - 1, 2, nz - 2)]
    for to in near_z:
        greet(barrier, to, tp)
    for d in range(1, NX):
        greet(barrier, z * NX + (x + d) % NX, tp)

    def greet_tp(d, carry):
        greet(barrier, kv, (tp + d) % n_tp)
        return carry

    lax.fori_loop(1, n_tp, greet_tp, 0)

    in_tok = local(tok_hbm, tokx.at[x], 2)
    in_gain = local(ngain_hbm, gp.at[x], 3)
    in_w = [local(w, wst.at[i], 0) for i, w in enumerate((qw_hbm, kw_hbm, vw_hbm, gw_hbm))]
    in_out = local(out_hbm, out_all.at[z], 4)
    in_up = local(up_hbm, up_all.at[z], 5)
    in_down = local(down_hbm, down_all.at[z], 6)
    lanes_z = pl.ds(pl.multiple_of(z * 256, 256), 256)
    in_b = [
        local(bw_hbm.at[:, lanes_z], bdw.at[0], 1),
        local(dw_hbm.at[:, lanes_z], bdw.at[1], 1),
    ]
    in_block = [
        local(bbeta_hbm, bbeta_ref, 7),
        local(bdecay_hbm, bdecay_ref, 8),
        local(live_hbm, live_ref, 9),
        local(keys_hbm, keys, 10),
        local(vals_hbm, vals, 11),
        local(state_hbm, state, 12),
    ]
    in_small = [
        local(rate_hbm, rate_ref, 13),
        local(hgain_hbm, hgain_ref, 14),
        local(mgain_hbm, mgain_ref, 15),
    ]

    def round_send(i):
        for to in near_z:
            greet(round_r.at[i], to, tp)

    def round_wait(i):
        pl.semaphore_wait(round_r.at[i], 4)

    in_tok.wait()
    in_gain.wait()
    pltpu.make_async_copy(wst, wst, loc.at[0]).wait()
    mine = pl.ds(pl.multiple_of(x * 64, 64), 64)
    pl.semaphore_wait(barrier, 4 + NX - 1 + n_tp - 1)

    sent_x = []
    for d in range(1, NX):
        to = (x + d) % NX
        peer = z * NX + to
        sent_x.append(remote(tokx.at[x], tokx.at[x], xs.at[0], xr.at[0], peer, tp))
        sent_x.append(remote(gp.at[x], gp.at[x], xs.at[1], xr.at[1], peer, tp))
        sent_x.append(remote(wst.at[to], wcat.at[mine, :], xs.at[2], xr.at[2], peer, tp))
    for copy in sent_x:
        copy.start()

    sent_t = []
    for d in range(1, nz):
        to = (z + d) % nz
        part = tokl.at[pl.ds(pl.multiple_of(to * 32, 32), 32), :]
        sent_t.append(remote(part, tokt, ts, tr, to * NX + x, tp))

    def ring(way, step, what):
        to = up_z if way == 0 else down_z
        block = (z + nz - (step - 1)) % nz if way == 0 else (z + step - 1) % nz
        ref = (out_all, up_all, up_all, down_all, down_all)[what].at[block]
        first, rows = (0, 64) if what == 0 else (32 * ((what - 1) % 2), 32)
        if step == nz // 2:
            first, rows = first + rows // 2 * way, rows // 2
        ref = ref.at[pl.ds(first, rows)]
        return remote(
            ref, ref, ring_s.at[(what + 1) // 2], ring_r.at[way, step - 1, what], to, tp
        )

    half = nz // 2

    def ring_start(step, what):
        for way in range(2):
            ring(way, step, what).start()

    def ring_pass(step, what):
        for way in range(2):
            ring(way, step, what).wait_recv()
            if step < half:
                ring(way, step + 1, what).start()

    OUT, UP, UQ, LOW, HIGH = 0, 1, 2, 3, 4

    round_send(0)
    in_out.wait()
    in_up.wait()
    in_down.wait()
    ring_start(1, OUT)
    ring_start(1, UP)
    ring_start(1, UQ)
    ring_start(1, LOW)

    for copy in in_block:
        copy.wait()
    for i in range(4):
        pairs = [(2 * i + j // 2, slice(j % 2, j % 2 + 1)) for j in range(4)]
        bbeta[i] = jnp.concatenate([bbeta_ref[pair] for pair in pairs], axis=1)
        bdecay[i] = jnp.concatenate([bdecay_ref[pair] for pair in pairs], axis=1)

    mask[...] = jnp.where((iota((256, 256), 0) >> 6) == (iota((256, 256), 1) >> 6), 1.0, 0.0).astype(
        BF16
    )
    wcat[mine, :] = wst[x]
    tokl[...] = tokx[x].astype(F32).T.astype(BF16)

    @pl.when(z == tp)
    def _():
        tokt[...] = tokl[pl.ds(pl.multiple_of(z * 32, 32), 32), :]


    def before(gs, between):
        state_before(gs, between, keys, vals, state, bbeta, bdecay, live_ref, mask)

    def early():
        round_wait(0)
        round_send(1)

        @pl.when(z == tp)
        def _():
            for copy in sent_t:
                copy.start()

        ring_pass(1, OUT)

    before((0, 1), early)

    three = pl.ds(0, NX - 1)

    def whole(ref, s, r):
        return remote(ref, ref, s, r, kv, tp)

    all_x = [
        whole(tokx.at[three], xs.at[0], xr.at[0]),
        whole(gp.at[three], xs.at[1], xr.at[1]),
        whole(wst.at[three], xs.at[2], xr.at[2]),
    ]
    for copy in all_x:
        copy.wait_recv()
    t = tokx[...].reshape(256, 256).astype(F32).T
    squares = jnp.sum(t * t, axis=1, keepdims=True)
    normed = (t * jnp.concatenate([gp[i] for i in range(NX)], axis=1)).astype(BF16)
    projected = dot(normed, wcat[...])
    pltpu.make_async_copy(bdw, bdw, loc.at[1]).wait()
    small = jnp.concatenate(
        [bdw[...].astype(F32).reshape(32, 256), jnp.zeros((96, 256), F32)], axis=0
    ).astype(BF16)
    extra = dot_nt(normed, small)
    proj_s[...] = projected.reshape(n_kv, 8, 256).astype(BF16)
    lane = iota((256, 128), 1)
    high = squares.astype(BF16).astype(F32)
    extra = jnp.where(lane == 32, high, jnp.where(lane == 33, squares - high, extra))
    ex_s[...] = extra.reshape(n_kv, 8, 128).astype(BF16)
    proj_r[kv] = proj_s[kv]
    ex_r[z] = ex_s[kv]

    sent_p = []
    for far in (4, 3, 5, 2, 6, 1, 7, 0):
        row = ((z + far) % nz) * NX
        for side in range(NX):
            if far or side:
                to = row + (x + side) % NX
                sent_p.append(remote(proj_s.at[to], proj_r.at[kv], ps.at[0], pr.at[0], to, tp))

    def send_extra(d, carry):
        to = ((z + d) % nz) * NX + x
        remote(ex_s.at[to], ex_r.at[z], ps.at[1], pr.at[1], to, tp).start()
        return carry

    round_wait(1)
    lax.fori_loop(1, nz, send_extra, 0)
    for copy in sent_p:
        copy.start()

    def later():
        ring_pass(2, OUT)
        ring_pass(1, UP)
        ring_pass(1, UQ)
        ring_start(1, HIGH)

    before((2, 3), later)

    ring_pass(3, OUT)
    ring_pass(1, LOW)

    some = pl.ds(0, n_kv - 1)
    few = pl.ds(0, nz - 1)
    all_proj = remote(proj_s.at[some], proj_r.at[some], ps.at[0], pr.at[0], kv, tp)
    all_extra = remote(ex_s.at[few], ex_r.at[few], ps.at[1], pr.at[1], kv, tp)
    all_extra.wait_recv()
    all_proj.wait_recv()

    for copy in in_small:
        copy.wait()
    total = jnp.sum(proj_r[...].astype(F32).reshape(nz, NX, 8, 256), axis=0)
    extra = jnp.sum(ex_r[...].astype(F32), axis=0)
    inverse_rms = lax.rsqrt((extra[:, 32:33] + extra[:, 33:34]) / MODEL + EPS)
    extra = extra * inverse_rms
    queries, key_raw, value_raw, gate_raw = [total[i] * inverse_rms for i in range(4)]
    lane = iota((8, 128), 1)
    cols, heads = [], []
    for h in range(2):
        at = slice(128 * h, 128 * h + 128)
        k = key_raw[:, at]
        k = k * lax.rsqrt(jnp.sum(k * k, axis=1, keepdims=True) + EPS)
        k = k.astype(BF16).astype(F32)
        v = value_raw[:, at].astype(BF16).astype(F32)
        q = queries[:, at]
        b = jnp.sum(jnp.where(lane == 2 * tp + h, extra, 0.0), axis=1, keepdims=True)
        b = 1.0 / (1.0 + jnp.exp(-b))
        a = jnp.sum(jnp.where(lane == HEADS + 2 * tp + h, extra, 0.0), axis=1, keepdims=True)
        a = jnp.maximum(a, 0.0) + jnp.log1p(jnp.exp(-jnp.abs(a)))
        e = jnp.exp(-rate_ref[h] * a)
        qk = jnp.sum(q * k, axis=1, keepdims=True)
        cols += [k, q]
        heads.append((k, v, q, b, e, qk))
    columns = jnp.concatenate(cols + [jnp.zeros((96, 128), F32)], axis=0).T
    updates, readouts = {}, []
    for h in range(2):
        k, v, q, b, e, qk = heads[h]
        lines = []
        for s in range(8):
            old = state[s, h]
            one = slice(s, s + 1)
            kcol = columns[:, 16 * h + s : 16 * h + s + 1]
            qcol = columns[:, 16 * h + 8 + s : 16 * h + 9 + s]
            ks = jnp.sum(old * kcol, axis=0, keepdims=True)
            qs = jnp.sum(old * qcol, axis=0, keepdims=True)
            u = b[one] * (v[one] - e[one] * ks)
            updates[s, h] = u
            lines.append(e[one] * qs + qk[one] * u)
        readouts.append(jnp.concatenate(lines, axis=0))
    gated = []
    for h in range(2):
        rd = readouts[h]
        gate = gate_raw[:, 128 * h : 128 * h + 128]
        scaled = rd * lax.rsqrt(jnp.sum(rd * rd, axis=1, keepdims=True) / 128 + EPS) * hgain_ref[...]
        gated.append(scaled * (gate / (1.0 + jnp.exp(-gate))))
    mh[x] = jnp.concatenate(gated, axis=1).astype(BF16).astype(F32)
    sent_m = []
    for d in range(1, NX):
        peer = z * NX + (x + d) % NX
        sent_m.append(remote(mh.at[x], mh.at[x], ms, mr, peer, tp))
    for copy in sent_m:
        copy.start()
    ring_pass(2, UP)
    ring_pass(2, UQ)
    for h in range(2):
        e = heads[h][4]
        for s in range(8):
            kcol = columns[:, 16 * h + s : 16 * h + s + 1]
            state[s, h] = e[s : s + 1] * state[s, h] + kcol * updates[s, h]

    ring_pass(1, HIGH)

    all_m = whole(mh.at[three], ms, mr)
    all_m.wait_recv()
    ring_pass(4, OUT)
    m = mh[...].reshape(32, 256)
    partial = dot_nt(m.astype(BF16), out_all[...].reshape(nz * 64, 256))

    @pl.when(z != tp)
    def _():
        sent_t[0].wait_recv()

    tokens = jnp.concatenate([tokt[...].astype(F32)] * nz, axis=1)
    partial = partial + jnp.where((iota((32, 64 * nz), 1) >> 6) == tp, tokens, 0.0)
    ar[tp] = partial.astype(BF16)

    def send_ar(d, carry):
        to = (tp + d) % n_tp
        remote(ar.at[tp], ar.at[tp], asem, arr, kv, to).start()
        return carry

    lax.fori_loop(1, n_tp, send_ar, 0)
    ring_pass(3, UP)
    ring_pass(3, UQ)
    tps = pl.ds(0, n_tp - 1)
    all_ar = remote(ar.at[tps], ar.at[tps], asem, arr, kv, tp)
    gains = []
    for p in range(nz):
        gain = mgain_ref[pl.ds(2 * p + x // 2, 1), :]
        gains.append(jnp.where(x % 2 == 0, gain[:, :64], gain[:, 64:]))
    gains = jnp.concatenate(gains, axis=1)
    ring_pass(2, LOW)
    all_ar.wait_recv()
    ring_pass(2, HIGH)

    attended = jnp.sum(ar[...].astype(F32), axis=0)
    residual = attended.astype(BF16).astype(F32)
    for i in range(nz):
        resid[i] = residual[:, 64 * i : 64 * i + 64]
    squares = jnp.sum(residual * residual, axis=1, keepdims=True)
    row = iota((32, 128), 0) == iota((32, 128), 1)
    sq[x] = jnp.sum(jnp.where(row, squares, 0.0), axis=0, keepdims=True)
    for d in range(1, NX):
        remote(sq.at[x], sq.at[x], sqs, sqr, z * NX + (x + d) % NX, tp).start()
    all_q = whole(sq.at[three], sqs, sqr)
    mlp_in = (residual * gains).astype(BF16)
    ring_pass(4, UP)
    ring_pass(4, UQ)
    pre = dot(mlp_in, up_all[...].reshape(nz * 64, 1024))
    ax[x] = pre.astype(BF16)
    sent_u = []
    for d in range(1, NX):
        peer = z * NX + (x + d) % NX
        sent_u.append(remote(ax.at[x], ax.at[x], us, ur, peer, tp))
    for copy in sent_u:
        copy.start()
    ring_pass(3, LOW)
    ring_pass(3, HIGH)
    all_u = whole(ax.at[three], us, ur)
    all_u.wait_recv()
    all_q.wait_recv()
    total = jnp.sum(ax[...].astype(F32), axis=0)
    squares = jnp.where(row, jnp.sum(sq[...], axis=0), 0.0)
    rms = lax.rsqrt(jnp.sum(squares, axis=1, keepdims=True) / MODEL + EPS)
    hidden = jnp.maximum(total * rms, 0.0)
    hidden = (hidden * hidden).astype(BF16)
    near, distant = (0, 1, 7, 2), (6, 3, 5, 4)

    def project(half, places):
        for i in range(0, 4, 2):
            pair = [down_all[(z + places[j]) % nz] for j in (i, i + 1)]
            part = dot_nt(hidden, jnp.concatenate(pair, axis=0))
            rs[half, tp, :, 64 * i : 64 * i + 128] = part.astype(BF16)

        def send_rs(d, carry):
            to = (tp + d) % n_tp
            remote(rs.at[half, tp], rs.at[half, tp], ds_.at[half], dr.at[half], kv, to).start()
            return carry

        lax.fori_loop(1, n_tp, send_rs, 0)

    project(0, near)
    ring_pass(4, LOW)
    ring_pass(4, HIGH)
    project(1, distant)
    all_rs = [
        remote(rs.at[i, tps], rs.at[i, tps], ds_.at[i], dr.at[i], kv, tp) for i in range(2)
    ]

    for copy in all_x + [all_m, all_u, all_q]:
        copy.wait_send()

    @pl.when(z == tp)
    def _():
        whole(tokl.at[pl.ds(0, 32 * (nz - 1)), :], ts, tr).wait_send()

    for ref, sem in zip((out_all, up_all, down_all), range(3)):
        whole(ref.at[few], ring_s.at[sem], tr).wait_send()
    all_proj.wait_send()
    all_extra.wait_send()
    all_ar.wait_send()

    sent_f = []
    for half, places in enumerate((near, distant)):
        all_rs[half].wait_recv()
        added = jnp.sum(rs[half].astype(F32), axis=0)
        for i, place in enumerate(places):
            to = (z + place) % nz
            row = resid[to] + added[:, 64 * i : 64 * i + 64]
            fin_s[to] = row.astype(BF16)
            if place:
                copy = remote(fin_s.at[to], mx.at[z], fs, fr, to * NX + x, tp)
                copy.start()
                sent_f.append(copy)
            else:
                mx[z] = fin_s[z]
    all_f = whole(fin_s.at[few], fs, fr)
    for copy in all_rs:
        copy.wait_send()
    all_f.wait()
    mixed_ref[...] = mx[...].astype(F32).reshape(nz * 32, 64).T.astype(BF16)


def put(mixed, state, mixed_hbm, state_hbm, sem):
    copies = [pltpu.make_async_copy(mixed, mixed_hbm, sem.at[8])]
    for i in range(8):
        copies.append(pltpu.make_async_copy(state.at[i], state_hbm.at[i], sem.at[i]))
    for copy in copies:
        copy.start()
    for copy in copies:
        copy.wait()


def body(
    tokens,
    norm_gain,
    query_weight,
    key_weight,
    value_weight,
    gate_weight,
    beta_weight,
    decay_weight,
    decay_rate,
    head_gain,
    carried_state,
    block_keys,
    block_values,
    block_beta,
    block_decay,
    live_count,
    out_weight,
    mlp_gain,
    up_weight,
    down_weight,
):
    n_kv = lax.axis_size("kv")
    n_tp = lax.axis_size("tp")
    nz = n_kv // NX
    vmem = pl.BlockSpec(memory_space=pltpu.VMEM)
    hbm = pl.BlockSpec(memory_space=pltpu.HBM)
    dma = pltpu.SemaphoreType.DMA
    operands = (
        tokens.T,
        norm_gain.reshape(1, -1),
        query_weight,
        key_weight,
        value_weight,
        gate_weight,
        beta_weight.T,
        decay_weight.T,
        decay_rate,
        head_gain.reshape(1, -1),
        carried_state,
        block_keys,
        block_values,
        block_beta,
        block_decay,
        live_count,
        out_weight.T,
        mlp_gain.reshape(-1, 128),
        up_weight,
        down_weight.T,
    )
    mixed, new_state = pl.pallas_call(
        functools.partial(kernel, n_kv=n_kv, n_tp=n_tp),
        out_shape=(
            jax.ShapeDtypeStruct(tokens.shape[::-1], BF16),
            jax.ShapeDtypeStruct(carried_state.shape, F32),
        ),
        in_specs=[hbm] * 20,
        out_specs=(vmem, vmem),
        scratch_shapes=[
            pltpu.VMEM((4, 64, 256), BF16),
            pltpu.VMEM((256, 256), BF16),
            pltpu.VMEM((2, 16, 256), BF16),
            pltpu.VMEM((NX, 64, 256), BF16),
            pltpu.VMEM((NX, 1, 64), F32),
            pltpu.VMEM((256, 64), BF16),
            pltpu.VMEM((32, 64), BF16),
            pltpu.SMEM((2,), F32),
            pltpu.VMEM((1, 128), F32),
            pltpu.VMEM((8, 2, 64), F32),
            pltpu.VMEM((8, 2, 64), F32),
            pltpu.SMEM((8,), jnp.int32),
            pltpu.VMEM((16, 128), F32),
            pltpu.VMEM((n_kv, 8, 256), BF16),
            pltpu.VMEM((n_kv, 8, 256), BF16),
            pltpu.VMEM((n_kv, 8, 128), BF16),
            pltpu.VMEM((nz, 8, 128), BF16),
            pltpu.VMEM((8, 2, 64, 128), BF16),
            pltpu.VMEM((8, 2, 64, 128), BF16),
            pltpu.VMEM((256, 256), BF16),
            pltpu.VMEM((nz, 64, 1024), BF16),
            pltpu.VMEM((nz, 64, 1024), BF16),
            pltpu.VMEM((nz, 64, 256), BF16),
            pltpu.VMEM((4, 1, 256), F32),
            pltpu.VMEM((4, 1, 256), F32),
            pltpu.VMEM((NX, 8, 256), F32),
            pltpu.VMEM((n_tp, 32, 512), BF16),
            pltpu.VMEM((NX, 32, 1024), BF16),
            pltpu.VMEM((NX, 1, 128), F32),
            pltpu.VMEM((2, n_tp, 32, 256), BF16),
            pltpu.VMEM((nz, 32, 64), F32),
            pltpu.VMEM((nz, 32, 64), BF16),
            pltpu.VMEM((nz, 32, 64), BF16),
            dma((16,)),
            dma((3,)),
            dma((3,)),
            dma,
            dma,
            dma((2,)),
            dma((2,)),
            dma,
            dma,
            dma,
            dma,
            dma,
            dma,
            dma,
            dma,
            dma((2,)),
            dma((2,)),
            dma,
            dma,
            dma((3,)),
            dma((2, 4, 5)),
            pltpu.SemaphoreType.REGULAR((2,)),
        ],
        compiler_params=pltpu.CompilerParams(
            collective_id=0, has_side_effects=True, vmem_limit_bytes=40 * 1024 * 1024
        ),
        name="layer",
    )(*[pltpu.with_memory_space_constraint(a, pltpu.HBM) for a in operands])
    mixed, new_state = pl.pallas_call(
        put,
        out_shape=(
            jax.ShapeDtypeStruct(mixed.shape, BF16),
            jax.ShapeDtypeStruct(new_state.shape, F32),
        ),
        in_specs=[vmem, vmem],
        out_specs=(hbm, hbm),
        scratch_shapes=[dma((9,))],
        compiler_params=pltpu.CompilerParams(vmem_limit_bytes=16 * 1024 * 1024),
        name="put",
    )(mixed, new_state)
    return mixed.T, new_state


def solution(mesh):
    placed = (
        P(None, "kv"),
        P("kv"),
        P("kv", "tp"),
        P("kv", "tp"),
        P("kv", "tp"),
        P("kv", "tp"),
        P(),
        P(),
        P("tp"),
        P(),
        P("kv", "tp", None, None),
        P("kv", "tp", None, None),
        P("kv", "tp", None, None),
        P("kv", "tp", None),
        P("kv", "tp", None),
        P("kv"),
        P("tp", "kv"),
        P(),
        P("kv", "tp"),
        P("tp", "kv"),
    )
    return jax.shard_map(
        body,
        mesh=mesh,
        in_specs=placed,
        out_specs=(P(None, "kv"), P("kv", "tp", None, None)),
        check_vma=False,
    )
```
